128 devices in a mesh: sp: 16 (over z, x), fs: 4 (over y), tp: 2 (over core).
Axes of the slice: x: 4, y: 4, z: 4, core: 2. Of those that a mesh axis runs over, the one named last changes fastest.
Arguments:
- stream: bfloat16 [4, 16384, 2048], P('fs', 'sp', 'tp'), parts along dimension 0, may hold values from -6 to 6
- w_pool_in: bfloat16 [2048, 1024], P(None, 'tp'), may hold values from -0.125 to 0.125
- w_query: bfloat16 [2048, 1024], P(None, 'tp'), may hold values from -0.125 to 0.125
- w_forget: bfloat16 [2048, 1024], P(None, 'tp'), may hold values from -0.125 to 0.125
- w_value: bfloat16 [2048, 1024], P(None, 'tp'), may hold values from -0.125 to 0.125
- w_outgate: bfloat16 [2048, 1024], P(None, 'tp'), may hold values from -0.125 to 0.125
- pool_mix: bfloat16 [4, 256, 256], P('tp'), may hold values from -0.375 to 0.375
- pool_scale: float32 [1024], P('tp'), may hold values from 0.1 to 1.9
- lower_bound: float32 [1024], P('tp'), may hold values from 0.9 to 1
- extra_decay: float32 [16384, 8], P('sp', 'tp'), may hold values from -0.7 to 0
- rec_gain: float32 [128], replicated, may hold values from 0.1 to 1.9
- w_out_pool: bfloat16 [1024, 2048], P('tp'), may hold values from -0.125 to 0.125
- w_out_rec: bfloat16 [1024, 2048], P('tp'), may hold values from -0.125 to 0.125
- norm_gain: float32 [2048], P('tp'), may hold values from 0.1 to 1.9
- norm_bias: float32 [2048], P('tp'), may hold values from -3 to 3
Outputs:
- layer_out: bfloat16 [4, 16384, 2048], P('fs', 'sp', 'tp'), parts along dimension 0
The draws below stay inside these ranges and needn't reach their ends.
There are 4 independent parts, one for each index of `fs`. The reference program is written for one: setup_inputs(seed, part) draws one part's arguments, and reference() takes and returns one part's arrays. A program takes and returns all parts, laid end to end along the dimension named above; an argument that names none is the same for every part. Nothing has to cross between parts.
All inputs are finite; a program needn't handle non-finite values.
Results may differ from the reference program's by a relative error of at most 0.0085.
Values may be sent and summed in bfloat16 or wider, within the bound.
A program may use at most 128 MiB of HBM per device.

```python
import math
import jax
import jax.numpy as jnp
from jax import lax

D = 2048
POOL_W = 1024
REC_W = 1024
DK = 128
WMAX = 16
BLOCK_ROWS = 128
TOK_DEV = 1024
GROUP_CH = 256
HEADS = 8
SEQ = 16384


def draw_lower_bound(key, part):
    key_order = jax.random.fold_in(key, 11)
    key_fast = jax.random.fold_in(key, 12)
    key_slow = jax.random.fold_in(key, 13)
    order = jax.random.permutation(key_order, HEADS)
    chosen = order < HEADS // 2
    fast_gap = jnp.exp(jax.random.uniform(key_fast, (HEADS, DK), jnp.float32, math.log(0.03), math.log(0.06)))
    slow_gap = jnp.exp(jax.random.uniform(key_slow, (HEADS, DK), jnp.float32, math.log(0.16 / SEQ), math.log(0.8 / SEQ)))
    gaps = jnp.where(chosen[:, None], fast_gap, slow_gap)
    return (1.0 - gaps).reshape(REC_W).astype(jnp.float32)


def draw_extra_decay(key, part):
    key_base = jax.random.fold_in(key, 21)
    key_where = jax.random.fold_in(key, 22)
    key_drop = jax.random.fold_in(key, 23)
    blocks = SEQ // TOK_DEV
    base = jnp.exp(jax.random.uniform(key_base, (blocks,), jnp.float32, math.log(0.04 / SEQ), math.log(0.2 / SEQ)))
    base_rows = jnp.repeat(base, TOK_DEV)
    places = jax.random.randint(key_where, (2,), 0, SEQ)
    marked = jnp.any(jnp.arange(SEQ)[:, None] == places[None, :], axis=1)
    drops = jax.random.uniform(key_drop, (SEQ, HEADS), jnp.float32, 0.22, 0.69)
    total = base_rows[:, None] + jnp.where(marked[:, None], drops, jnp.float32(0.0))
    return (-total).astype(jnp.float32)


def shard_levels(rng, shape, split, least, largest):
    gain = 1.0
    for axis_at, parts in split:
        draws = jax.random.uniform(jax.random.fold_in(jax.random.fold_in(rng, 6), axis_at), (parts,), jnp.float32, least / len(split), largest / len(split))
        gain = gain * jnp.repeat(jnp.exp(draws), shape[axis_at] // parts).reshape((-1,) + (1,) * (len(shape) - 1 - axis_at))
    return gain


def normal_values(key, dims, width, bound, shards=(), dtype=jnp.bfloat16):
    factor_of = shard_levels(key, dims, shards, -0.22, 0.18) if shards else 1.0
    result = jax.random.normal(key, dims, jnp.float32) * width * factor_of
    return jnp.minimum(jnp.maximum(result, -bound), bound).astype(dtype)


def setup_inputs(seed: int = 0, part: int = 0) -> dict:
    key_list = jax.random.split(jax.random.key(seed), 16)
    own_keys = jax.random.split(jax.random.fold_in(key_list[15], part), 16)
    return {
        "stream": normal_values(own_keys[0], (1, SEQ, D), 1.0, 6.0, ((1, 16), (2, 2))),
        "w_pool_in": normal_values(key_list[1], (D, POOL_W), D ** -0.5, 0.125, ((1, 2),)),
        "w_query": normal_values(key_list[2], (D, REC_W), D ** -0.5, 0.125, ((1, 2),)),
        "w_forget": normal_values(key_list[3], (D, REC_W), D ** -0.5, 0.125, ((1, 2),)),
        "w_value": normal_values(key_list[4], (D, REC_W), D ** -0.5, 0.125, ((1, 2),)),
        "w_outgate": normal_values(key_list[5], (D, REC_W), D ** -0.5, 0.125, ((1, 2),)),
        "pool_mix": normal_values(key_list[6], (4, GROUP_CH, GROUP_CH), GROUP_CH ** -0.5, 0.375, ((0, 2),)),
        "pool_scale": jnp.clip(1.0 + 0.18 * jax.random.normal(key_list[7], (POOL_W,), jnp.float32), 0.1, 1.9),
        "lower_bound": draw_lower_bound(jax.random.fold_in(key_list[15], 71), part),
        "extra_decay": draw_extra_decay(jax.random.fold_in(key_list[15], 71), part),
        "rec_gain": jnp.clip(1.0 + 0.18 * jax.random.normal(key_list[10], (DK,), jnp.float32), 0.1, 1.9),
        "w_out_pool": normal_values(key_list[11], (POOL_W, D), (POOL_W + REC_W) ** -0.5, 0.125, ((0, 2),)),
        "w_out_rec": normal_values(key_list[12], (REC_W, D), (POOL_W + REC_W) ** -0.5, 0.125, ((0, 2),)),
        "norm_gain": jnp.clip(1.0 + 0.18 * jax.random.normal(key_list[13], (D,), jnp.float32), 0.1, 1.9),
        "norm_bias": normal_values(key_list[14], (D,), 0.5, 3.0, ((0, 2),), jnp.float32),
    }


ALPHA = 2.0 ** 0.25
EPS_RMS = 1e-06
EPS_NORM = 1e-05
HIGHEST = lax.Precision.HIGHEST

def pool_branch(pooled, pool_mix, pool_scale):
    length = pooled.shape[0]
    data = pooled.astype(jnp.float32)
    padded = jnp.pad(data, ((WMAX - 1, 0), (0, 0)))
    group_id = jnp.arange(POOL_W).astype(jnp.int32) // GROUP_CH
    window_len = jnp.left_shift(jnp.ones_like(group_id), group_id + 1)
    window_sum = jnp.zeros((length, POOL_W), jnp.float32)
    for lag_rows in range(WMAX):
        lagged = padded[WMAX - 1 - lag_rows:WMAX - 1 - lag_rows + length]
        window_sum = window_sum + jnp.where(lag_rows < window_len[None, :], lagged, jnp.float32(0.0))
    position = jnp.arange(1, length + 1).astype(jnp.float32)
    counts = jnp.minimum(position[:, None], window_len.astype(jnp.float32)[None, :])
    pool_diff = (window_sum / counts - data).astype(jnp.bfloat16)
    grouped = pool_diff.reshape(length, 4, GROUP_CH).astype(jnp.float32)
    mixed = jnp.einsum('tgc,gcd->tgd', grouped, pool_mix.astype(jnp.float32))
    return (mixed.reshape(length, POOL_W) * pool_scale).astype(jnp.bfloat16)

def recurrent_branch(queries, forget_in, value_in, gate_in, lower_bound, extra_decay, rec_gain):
    length = queries.shape[0]
    blocks = length // BLOCK_ROWS
    forget = lower_bound + (1.0 - lower_bound) * jax.nn.sigmoid(forget_in.astype(jnp.float32))
    log_keep = jnp.log(forget).reshape(length, HEADS, DK) + extra_decay[:, :, None]
    weight_in = (1.0 - forget).reshape(length, HEADS, DK)
    gated_query = jax.nn.silu(queries.astype(jnp.float32)).reshape(length, HEADS, DK)
    values = value_in.reshape(length, HEADS, DK)

    def to_blocks(arr):
        return arr.reshape(blocks, BLOCK_ROWS, HEADS, DK)
    lower_mask = jnp.tril(jnp.ones((BLOCK_ROWS, BLOCK_ROWS), jnp.float32))

    def block_step(state, inputs):
        query_blk, keep_blk, input_blk, value_blk = inputs
        value_wide = value_blk.astype(jnp.float32)
        log_total = jnp.cumsum(keep_blk, axis=0)
        query_up = query_blk * jnp.exp(log_total)
        input_down = input_blk * jnp.exp(-log_total)
        scores = jnp.einsum('thd,shd->hts', query_up, input_down, precision=HIGHEST) * lower_mask[None]
        scores = scores.astype(jnp.bfloat16).astype(jnp.float32)
        inside = jnp.einsum('hts,she->the', scores, value_wide, precision=HIGHEST)
        carried = jnp.einsum('thd,hde->the', query_up, state, precision=HIGHEST)
        log_end = log_total[-1]
        in_weight = (input_blk * jnp.exp(log_end[None] - log_total)).astype(jnp.bfloat16).astype(jnp.float32)
        new_state = jnp.exp(log_end)[:, :, None] * state + jnp.einsum('shd,she->hde', in_weight, value_wide, precision=HIGHEST)
        return (new_state, inside + carried)
    start_state = jnp.zeros((HEADS, DK, DK), jnp.float32)
    _, outputs = lax.scan(block_step, start_state, (to_blocks(gated_query), to_blocks(log_keep), to_blocks(weight_in), to_blocks(values)))
    rec_raw = outputs.reshape(length, HEADS, DK)
    rec_norm = rec_raw * lax.rsqrt(lax.optimization_barrier(jnp.mean(rec_raw * rec_raw, axis=-1, keepdims=True)) + EPS_RMS) * rec_gain
    gated = rec_norm * jax.nn.silu(gate_in.astype(jnp.float32)).reshape(length, HEADS, DK)
    return gated.reshape(length, REC_W).astype(jnp.bfloat16)

def reference(stream, w_pool_in, w_query, w_forget, w_value, w_outgate, pool_mix, pool_scale, lower_bound, extra_decay, rec_gain, w_out_pool, w_out_rec, norm_gain, norm_bias):
    features = stream[0]

    def project(weight):
        return jnp.dot(features, weight, preferred_element_type=jnp.float32).astype(jnp.bfloat16)
    pooled = project(w_pool_in)
    queries = project(w_query)
    forget_in = project(w_forget)
    value_in = project(w_value)
    gate_in = project(w_outgate)
    pool_out = pool_branch(pooled, pool_mix, pool_scale)
    rec_out = recurrent_branch(queries, forget_in, value_in, gate_in, lower_bound, extra_decay, rec_gain)
    mix = jnp.dot(pool_out, w_out_pool, preferred_element_type=jnp.float32) + jnp.dot(rec_out, w_out_rec, preferred_element_type=jnp.float32)
    resid = ALPHA * features.astype(jnp.float32) + mix
    row_mean = lax.optimization_barrier(jnp.mean(resid, axis=-1, keepdims=True))
    row_var = lax.optimization_barrier(jnp.mean((resid - row_mean) * (resid - row_mean), axis=-1, keepdims=True))
    normed = (resid - row_mean) * lax.rsqrt(row_var + EPS_NORM) * norm_gain + norm_bias
    return normed.astype(jnp.bfloat16)[None]
```

```python
import functools

import jax
import jax.numpy as jnp
from jax import lax
from jax.experimental import pallas as pl
from jax.experimental.pallas import tpu as pltpu
from jax.sharding import PartitionSpec as P

DK = 128
BLOCK_ROWS = 128
GROUP_CH = 256
HALO = 16
LANES = 128

ALPHA = 2.0**0.25
EPS_RMS = 1e-06
EPS_NORM = 1e-05
F32 = jnp.float32
BF16 = jnp.bfloat16
NT = (((1,), (1,)), ((), ()))
TN = (((0,), (0,)), ((), ()))


def dot(a, b, dims=None):
    if dims is None:
        return jnp.dot(a, b, preferred_element_type=F32)
    return lax.dot_general(a, b, dims, preferred_element_type=F32)


def half_sigmoid(x):
    return 0.5 + 0.5 * jnp.tanh(0.5 * x)


def mixer(
    n_sp, n_tp, rows_x,
    stream, w_pool, w_query, w_forget, w_value, w_gate,
    mix_in, scale_in, bound_in, extra_in, gain_in, wo_pool, wo_rec,
    out, stats,
    x_buf, w_buf, wo_buf, a_buf, v_buf, u_buf, e_buf, t_buf, p_buf, q_buf, g_buf, r_buf,
    o_buf, half_buf, state, mine_out, row_in, total_out, total_in, start_out, start_in, halo_in, stat_own, stat_peer, stat_sum,
    mix, scale, bound, extra, gain,
    x_loc, x_send, x_recv, w_sem, wo_loc, wo_send, wo_recv, a_send, a_recv,
    m_send, m_recv, r_send, r_recv, b_send, b_recv, h_send, h_recv, s_send, s_recv, o_sem, t_sem, small_sem,
):
    sp, tp = lax.axis_index("sp"), lax.axis_index("tp")
    peer = 1 - tp
    length, feats = stream.shape[1], stream.shape[2]
    chans = bound.shape[1]
    heads = chans // DK
    pool_w = scale.shape[1]
    groups = mix.shape[0]
    chunks = length // rows_x
    blocks = length // BLOCK_ROWS
    per = rows_x // BLOCK_ROWS
    row_n = heads
    col_n = n_sp // row_n
    x_at, z_at = lax.rem(sp, row_n), lax.div(sp, row_n)
    row0 = z_at * row_n

    def x_in(c):
        rows = pl.ds(c * rows_x, rows_x)
        return pltpu.make_async_copy(stream.at[0, rows], x_buf.at[tp, rows], x_loc.at[c])

    def x_out(c):
        rows = pl.ds(c * rows_x, rows_x)
        return pltpu.make_async_remote_copy(
            x_buf.at[tp, rows], x_buf.at[tp, rows], x_send.at[c], x_recv.at[c],
            device_id={"tp": peer}, device_id_type=pl.DeviceIdType.MESH)

    def w_in(i):
        src = (w_forget, w_value, w_pool, w_query, w_gate)[i]
        return [
            pltpu.make_async_copy(src.at[pl.ds(k * feats, feats)], w_buf.at[i, k], w_sem.at[i, k])
            for k in range(n_tp)
        ]

    my_cols = pl.ds(pl.multiple_of(tp * feats, LANES), feats)
    peer_cols = pl.ds(pl.multiple_of(peer * feats, LANES), feats)
    wo_places = ((wo_pool, pl.ds(0, pool_w)), (wo_rec, pl.ds(pool_w, chans)))

    def wo_in(i):
        src, place = wo_places[i]
        return pltpu.make_async_copy(src.at[:, my_cols], wo_buf.at[tp, place], wo_loc.at[i])

    def wo_out(i):
        src, place = wo_places[i]
        return pltpu.make_async_remote_copy(
            src.at[:, peer_cols], wo_buf.at[tp, place], wo_send.at[i], wo_recv.at[i],
            device_id={"tp": peer}, device_id_type=pl.DeviceIdType.MESH)

    def a_out(i, c):
        rows, cols = pl.ds(c * rows_x, rows_x), wo_places[i][1]
        return pltpu.make_async_remote_copy(
            a_buf.at[tp, rows, cols], a_buf.at[tp, rows, cols], a_send.at[i, c], a_recv.at[i, c],
            device_id={"tp": peer}, device_id_type=pl.DeviceIdType.MESH)

    def mine_to(k, slot):
        return pltpu.make_async_remote_copy(
            mine_out.at[k], row_in.at[slot], m_send.at[k], m_recv.at[slot],
            device_id={"sp": row0 + k}, device_id_type=pl.DeviceIdType.MESH)

    def total_to(k, slot):
        return pltpu.make_async_remote_copy(
            total_out, total_in.at[slot], r_send.at[k], r_recv.at[slot],
            device_id={"sp": k * row_n + x_at}, device_id_type=pl.DeviceIdType.MESH)

    def start_to(k, slot):
        return pltpu.make_async_remote_copy(
            start_out.at[k], start_in.at[slot], b_send.at[k], b_recv.at[slot],
            device_id={"sp": row0 + k}, device_id_type=pl.DeviceIdType.MESH)

    def greet(k):
        pl.semaphore_signal(
            barrier, inc=1, device_id={"sp": k}, device_id_type=pl.DeviceIdType.MESH)

    def each(low, high, do):
        def step(k, _):
            do(k)
            return 0

        lax.fori_loop(low, high, step, 0)

    def h_out(k):
        return pltpu.make_async_remote_copy(
            p_buf.at[pl.ds(BLOCK_ROWS + length - HALO, HALO)], halo_in, h_send, h_recv,
            device_id={"sp": k}, device_id_type=pl.DeviceIdType.MESH)

    def s_out(c):
        return pltpu.make_async_remote_copy(
            stat_own.at[c], stat_peer.at[c], s_send.at[c], s_recv.at[c],
            device_id={"tp": peer}, device_id_type=pl.DeviceIdType.MESH)

    def o_out(c):
        rows = pl.ds(c * rows_x, rows_x)
        return pltpu.make_async_copy(o_buf.at[rows], out.at[rows], o_sem.at[c])

    def t_out(c):
        rows = pl.ds(c * rows_x, rows_x)
        return pltpu.make_async_copy(stat_sum.at[c], stats.at[rows], t_sem.at[c])

    smalls = [
        pltpu.make_async_copy(src, dst, small_sem.at[i])
        for i, (src, dst) in enumerate(
            ((bound_in, bound), (extra_in, extra), (mix_in, mix), (scale_in, scale), (gain_in, gain)))
    ]

    for c in range(chunks):
        x_in(c).start()
        if c == 0:
            for i in (0, 1):
                for copy in w_in(i):
                    copy.start()
            for copy in smalls:
                copy.start()

    barrier = pltpu.get_barrier_semaphore()
    pl.semaphore_signal(barrier, inc=1, device_id={"tp": peer}, device_id_type=pl.DeviceIdType.MESH)
    p_buf[pl.ds(0, BLOCK_ROWS), :] = jnp.zeros((BLOCK_ROWS, pool_w), BF16)
    state[...] = jnp.zeros_like(state)
    with jax.named_scope("entry"):
        pl.semaphore_wait(barrier, 1 + x_at + z_at)
    for step in range(1, row_n):
        greet(row0 + lax.rem(x_at + step, row_n))
    for step in range(1, col_n):
        greet(lax.rem(z_at + step, col_n) * row_n + x_at)
    leads = (x_at == 0) & (z_at > 0)
    ends = (x_at == row_n - 1) & (z_at < col_n - 1)
    later = (row_n - 1 - x_at) + (col_n - 1 - z_at) + jnp.where(ends, 1, 0)

    for c in range(chunks):
        x_in(c).wait()
        x_out(c).start()

    row_ids = lax.broadcasted_iota(jnp.int32, (BLOCK_ROWS, BLOCK_ROWS), 0)
    col_ids = lax.broadcasted_iota(jnp.int32, (BLOCK_ROWS, BLOCK_ROWS), 1)
    lower = row_ids >= col_ids
    tri = jnp.where(lower, 1.0, 0.0).astype(BF16)
    lower_twice = jnp.concatenate([row_ids, row_ids], axis=1) >= jnp.concatenate([col_ids, col_ids], axis=1)
    tri_twice = jnp.concatenate([tri, tri], axis=1)
    ones = jnp.ones((2 * BLOCK_ROWS, DK), BF16)

    for i in (0, 1):
        for copy in w_in(i):
            copy.wait()
    for copy in smalls:
        copy.wait()
    for i in (2, 3, 4):
        for copy in w_in(i):
            copy.start()
    for i in range(2):
        wo_in(i).start()
        wo_out(i).start()

    def first(c, _):
        @pl.when((c == 1) & leads)
        def _():
            with jax.named_scope("lead"):
                pl.semaphore_wait(barrier, later)
            greet(sp - 1)

        rows = pl.ds(pl.multiple_of(c * rows_x, rows_x), rows_x)
        own = x_buf[tp, rows]
        f_own = dot(own, w_buf[0, tp])
        v_own = dot(own, w_buf[1, tp])
        x_out(c).wait_recv()
        other = x_buf[peer, rows]
        f_in = (f_own + dot(other, w_buf[0, peer])).astype(BF16).astype(F32)
        vals = (v_own + dot(other, w_buf[1, peer])).astype(BF16)
        v_buf[rows, :] = vals
        open_part = 1.0 - bound[...]
        for j in range(per):
            part = slice(j * BLOCK_ROWS, (j + 1) * BLOCK_ROWS)
            b = c * per + j
            brows = pl.ds(pl.multiple_of(b * BLOCK_ROWS, BLOCK_ROWS), BLOCK_ROWS)
            weight = open_part * (0.5 - 0.5 * jnp.tanh(0.5 * f_in[part]))
            keep = jnp.log(1.0 - weight)
            high = keep.astype(BF16)
            low = (keep - high.astype(F32)).astype(BF16)
            drop = extra[:, brows]
            drop_high = drop.astype(BF16).astype(F32)
            drop_low = drop - drop_high
            drops = []
            for h in range(heads):
                pair = jnp.concatenate([drop_high[h:h + 1], drop_low[h:h + 1]], axis=1)
                wide = jnp.where(lower_twice, jnp.broadcast_to(pair, (BLOCK_ROWS, 2 * BLOCK_ROWS)), 0.0)
                drops.append(dot(wide.astype(BF16), ones))
            total = dot(tri_twice, jnp.concatenate([high, low], axis=0)) + jnp.concatenate(drops, axis=1)
            middle = 0.5 * total[BLOCK_ROWS - 1:BLOCK_ROWS]
            e_buf[brows, :] = jnp.exp(total - middle)
            down = (weight * jnp.exp(middle - total)).astype(BF16)
            u_buf[brows, :] = down
            half = jnp.exp(middle)
            half_buf[b] = jnp.broadcast_to(half, (8, chans))
            for h in range(heads):
                lanes = slice(h * DK, (h + 1) * DK)
                hh = half[:, lanes]
                term = dot(vals[part, lanes], down[:, lanes], TN) * hh
                t_buf[b, :, lanes] = term
                state[:, lanes] = hh * hh * state[:, lanes] + term
        return 0

    with jax.named_scope("L_first"):
        lax.fori_loop(0, chunks, first, 0)

    for copy in w_in(2):
        copy.wait()

    def second(c, _):
        start = c * rows_x if isinstance(c, int) else pl.multiple_of(c * rows_x, rows_x)
        rows = pl.ds(start, rows_x)
        pooled = dot(x_buf[tp, rows], w_buf[2, tp]) + dot(x_buf[peer, rows], w_buf[2, peer])
        p_buf[pl.ds(start + BLOCK_ROWS, rows_x), :] = pooled.astype(BF16)
        return 0

    second(chunks - 1, 0)

    @pl.when(jnp.logical_not(leads) & (sp + 1 < n_sp))
    def _():
        with jax.named_scope("later"):
            pl.semaphore_wait(barrier, later)

    @pl.when(sp + 1 < n_sp)
    def _():
        h_out(sp + 1).start()

    log_half = half_buf[0, 0:1]
    for b in range(1, blocks):
        log_half = log_half * half_buf[b, 0:1]
    keep_all = jnp.broadcast_to(log_half * log_half, (HALO, chans)).astype(BF16)
    for h in range(heads):
        lanes = slice(h * DK, (h + 1) * DK)
        mine_out[h, pl.ds(0, DK), :] = state[:, lanes].astype(BF16)
        mine_out[h, pl.ds(DK, HALO), :] = keep_all[:, lanes]
    for step in range(1, row_n):
        mine_to(lax.rem(x_at + step, row_n), x_at).start()
    row_in[x_at] = mine_out[x_at]

    with jax.named_scope("L_second"):
        lax.fori_loop(0, chunks - 1, second, 0)

    for i in (3, 4):
        for copy in w_in(i):
            copy.wait()

    wide_rows = lax.broadcasted_iota(jnp.int32, (BLOCK_ROWS, 2 * BLOCK_ROWS), 0) + BLOCK_ROWS
    wide_cols = lax.broadcasted_iota(jnp.int32, (BLOCK_ROWS, 2 * BLOCK_ROWS), 1)
    back = wide_rows - wide_cols
    count = lax.broadcasted_iota(jnp.int32, (BLOCK_ROWS, LANES), 0) + (sp * length + 1)

    def part_of(ref, at):
        return ref[at, pl.ds(0, DK), :].astype(F32), ref[at, pl.ds(DK, HALO), :].astype(F32)[0:1]

    def fold_row():
        for step in range(1, row_n):
            with jax.named_scope("row_recv"):
                mine_to(x_at, lax.rem(x_at + step, row_n)).wait_recv()
        total, kept = part_of(row_in, 0)
        for k in range(1, row_n):
            term, keep = part_of(row_in, k)
            total = keep * total + term
            kept = kept * keep
        total_out[pl.ds(0, DK), :] = total.astype(BF16)
        total_out[pl.ds(DK, HALO), :] = jnp.broadcast_to(kept, (HALO, DK)).astype(BF16)
        each(z_at + 1, col_n, lambda k: total_to(k, z_at).start())

    def fold_column():
        state[:, pl.ds(0, DK)] = jnp.zeros((DK, DK), F32)

        def take(k):
            with jax.named_scope("col_recv"):
                total_to(z_at, k).wait_recv()
            term, keep = part_of(total_in, k)
            state[:, pl.ds(0, DK)] = keep * state[:, pl.ds(0, DK)] + term

        each(0, z_at, take)
        total = state[:, pl.ds(0, DK)]
        for k in range(row_n):
            start_out[k] = total.astype(BF16)
            if k + 1 < row_n:
                term, keep = part_of(row_in, k)
                total = keep * total + term
        for step in range(1, row_n):
            k = lax.rem(x_at + step, row_n)

            @pl.when(row0 + k > 0)
            def _():
                start_to(k, x_at).start()

        start_in[x_at] = start_out[x_at]

    def third(step, _):
        c = chunks - 1 - step

        @pl.when(step == 1)
        def _():
            fold_row()

        @pl.when(step == chunks - 1)
        def _():
            fold_column()

        @pl.when((step == chunks - 1) & (sp > 0))
        def _():
            with jax.named_scope("halo_recv"):
                h_out(sp).wait_recv()
            p_buf[pl.ds(BLOCK_ROWS - HALO, HALO), :] = halo_in[...]

        rows = pl.ds(pl.multiple_of(c * rows_x, rows_x), rows_x)
        own, other = x_buf[tp, rows], x_buf[peer, rows]
        q_in = (dot(own, w_buf[3, tp]) + dot(other, w_buf[3, peer])).astype(BF16).astype(F32)
        ups = (q_in * half_sigmoid(q_in) * e_buf[rows, :]).astype(BF16)
        q_buf[rows, :] = ups
        g_in = dot(own, w_buf[4, tp]) + dot(other, w_buf[4, peer])
        g_buf[rows, :] = g_in.astype(BF16)
        for k in range(per):
            start = pl.multiple_of(c * rows_x + k * BLOCK_ROWS, BLOCK_ROWS)
            brows = pl.ds(start, BLOCK_ROWS)
            near = p_buf[pl.ds(start, 2 * BLOCK_ROWS), :]
            for j in range(groups):
                lanes = slice(j * GROUP_CH, (j + 1) * GROUP_CH)
                window = jnp.left_shift(jnp.int32(2), tp * groups + j)
                band = jnp.where((back >= 0) & (back < window), 1.0, 0.0).astype(BF16)
                share = 1.0 / jnp.minimum(count + start, window).astype(F32)
                share = jnp.concatenate([share] * (GROUP_CH // LANES), axis=1)
                sums = dot(band, near[:, lanes])
                diff = (sums * share - near[BLOCK_ROWS:, lanes].astype(F32)).astype(BF16)
                a_buf[tp, brows, lanes] = (dot(diff, mix[j]) * scale[:, lanes]).astype(BF16)
            for h in range(heads):
                lanes = slice(h * DK, (h + 1) * DK)
                up = ups[k * BLOCK_ROWS:(k + 1) * BLOCK_ROWS, lanes]
                scores = jnp.where(lower, dot(up, u_buf[brows, lanes], NT), 0.0).astype(BF16)
                e_buf[brows, lanes] = dot(scores, v_buf[brows, lanes])
        a_out(0, c).start()
        return 0

    with jax.named_scope("L_third"):
        lax.fori_loop(0, chunks, third, 0)

    for i in range(2):
        wo_in(i).wait()
        wo_out(i).wait_recv()

    pool_at, rec_at = wo_places[0][1], wo_places[1][1]

    def pool_part(step, _):
        c = chunks - 1 - step
        rows = pl.ds(pl.multiple_of(c * rows_x, rows_x), rows_x)
        mine = dot(a_buf[tp, rows, pool_at], wo_buf[tp, pool_at]) + ALPHA * x_buf[tp, rows].astype(F32)
        a_out(0, c).wait_recv()
        r_buf[rows, :] = mine + dot(a_buf[peer, rows, pool_at], wo_buf[peer, pool_at])
        return 0

    with jax.named_scope("L_pool_part"):
        lax.fori_loop(0, chunks, pool_part, 0)

    for step in range(1, row_n):
        k = lax.rem(x_at + step, row_n)

        @pl.when(sp > 0)
        def _():
            with jax.named_scope("start_recv"):
                start_to(x_at, k).wait_recv()

    @pl.when(sp > 0)
    def _():
        for h in range(heads):
            state[:, h * DK:(h + 1) * DK] = start_in[h].astype(F32)

    @pl.when(sp == 0)
    def _():
        state[...] = jnp.zeros_like(state)

    def fourth(c, _):
        for k in range(per):
            b = c * per + k
            rows = pl.ds(pl.multiple_of(b * BLOCK_ROWS, BLOCK_ROWS), BLOCK_ROWS)
            half = half_buf[b, 0:1]
            before = state[...] * half
            carried = before.astype(BF16)
            state[...] = before * half + t_buf[b]
            for h in range(heads):
                lanes = slice(h * DK, (h + 1) * DK)
                raw = e_buf[rows, lanes] + dot(q_buf[rows, lanes], carried[:, lanes], NT)
                power = jnp.mean(raw * raw, axis=-1, keepdims=True)
                gate = g_buf[rows, lanes].astype(F32)
                rec = raw * lax.rsqrt(power + EPS_RMS) * gain[...] * (gate * half_sigmoid(gate))
                a_buf[tp, rows, pool_w + h * DK:pool_w + (h + 1) * DK] = rec.astype(BF16)
        a_out(1, c).start()
        return 0

    with jax.named_scope("L_fourth"):
        lax.fori_loop(0, chunks, fourth, 0)

    def fold(x):
        acc = x[:, :LANES]
        for k in range(1, feats // LANES):
            acc = acc + x[:, k * LANES:(k + 1) * LANES]
        return acc

    first_half = lax.broadcasted_iota(jnp.int32, (rows_x, LANES), 1) < LANES // 2

    def fifth(c, _):
        rows = pl.ds(pl.multiple_of(c * rows_x, rows_x), rows_x)
        mine = r_buf[rows, :] + dot(a_buf[tp, rows, rec_at], wo_buf[tp, rec_at])
        a_out(1, c).wait_recv()
        resid = mine + dot(a_buf[peer, rows, rec_at], wo_buf[peer, rec_at])
        o_buf[rows, :] = resid.astype(BF16)
        sums, squares = fold(resid), fold(resid * resid)
        sums = sums + pltpu.roll(sums, LANES // 2, 1)
        squares = squares + pltpu.roll(squares, LANES // 2, 1)
        stat_own[c] = jnp.where(first_half, sums, squares)
        s_out(c).start()
        o_out(c).start()
        return 0

    with jax.named_scope("L_fifth"):
        lax.fori_loop(0, chunks, fifth, 0)

    for c in range(chunks):
        s_out(c).wait_recv()
        stat_sum[c] = stat_own[c] + stat_peer[c]
        t_out(c).start()

    for c in range(chunks):
        x_out(c).wait_send()
        s_out(c).wait_send()
        o_out(c).wait()
        t_out(c).wait()
        for i in range(2):
            a_out(i, c).wait_send()
    for i in range(2):
        wo_out(i).wait_send()

    for step in range(1, row_n):
        k = lax.rem(x_at + step, row_n)
        mine_to(k, x_at).wait_send()

        @pl.when(row0 + k > 0)
        def _():
            start_to(k, x_at).wait_send()

    each(z_at + 1, col_n, lambda k: total_to(k, z_at).wait_send())

    @pl.when(sp + 1 < n_sp)
    def _():
        h_out(sp + 1).wait_send()


def finish(width, rows, resid, stats, norm_gain, norm_bias, out,
           r_buf, s_buf, o_buf, gain, bias, r_sem, s_sem, o_sem, n_sem):
    pieces = resid.shape[0] // rows

    def copies(c):
        part = pl.ds(c * rows, rows)
        return (
            pltpu.make_async_copy(stats.at[part], s_buf.at[part], s_sem.at[c]),
            pltpu.make_async_copy(resid.at[part], r_buf.at[part], r_sem.at[c]),
            pltpu.make_async_copy(o_buf.at[part], out.at[0, part], o_sem.at[c]),
        )

    norms = (
        pltpu.make_async_copy(norm_gain, gain, n_sem.at[0]),
        pltpu.make_async_copy(norm_bias, bias, n_sem.at[1]),
    )
    for copy in norms:
        copy.start()
    for c in range(pieces):
        for copy in copies(c)[:2]:
            copy.start()
    for copy in norms:
        copy.wait()
    first_half = lax.broadcasted_iota(jnp.int32, (rows, LANES), 1) < LANES // 2
    for c in range(pieces):
        part = pl.ds(c * rows, rows)
        for copy in copies(c)[:2]:
            copy.wait()
        both = s_buf[part, :]
        mean = jnp.sum(jnp.where(first_half, both, 0.0), axis=1, keepdims=True) / width
        square = jnp.sum(jnp.where(first_half, 0.0, both), axis=1, keepdims=True) / width
        inv = lax.rsqrt(square - mean * mean + EPS_NORM)
        o_buf[part, :] = ((r_buf[part, :].astype(F32) - mean) * inv * gain[...] + bias[...]).astype(BF16)
        copies(c)[2].start()
    for c in range(pieces):
        copies(c)[2].wait()


def solution(mesh):
    n_sp, n_tp = mesh.shape["sp"], mesh.shape["tp"]

    def local(stream, w_pool, w_query, w_forget, w_value, w_gate, mix, scale, bound, extra,
              gain, wo_pool, wo_rec, norm_gain, norm_bias):
        length, feats = stream.shape[1], stream.shape[2]
        chans, pool_w = bound.shape[0], scale.shape[0]
        heads = chans // DK
        blocks = length // BLOCK_ROWS
        rows_x = 256
        chunks = length // rows_x
        hbm = pl.BlockSpec(memory_space=pl.ANY)
        dma = pltpu.SemaphoreType.DMA
        scratch = [
            pltpu.VMEM((n_tp, length, feats), BF16),
            pltpu.VMEM((5, n_tp, feats, chans), BF16),
            pltpu.VMEM((n_tp, pool_w + chans, feats), BF16),
            pltpu.VMEM((n_tp, length, pool_w + chans), BF16),
            pltpu.VMEM((length, chans), BF16),
            pltpu.VMEM((length, chans), BF16),
            pltpu.VMEM((length, chans), F32),
            pltpu.VMEM((blocks, DK, chans), F32),
            pltpu.VMEM((BLOCK_ROWS + length, pool_w), BF16),
            pltpu.VMEM((length, chans), BF16),
            pltpu.VMEM((length, chans), BF16),
            pltpu.VMEM((length, feats), F32),
            pltpu.VMEM((length, feats), BF16),
            pltpu.VMEM((blocks, 8, chans), F32),
            pltpu.VMEM((DK, chans), F32),
            pltpu.VMEM((heads, DK + HALO, DK), BF16),
            pltpu.VMEM((heads, DK + HALO, DK), BF16),
            pltpu.VMEM((DK + HALO, DK), BF16),
            pltpu.VMEM((n_sp // heads, DK + HALO, DK), BF16),
            pltpu.VMEM((heads, DK, DK), BF16),
            pltpu.VMEM((heads, DK, DK), BF16),
            pltpu.VMEM((HALO, pool_w), BF16),
            pltpu.VMEM((chunks, rows_x, LANES), F32),
            pltpu.VMEM((chunks, rows_x, LANES), F32),
            pltpu.VMEM((chunks, rows_x, LANES), F32),
            pltpu.VMEM(mix.shape, BF16),
            pltpu.VMEM((1, pool_w), F32),
            pltpu.VMEM((1, chans), F32),
            pltpu.VMEM((chans // DK, length), F32),
            pltpu.VMEM((1, DK), F32),
            dma((chunks,)), dma((chunks,)), dma((chunks,)), dma((5, n_tp)),
            dma((2,)), dma((2,)), dma((2,)), dma((2, chunks)), dma((2, chunks)),
            dma((heads,)), dma((heads,)), dma((n_sp // heads,)), dma((n_sp // heads,)),
            dma((heads,)), dma((heads,)), dma, dma, dma((chunks,)), dma((chunks,)), dma((chunks,)),
            dma((chunks,)), dma((5,)),
        ]
        row = lambda x: x.reshape(1, -1)
        resid, stats = pl.pallas_call(
            functools.partial(mixer, n_sp, n_tp, rows_x),
            out_shape=(
                jax.ShapeDtypeStruct((length, feats), BF16), jax.ShapeDtypeStruct((length, LANES), F32)),
            in_specs=[hbm] * 13,
            out_specs=(hbm, hbm),
            scratch_shapes=scratch,
            compiler_params=pltpu.CompilerParams(
                collective_id=0, has_side_effects=True, vmem_limit_bytes=60 * 1024 * 1024),
            name="mixer",
        )(stream, w_pool, w_query, w_forget, w_value, w_gate, mix, row(scale), row(bound), extra.T,
          row(gain), wo_pool, wo_rec)
        piece = 128
        pieces = length // piece
        return pl.pallas_call(
            functools.partial(finish, n_tp * feats, piece),
            out_shape=jax.ShapeDtypeStruct(stream.shape, BF16),
            in_specs=[hbm] * 4,
            out_specs=hbm,
            scratch_shapes=[
                pltpu.VMEM((length, feats), BF16),
                pltpu.VMEM((length, LANES), F32),
                pltpu.VMEM((length, feats), BF16),
                pltpu.VMEM((1, feats), F32),
                pltpu.VMEM((1, feats), F32),
                dma((pieces,)), dma((pieces,)), dma((pieces,)), dma((2,)),
            ],
            compiler_params=pltpu.CompilerParams(vmem_limit_bytes=60 * 1024 * 1024),
            name="finish",
        )(resid, stats, row(norm_gain), row(norm_bias))

    placed = (
        P("fs", "sp", "tp"), P(None, "tp"), P(None, "tp"), P(None, "tp"), P(None, "tp"),
        P(None, "tp"), P("tp", None, None), P("tp"), P("tp"), P("sp", "tp"), P(),
        P("tp", None), P("tp", None), P("tp"), P("tp"),
    )
    return jax.shard_map(
        local, mesh=mesh, in_specs=placed, out_specs=P("fs", "sp", "tp"), check_vma=False
    )
```

```python
import functools

import jax
import jax.numpy as jnp
from jax import lax
from jax.experimental import pallas as pl
from jax.experimental.pallas import tpu as pltpu
from jax.sharding import PartitionSpec as P

DK = 128
BLOCK_ROWS = 128
GROUP_CH = 256
HALO = 16
LANES = 128

LIMIT = 56 * 1024 * 1024
ALPHA = 2.0**0.25
EPS_RMS = 1e-06
EPS_NORM = 1e-05
F32 = jnp.float32
BF16 = jnp.bfloat16
NT = (((1,), (1,)), ((), ()))
TN = (((0,), (0,)), ((), ()))
OWN, PEER = 0, 1


def dot(a, b, dims=None):
    if dims is None:
        return jnp.dot(a, b, preferred_element_type=F32)
    return lax.dot_general(a, b, dims, preferred_element_type=F32)


def half_sigmoid(x):
    return 0.5 + 0.5 * jnp.tanh(0.5 * x)


def mixer(
    n_sp, n_tp, rows_x,
    stream, w_pool, w_query, w_forget, w_value, w_gate,
    mix_in, scale_in, bound_in, extra_in, gain_in, wo_pool, wo_rec,
    r_buf, stats,
    x_buf, w_buf, wo_buf, a_buf, v_buf, u_buf, e_buf, t_buf, p_buf, q_buf, g_buf, f_buf,
    half_buf, state, mine_out, row_in, total_out, total_in, start_out, start_in, halo_in,
    stat_own, stat_peer, bands,
    mix, scale, bound, extra, gain,
    x_loc, x_send, x_recv, w_sem, wo_loc, wo_send, wo_recv, a_send, a_recv,
    m_send, m_recv, r_send, r_recv, b_send, b_recv, h_send, h_recv, s_send, s_recv, small_sem,
):
    sp, tp = lax.axis_index("sp"), lax.axis_index("tp")
    peer = 1 - tp
    length, feats = stream.shape[1], stream.shape[2]
    chans = bound.shape[1]
    heads = chans // DK
    pool_w = scale.shape[1]
    groups = mix.shape[0]
    chunks = length // rows_x
    blocks = length // BLOCK_ROWS
    per = rows_x // BLOCK_ROWS
    row_n = heads
    col_n = n_sp // row_n
    x_at, z_at = lax.rem(sp, row_n), lax.div(sp, row_n)
    row0 = z_at * row_n
    mesh_id = pl.DeviceIdType.MESH

    def rows_of(c):
        return slice(c * rows_x, (c + 1) * rows_x)

    def block_of(b):
        return slice(b * BLOCK_ROWS, (b + 1) * BLOCK_ROWS)

    def head_of(h):
        return slice(h * DK, (h + 1) * DK)

    def x_in(c):
        rows = pl.ds(c * rows_x, rows_x)
        return pltpu.make_async_copy(stream.at[0, rows], x_buf.at[OWN, rows], x_loc.at[c])

    def x_out(c):
        rows = pl.ds(c * rows_x, rows_x)
        return pltpu.make_async_remote_copy(
            x_buf.at[OWN, rows], x_buf.at[PEER, rows], x_send.at[c], x_recv.at[c],
            device_id={"tp": peer}, device_id_type=mesh_id)

    my_cols = pl.ds(pl.multiple_of(tp * feats, LANES), feats)
    peer_cols = pl.ds(pl.multiple_of(peer * feats, LANES), feats)
    wo_places = ((wo_pool, pl.ds(0, pool_w)), (wo_rec, pl.ds(pool_w, chans)))

    def w_in(i, side):
        src = (w_forget, w_value, w_pool, w_query, w_gate)[i]
        return pltpu.make_async_copy(
            src.at[my_cols if side == OWN else peer_cols], w_buf.at[i, side], w_sem.at[i, side])

    def wo_in(i):
        src, place = wo_places[i]
        return pltpu.make_async_copy(src.at[:, my_cols], wo_buf.at[OWN, place], wo_loc.at[i])

    def wo_out(i):
        src, place = wo_places[i]
        return pltpu.make_async_remote_copy(
            src.at[:, peer_cols], wo_buf.at[PEER, place], wo_send.at[i], wo_recv.at[i],
            device_id={"tp": peer}, device_id_type=mesh_id)

    def a_out(i, c):
        rows, cols = pl.ds(c * rows_x, rows_x), wo_places[i][1]
        return pltpu.make_async_remote_copy(
            a_buf.at[OWN, rows, cols], a_buf.at[PEER, rows, cols], a_send.at[i, c], a_recv.at[i, c],
            device_id={"tp": peer}, device_id_type=mesh_id)

    def mine_to(k, slot):
        return pltpu.make_async_remote_copy(
            mine_out.at[k], row_in.at[slot], m_send.at[k], m_recv.at[slot],
            device_id={"sp": row0 + k}, device_id_type=mesh_id)

    def total_to(k, slot):
        return pltpu.make_async_remote_copy(
            total_out, total_in.at[slot], r_send.at[k], r_recv.at[slot],
            device_id={"sp": k * row_n + x_at}, device_id_type=mesh_id)

    def start_to(k, slot):
        return pltpu.make_async_remote_copy(
            start_out.at[k], start_in.at[slot], b_send.at[k], b_recv.at[slot],
            device_id={"sp": row0 + k}, device_id_type=mesh_id)

    def h_out(k):
        return pltpu.make_async_remote_copy(
            p_buf.at[pl.ds(BLOCK_ROWS + length - HALO, HALO)], halo_in, h_send, h_recv,
            device_id={"sp": k}, device_id_type=mesh_id)

    def s_out(c):
        return pltpu.make_async_remote_copy(
            stat_own.at[c], stat_peer.at[c], s_send.at[c], s_recv.at[c],
            device_id={"tp": peer}, device_id_type=mesh_id)

    def greet(k):
        pl.semaphore_signal(barrier, inc=1, device_id={"sp": k}, device_id_type=mesh_id)

    def each(low, high, do):
        def step(k, _):
            do(k)
            return 0

        lax.fori_loop(low, high, step, 0)

    smalls = [
        pltpu.make_async_copy(src, dst, small_sem.at[i])
        for i, (src, dst) in enumerate(
            ((extra_in, extra), (bound_in, bound), (mix_in, mix), (scale_in, scale), (gain_in, gain)))
    ]

    smalls[0].start()
    x_in(0).start()
    w_in(0, OWN).start()
    w_in(1, OWN).start()
    for c in range(1, chunks):
        x_in(c).start()
    w_in(0, PEER).start()
    w_in(1, PEER).start()
    for copy in smalls[1:]:
        copy.start()

    barrier = pltpu.get_barrier_semaphore()
    pl.semaphore_signal(barrier, inc=1, device_id={"tp": peer}, device_id_type=mesh_id)
    p_buf[0:BLOCK_ROWS, :] = jnp.zeros((BLOCK_ROWS, pool_w), BF16)
    with jax.named_scope("entry"):
        pl.semaphore_wait(barrier, 1 + x_at + z_at)
    for step in range(1, row_n):
        greet(row0 + lax.rem(x_at + step, row_n))
    for step in range(1, col_n):
        greet(lax.rem(z_at + step, col_n) * row_n + x_at)
    leads = (x_at == 0) & (z_at > 0)
    ends = (x_at == row_n - 1) & (z_at < col_n - 1)
    later = (row_n - 1 - x_at) + (col_n - 1 - z_at) + jnp.where(ends, 1, 0)

    with jax.named_scope("x0"):
        x_in(0).wait()
        x_out(0).start()
        smalls[0].wait()

    row_ids = lax.broadcasted_iota(jnp.int32, (BLOCK_ROWS, BLOCK_ROWS), 0)
    col_ids = lax.broadcasted_iota(jnp.int32, (BLOCK_ROWS, BLOCK_ROWS), 1)
    lower = row_ids >= col_ids

    with jax.named_scope("drops"):
        lower_twice = jnp.concatenate([row_ids, row_ids], axis=1) >= jnp.concatenate([col_ids, col_ids], axis=1)
        ones = jnp.ones((2 * BLOCK_ROWS, DK), BF16)
        for b in range(blocks):
            drop = extra[:, block_of(b)]
            drop_high = drop.astype(BF16).astype(F32)
            drop_low = drop - drop_high
            for h in range(heads):
                pair = jnp.concatenate([drop_high[h:h + 1], drop_low[h:h + 1]], axis=1)
                wide = jnp.where(lower_twice, jnp.broadcast_to(pair, (BLOCK_ROWS, 2 * BLOCK_ROWS)), 0.0)
                e_buf[block_of(b), head_of(h)] = dot(wide.astype(BF16), ones)
        wide_rows = lax.broadcasted_iota(jnp.int32, (BLOCK_ROWS, 2 * BLOCK_ROWS), 0) + BLOCK_ROWS
        wide_cols = lax.broadcasted_iota(jnp.int32, (BLOCK_ROWS, 2 * BLOCK_ROWS), 1)
        back = wide_rows - wide_cols
        for j in range(groups):
            window = jnp.left_shift(jnp.int32(2), tp * groups + j)
            share = 1.0 / window.astype(F32)
            inside = (back >= 0) & (back < window)
            bands[j] = (jnp.where(inside, share, 0.0) - jnp.where(back == 0, 1.0, 0.0)).astype(BF16)
        state[...] = jnp.zeros_like(state)

    with jax.named_scope("x_rest"):
        for c in range(1, chunks):
            x_in(c).wait()
            x_out(c).start()
    with jax.named_scope("w01"):
        for i in (0, 1):
            w_in(i, OWN).wait()

    tri = jnp.where(lower, 1.0, 0.0).astype(BF16)
    tri_twice = jnp.concatenate([tri, tri], axis=1)

    def proj(i, c):
        rows = rows_of(c)
        return dot(x_buf[OWN, rows, :], w_buf[i, OWN]) + dot(x_buf[PEER, rows, :], w_buf[i, PEER])

    class Post:
        def __init__(self, c):
            self.blocks = [c * per + j for j in range(per)]
            self.weight, self.split, self.total = {}, {}, {}
            self.down, self.half = {}, {}

        def logs(self):
            open_part = 1.0 - bound[...]
            for b in self.blocks:
                f_in = f_buf[block_of(b), :].astype(F32)
                weight = open_part * (0.5 - 0.5 * jnp.tanh(0.5 * f_in))
                keep = jnp.log(1.0 - weight)
                high = keep.astype(BF16)
                low = (keep - high.astype(F32)).astype(BF16)
                self.weight[b], self.split[b] = weight, jnp.concatenate([high, low], axis=0)

        def sums(self):
            for b in self.blocks:
                self.total[b] = dot(tri_twice, self.split[b]) + e_buf[block_of(b), :]

        def exps(self):
            for b in self.blocks:
                total = self.total[b]
                middle = 0.5 * total[BLOCK_ROWS - 1:BLOCK_ROWS]
                e_buf[block_of(b), :] = jnp.exp(total - middle)
                down = (self.weight[b] * jnp.exp(middle - total)).astype(BF16)
                u_buf[block_of(b), :] = down
                half = jnp.exp(middle)
                half_buf[b] = jnp.broadcast_to(half, (8, chans))
                self.down[b], self.half[b] = down, half

        def states(self):
            for b in self.blocks:
                for h in range(heads):
                    lanes = head_of(h)
                    hh = self.half[b][:, lanes]
                    term = dot(v_buf[block_of(b), lanes], self.down[b][:, lanes], TN) * hh
                    t_buf[b, :, lanes] = term
                    state[:, lanes] = hh * hh * state[:, lanes] + term

    def put_pool(c):
        p_buf[BLOCK_ROWS + c * rows_x:BLOCK_ROWS + (c + 1) * rows_x, :] = proj(2, c).astype(BF16)

    with jax.named_scope("first0"):
        own = x_buf[OWN, rows_of(0), :]
        f_own = dot(own, w_buf[0, OWN])
        v_own = dot(own, w_buf[1, OWN])
        with jax.named_scope("x_recv0"):
            x_out(0).wait_recv()
            for i in (0, 1):
                w_in(i, PEER).wait()
            for copy in smalls[1:]:
                copy.wait()
        for i in (2, 3, 4):
            for side in (OWN, PEER):
                w_in(i, side).start()
        for i in range(2):
            wo_in(i).start()
            wo_out(i).start()
        other = x_buf[PEER, rows_of(0), :]
        f_buf[rows_of(0), :] = (f_own + dot(other, w_buf[0, PEER])).astype(BF16)
        v_buf[rows_of(0), :] = (v_own + dot(other, w_buf[1, PEER])).astype(BF16)

    for c in range(1, chunks):
        with jax.named_scope("first"):
            with jax.named_scope("x_recv"):
                x_out(c).wait_recv()
            if c == 2:
                @pl.when(leads)
                def _():
                    with jax.named_scope("lead"):
                        pl.semaphore_wait(barrier, later)
                    greet(sp - 1)
            post = Post(c - 1)
            post.logs()
            f_buf[rows_of(c), :] = proj(0, c).astype(BF16)
            post.sums()
            v_buf[rows_of(c), :] = proj(1, c).astype(BF16)
            post.exps()
            post.states()

    with jax.named_scope("w2"):
        for side in (OWN, PEER):
            w_in(2, side).wait()
    with jax.named_scope("second0"):
        post = Post(chunks - 1)
        post.logs()
        put_pool(chunks - 1)
        post.sums()
        put_pool(chunks - 2)
        post.exps()
        post.states()
        log_half = half_buf[0, 0:1]
        for b in range(1, blocks):
            log_half = log_half * half_buf[b, 0:1]
        keep_all = jnp.broadcast_to(log_half * log_half, (HALO, chans)).astype(BF16)
        for h in range(heads):
            mine_out[h, 0:DK, :] = state[:, head_of(h)].astype(BF16)
            mine_out[h, DK:DK + HALO, :] = keep_all[:, head_of(h)]

    @pl.when(jnp.logical_not(leads) & (sp + 1 < n_sp))
    def _():
        with jax.named_scope("later"):
            pl.semaphore_wait(barrier, later)

    for step in range(1, row_n):
        mine_to(lax.rem(x_at + step, row_n), x_at).start()
    row_in[x_at] = mine_out[x_at]

    @pl.when(sp + 1 < n_sp)
    def _():
        h_out(sp + 1).start()

    with jax.named_scope("second"):
        for c in range(chunks - 2):
            put_pool(c)

    with jax.named_scope("w34"):
        for i in (3, 4):
            for side in (OWN, PEER):
                w_in(i, side).wait()

    def part_of(ref, at):
        return ref[at, 0:DK, :].astype(F32), ref[at, DK:DK + HALO, :].astype(F32)[0:1]

    def fold_row():
        for step in range(1, row_n):
            with jax.named_scope("row_recv"):
                mine_to(x_at, lax.rem(x_at + step, row_n)).wait_recv()
        total, kept = part_of(row_in, 0)
        for k in range(1, row_n):
            term, keep = part_of(row_in, k)
            total = keep * total + term
            kept = kept * keep
        total_out[0:DK, :] = total.astype(BF16)
        total_out[DK:DK + HALO, :] = jnp.broadcast_to(kept, (HALO, DK)).astype(BF16)
        each(z_at + 1, col_n, lambda k: total_to(k, z_at).start())

    def fold_column():
        state[:, 0:DK] = jnp.zeros((DK, DK), F32)

        def take(k):
            with jax.named_scope("col_recv"):
                total_to(z_at, k).wait_recv()
            term, keep = part_of(total_in, k)
            state[:, 0:DK] = keep * state[:, 0:DK] + term

        each(0, z_at, take)
        total = state[:, 0:DK]
        for k in range(row_n):
            start_out[k] = total.astype(BF16)
            if k + 1 < row_n:
                term, keep = part_of(row_in, k)
                total = keep * total + term
        for step in range(1, row_n):
            k = lax.rem(x_at + step, row_n)

            @pl.when(row0 + k > 0)
            def _():
                start_to(k, x_at).start()

        start_in[x_at] = start_out[x_at]

    count = lax.broadcasted_iota(jnp.int32, (BLOCK_ROWS, LANES), 0) + (sp * length + 1)

    class Third:
        def __init__(self, c):
            self.c, self.rows = c, rows_of(c)
            self.blocks = [c * per + k for k in range(per)]
            self.diff, self.scores = {}, {}

        def query(self):
            q_in = proj(3, self.c).astype(BF16).astype(F32)
            q_buf[self.rows, :] = (q_in * half_sigmoid(q_in) * e_buf[self.rows, :]).astype(BF16)

        def band(self):
            for b in self.blocks:
                near = p_buf[b * BLOCK_ROWS:(b + 2) * BLOCK_ROWS, :]
                for j in range(groups):
                    lanes = slice(j * GROUP_CH, (j + 1) * GROUP_CH)
                    if b:
                        self.diff[b, j] = dot(bands[j], near[:, lanes]).astype(BF16)
                        continue
                    window = jnp.left_shift(jnp.int32(2), tp * groups + j)
                    inside = jnp.where((back >= 0) & (back < window), 1.0, 0.0).astype(BF16)
                    share = 1.0 / jnp.minimum(count, window).astype(F32)
                    share = jnp.concatenate([share] * (GROUP_CH // LANES), axis=1)
                    sums = dot(inside, near[:, lanes])
                    self.diff[b, j] = (sums * share - near[BLOCK_ROWS:, lanes].astype(F32)).astype(BF16)

        def gates(self):
            g_buf[self.rows, :] = proj(4, self.c).astype(BF16)

        def mixed(self):
            for b in self.blocks:
                for j in range(groups):
                    lanes = slice(j * GROUP_CH, (j + 1) * GROUP_CH)
                    a_buf[OWN, block_of(b), lanes] = (dot(self.diff[b, j], mix[j]) * scale[:, lanes]).astype(BF16)

        def score(self):
            for b in self.blocks:
                for h in range(heads):
                    up, down = q_buf[block_of(b), head_of(h)], u_buf[block_of(b), head_of(h)]
                    self.scores[b, h] = jnp.where(lower, dot(up, down, NT), 0.0).astype(BF16)

        def inner(self):
            for b in self.blocks:
                for h in range(heads):
                    e_buf[block_of(b), head_of(h)] = dot(self.scores[b, h], v_buf[block_of(b), head_of(h)])

    for c in reversed(range(chunks)):
        if c == 1:
            fold_row()
        if c == 0:
            fold_column()

            @pl.when(sp > 0)
            def _():
                with jax.named_scope("halo_recv"):
                    h_out(sp).wait_recv()
                p_buf[BLOCK_ROWS - HALO:BLOCK_ROWS, :] = halo_in[...]

        with jax.named_scope("third"):
            part = Third(c)
            part.query()
            part.band()
            part.gates()
            part.mixed()
            part.score()
            part.inner()
            a_out(0, c).start()

    with jax.named_scope("wo"):
        for i in range(2):
            wo_in(i).wait()
            wo_out(i).wait_recv()

    pool_at, rec_at = slice(0, pool_w), slice(pool_w, pool_w + chans)

    def pool_part(c):
        rows = rows_of(c)
        r_buf[rows, :] = (
            dot(a_buf[OWN, rows, pool_at], wo_buf[OWN, pool_at]) + dot(a_buf[PEER, rows, pool_at], wo_buf[PEER, pool_at])
            + ALPHA * x_buf[OWN, rows, :].astype(F32))

    with jax.named_scope("pool"):
        for c in reversed(range(2, chunks)):
            a_out(0, c).wait_recv()
        for c in reversed(range(2, chunks)):
            pool_part(c)

    for step in range(1, row_n):
        k = lax.rem(x_at + step, row_n)

        @pl.when(sp > 0)
        def _():
            with jax.named_scope("start_recv"):
                start_to(x_at, k).wait_recv()

    @pl.when(sp > 0)
    def _():
        for h in range(heads):
            state[:, head_of(h)] = start_in[h].astype(F32)

    @pl.when(sp == 0)
    def _():
        state[...] = jnp.zeros_like(state)

    def fourth(c):
        for k in range(per):
            b = c * per + k
            half = half_buf[b, 0:1]
            before = state[...] * half
            carried = before.astype(BF16)
            state[...] = before * half + t_buf[b]
            for h in range(heads):
                lanes = head_of(h)
                raw = e_buf[block_of(b), lanes] + dot(q_buf[block_of(b), lanes], carried[:, lanes], NT)
                power = jnp.mean(raw * raw, axis=-1, keepdims=True)
                gate = g_buf[block_of(b), lanes].astype(F32)
                rec = raw * lax.rsqrt(power + EPS_RMS) * gain[...] * (gate * half_sigmoid(gate))
                a_buf[OWN, block_of(b), pool_w + h * DK:pool_w + (h + 1) * DK] = rec.astype(BF16)

    for c in range(chunks):
        with jax.named_scope("fourth"):
            fourth(c)
            if c < 2:
                a_out(0, 1 - c).wait_recv()
                pool_part(1 - c)
            a_out(1, c).start()

    def fold(x):
        acc = x[:, :LANES]
        for k in range(1, feats // LANES):
            acc = acc + x[:, k * LANES:(k + 1) * LANES]
        return acc

    first_half = lax.broadcasted_iota(jnp.int32, (rows_x, LANES), 1) < LANES // 2

    for c in range(chunks):
        with jax.named_scope("fifth"):
            rows = rows_of(c)
            a_out(1, c).wait_recv()
            resid = r_buf[rows, :] + (
                dot(a_buf[OWN, rows, rec_at], wo_buf[OWN, rec_at]) + dot(a_buf[PEER, rows, rec_at], wo_buf[PEER, rec_at]))
            r_buf[rows, :] = resid
            sums, squares = fold(resid), fold(resid * resid)
            sums = sums + pltpu.roll(sums, LANES // 2, 1)
            squares = squares + pltpu.roll(squares, LANES // 2, 1)
            stat_own[c] = jnp.where(first_half, sums, squares)
            s_out(c).start()

    with jax.named_scope("tail"):
        for c in range(chunks):
            s_out(c).wait_recv()
            stats[rows_of(c), :] = stat_own[c] + stat_peer[c]

        for c in range(chunks):
            x_out(c).wait_send()
            s_out(c).wait_send()
            for i in range(2):
                a_out(i, c).wait_send()
        for i in range(2):
            wo_out(i).wait_send()
        for step in range(1, row_n):
            k = lax.rem(x_at + step, row_n)
            mine_to(k, x_at).wait_send()

            @pl.when(row0 + k > 0)
            def _():
                start_to(k, x_at).wait_send()

        each(z_at + 1, col_n, lambda k: total_to(k, z_at).wait_send())

        @pl.when(sp + 1 < n_sp)
        def _():
            h_out(sp + 1).wait_send()


def finish(width, rows, resid, stats, gain, bias, out, o_buf, o_sem):
    pieces = resid.shape[0] // rows

    def leave(c):
        part = pl.ds(c * rows, rows)
        return pltpu.make_async_copy(o_buf.at[part], out.at[0, part], o_sem.at[c])

    first_half = lax.broadcasted_iota(jnp.int32, (rows, LANES), 1) < LANES // 2
    for c in range(pieces):
        part = slice(c * rows, (c + 1) * rows)
        both = stats[part, :]
        mean = jnp.sum(jnp.where(first_half, both, 0.0), axis=1, keepdims=True) / width
        square = jnp.sum(jnp.where(first_half, 0.0, both), axis=1, keepdims=True) / width
        inv = lax.rsqrt(square - mean * mean + EPS_NORM)
        o_buf[part, :] = ((resid[part, :] - mean) * inv * gain[...] + bias[...]).astype(BF16)
        leave(c).start()
    for c in range(pieces):
        leave(c).wait()


def solution(mesh):
    n_sp, n_tp = mesh.shape["sp"], mesh.shape["tp"]

    def local(stream, w_pool, w_query, w_forget, w_value, w_gate, mix, scale, bound, extra,
              gain, wo_pool, wo_rec, norm_gain, norm_bias):
        length, feats = stream.shape[1], stream.shape[2]
        chans, pool_w = bound.shape[0], scale.shape[0]
        heads = chans // DK
        blocks = length // BLOCK_ROWS
        rows_x = 256
        chunks = length // rows_x
        hbm = pl.BlockSpec(memory_space=pl.ANY)
        vmem = pl.BlockSpec(memory_space=pltpu.VMEM)
        dma = pltpu.SemaphoreType.DMA
        scratch = [
            pltpu.VMEM((n_tp, length, feats), BF16),
            pltpu.VMEM((5, n_tp, feats, chans), BF16),
            pltpu.VMEM((n_tp, pool_w + chans, feats), BF16),
            pltpu.VMEM((n_tp, length, pool_w + chans), BF16),
            pltpu.VMEM((length, chans), BF16),
            pltpu.VMEM((length, chans), BF16),
            pltpu.VMEM((length, chans), F32),
            pltpu.VMEM((blocks, DK, chans), F32),
            pltpu.VMEM((BLOCK_ROWS + length, pool_w), BF16),
            pltpu.VMEM((length, chans), BF16),
            pltpu.VMEM((length, chans), BF16),
            pltpu.VMEM((length, chans), BF16),
            pltpu.VMEM((blocks, 8, chans), F32),
            pltpu.VMEM((DK, chans), F32),
            pltpu.VMEM((heads, DK + HALO, DK), BF16),
            pltpu.VMEM((heads, DK + HALO, DK), BF16),
            pltpu.VMEM((DK + HALO, DK), BF16),
            pltpu.VMEM((n_sp // heads, DK + HALO, DK), BF16),
            pltpu.VMEM((heads, DK, DK), BF16),
            pltpu.VMEM((heads, DK, DK), BF16),
            pltpu.VMEM((HALO, pool_w), BF16),
            pltpu.VMEM((chunks, rows_x, LANES), F32),
            pltpu.VMEM((chunks, rows_x, LANES), F32),
            pltpu.VMEM((mix.shape[0], BLOCK_ROWS, 2 * BLOCK_ROWS), BF16),
            pltpu.VMEM(mix.shape, BF16),
            pltpu.VMEM((1, pool_w), F32),
            pltpu.VMEM((1, chans), F32),
            pltpu.VMEM((heads, length), F32),
            pltpu.VMEM((1, DK), F32),
            dma((chunks,)), dma((chunks,)), dma((chunks,)), dma((5, n_tp)),
            dma((2,)), dma((2,)), dma((2,)), dma((2, chunks)), dma((2, chunks)),
            dma((heads,)), dma((heads,)), dma((n_sp // heads,)), dma((n_sp // heads,)),
            dma((heads,)), dma((heads,)), dma, dma, dma((chunks,)), dma((chunks,)), dma((5,)),
        ]
        row = lambda x: x.reshape(1, -1)
        resid, stats = pl.pallas_call(
            functools.partial(mixer, n_sp, n_tp, rows_x),
            out_shape=(pltpu.VMEM((length, feats), F32), pltpu.VMEM((length, LANES), F32)),
            in_specs=[hbm] * 13,
            out_specs=(vmem, vmem),
            scratch_shapes=scratch,
            compiler_params=pltpu.CompilerParams(
                collective_id=0, has_side_effects=True, vmem_limit_bytes=LIMIT),
            name="mixer",
        )(stream, w_pool, w_query, w_forget, w_value, w_gate, mix, row(scale), row(bound), extra.T,
          row(gain), wo_pool, wo_rec)
        piece = 128
        pieces = length // piece
        return pl.pallas_call(
            functools.partial(finish, n_tp * feats, piece),
            out_shape=jax.ShapeDtypeStruct(stream.shape, BF16),
            in_specs=[vmem] * 4,
            out_specs=hbm,
            scratch_shapes=[pltpu.VMEM((length, feats), BF16), dma((pieces,))],
            compiler_params=pltpu.CompilerParams(vmem_limit_bytes=16 * 1024 * 1024),
            name="finish",
        )(resid, stats, row(norm_gain), row(norm_bias))

    placed = (
        P("fs", "sp", "tp"), P(None, "tp"), P(None, "tp"), P(None, "tp"), P(None, "tp"),
        P(None, "tp"), P("tp", None, None), P("tp"), P("tp"), P("sp", "tp"), P(),
        P("tp", None), P("tp", None), P("tp"), P("tp"),
    )
    return jax.shard_map(
        local, mesh=mesh, in_specs=placed, out_specs=P("fs", "sp", "tp"), check_vma=False
    )
```

```python
import functools

import jax
import jax.numpy as jnp
from jax import lax
from jax.experimental import pallas as pl
from jax.experimental.pallas import tpu as pltpu
from jax.sharding import PartitionSpec as P

DK = 128
BLOCK_ROWS = 128
GROUP_CH = 256
HALO = 16
LANES = 128

LIMIT = 56 * 1024 * 1024
ALPHA = 2.0**0.25
EPS_RMS = 1e-06
EPS_NORM = 1e-05
F32 = jnp.float32
BF16 = jnp.bfloat16
NT = (((1,), (1,)), ((), ()))
TN = (((0,), (0,)), ((), ()))
OWN, PEER = 0, 1


def dot(a, b, dims=None):
    if dims is None:
        return jnp.dot(a, b, preferred_element_type=F32)
    return lax.dot_general(a, b, dims, preferred_element_type=F32)


def half_sigmoid(x):
    return 0.5 + 0.5 * jnp.tanh(0.5 * x)


def mixer(
    n_sp, n_tp, rows_x,
    stream, w_pool, w_query, w_forget, w_value, w_gate,
    mix_in, scale_in, bound_in, extra_in, gain_in, wo_pool, wo_rec,
    r_buf, stats,
    x_buf, w_buf, wo_buf, a_buf, v_buf, u_buf, e_buf, t_buf, p_buf, q_buf, g_buf, f_buf,
    half_buf, state, mine_out, row_in, total_out, total_in, start_out, start_in, halo_in,
    stat_own, stat_peer, bands,
    mix, scale, bound, extra, gain,
    x_loc, x_send, x_recv, w_sem, wo_loc, wo_send, wo_recv, a_send, a_recv,
    m_send, m_recv, r_send, r_recv, b_send, b_recv, h_send, h_recv, s_send, s_recv, small_sem, ready,
):
    sp, tp = lax.axis_index("sp"), lax.axis_index("tp")
    peer = 1 - tp
    length, feats = stream.shape[1], stream.shape[2]
    chans = bound.shape[1]
    heads = chans // DK
    pool_w = scale.shape[1]
    groups = mix.shape[0]
    chunks = length // rows_x
    blocks = length // BLOCK_ROWS
    per = rows_x // BLOCK_ROWS
    row_n = heads
    col_n = n_sp // row_n
    x_at, z_at = lax.rem(sp, row_n), lax.div(sp, row_n)
    row0 = z_at * row_n
    mesh_id = pl.DeviceIdType.MESH

    def rows_of(c):
        return slice(c * rows_x, (c + 1) * rows_x)

    def block_of(b):
        return slice(b * BLOCK_ROWS, (b + 1) * BLOCK_ROWS)

    def head_of(h):
        return slice(h * DK, (h + 1) * DK)

    x_pieces = ((0, rows_x), (rows_x, rows_x), (2 * rows_x, length - 2 * rows_x))
    pool_pieces = ((length // 2, length // 2), (0, length // 2))
    rec_pieces = ((0, 2 * rows_x),) + tuple((c * rows_x, rows_x) for c in range(2, chunks))
    stat_pieces = ((0, length // 2), (length // 2, length // 2))

    def to_peer(src, dst, send, recv):
        return pltpu.make_async_remote_copy(
            src, dst, send, recv, device_id={"tp": peer}, device_id_type=mesh_id)

    def to_sp(src, dst, send, recv, k):
        return pltpu.make_async_remote_copy(
            src, dst, send, recv, device_id={"sp": k}, device_id_type=mesh_id)

    def x_in(i):
        rows = pl.ds(*x_pieces[i])
        return pltpu.make_async_copy(stream.at[0, rows], x_buf.at[OWN, rows], x_loc.at[i])

    def x_out(i):
        rows = pl.ds(*x_pieces[i])
        return to_peer(x_buf.at[OWN, rows], x_buf.at[PEER, rows], x_send, x_recv.at[i])

    my_cols = pl.ds(pl.multiple_of(tp * feats, LANES), feats)
    peer_cols = pl.ds(pl.multiple_of(peer * feats, LANES), feats)
    wo_places = ((wo_pool, pl.ds(0, pool_w)), (wo_rec, pl.ds(pool_w, chans)))

    w_groups = {(0, OWN): 0, (1, OWN): 1, (0, PEER): 2, (1, PEER): 2, (2, OWN): 3, (2, PEER): 3}

    def w_in(i, side):
        src = (w_forget, w_value, w_pool, w_query, w_gate)[i]
        return pltpu.make_async_copy(
            src.at[my_cols if side == OWN else peer_cols], w_buf.at[i, side], w_sem.at[w_groups.get((i, side), 4)])

    def w_wait(ref, group):
        pltpu.make_async_copy(ref, ref, w_sem.at[group]).wait()

    def wo_in(i):
        src, place = wo_places[i]
        return pltpu.make_async_copy(src.at[:, my_cols], wo_buf.at[OWN, place], wo_loc)

    def wo_out(i):
        src, place = wo_places[i]
        return to_peer(src.at[:, peer_cols], wo_buf.at[PEER, place], wo_send, wo_recv)

    def pool_out(i):
        rows, cols = pl.ds(*pool_pieces[i]), wo_places[0][1]
        return to_peer(a_buf.at[OWN, rows, cols], a_buf.at[PEER, rows, cols], a_send, a_recv.at[i])

    def rec_out(i):
        rows, cols = pl.ds(*rec_pieces[i]), wo_places[1][1]
        return to_peer(a_buf.at[OWN, rows, cols], a_buf.at[PEER, rows, cols], a_send, a_recv.at[len(pool_pieces) + i])

    def mine_to(k, slot):
        return to_sp(mine_out.at[k], row_in.at[slot], m_send, m_recv, row0 + k)

    def total_to(k, slot):
        return to_sp(total_out, total_in.at[slot], r_send, r_recv, k * row_n + x_at)

    def start_to(k, slot):
        return to_sp(start_out.at[k], start_in.at[slot], b_send, b_recv, row0 + k)

    def some(ref, count, send, recv):
        return to_sp(ref.at[0:count], ref.at[0:count], send, recv, row0)

    def when_equal(value, counts, do):
        for n in counts:
            @pl.when(value == n)
            def _():
                do(n)

    def h_out(k):
        return to_sp(p_buf.at[pl.ds(BLOCK_ROWS + length - HALO, HALO)], halo_in, h_send, h_recv, k)

    def s_out(i):
        rows = pl.ds(*stat_pieces[i])
        return to_peer(stat_own.at[rows], stat_peer.at[rows], s_send, s_recv.at[i])

    def greet(k):
        pl.semaphore_signal(ready, inc=1, device_id={"sp": k}, device_id_type=mesh_id)

    def each(low, high, do):
        def step(k, _):
            do(k)
            return 0

        lax.fori_loop(low, high, step, 0)

    smalls = [
        pltpu.make_async_copy(src, dst, small_sem.at[i])
        for i, (src, dst) in enumerate(
            ((extra_in, extra), (bound_in, bound), (mix_in, mix), (scale_in, scale), (gain_in, gain)))
    ]

    smalls[0].start()
    x_in(0).start()
    x_in(1).start()
    w_in(0, OWN).start()
    w_in(1, OWN).start()
    x_in(2).start()
    w_in(0, PEER).start()
    w_in(1, PEER).start()
    for copy in smalls[1:]:
        copy.start()

    barrier = pltpu.get_barrier_semaphore()
    pl.semaphore_signal(barrier, inc=1, device_id={"tp": peer}, device_id_type=mesh_id)

    def hail(k):
        pl.semaphore_signal(barrier, inc=1, device_id={"sp": k}, device_id_type=mesh_id)

    each(x_at + 1, row_n, lambda k: hail(row0 + k))
    each(z_at + 1, col_n, lambda k: hail(k * row_n + x_at))
    leads = (x_at == 0) & (z_at > 0)
    ends = (x_at == row_n - 1) & (z_at < col_n - 1)
    later = (row_n - 1 - x_at) + (col_n - 1 - z_at) + jnp.where(ends, 1, 0)
    p_buf[0:BLOCK_ROWS, :] = jnp.zeros((BLOCK_ROWS, pool_w), BF16)
    with jax.named_scope("extra"):
        smalls[0].wait()

    row_ids = lax.broadcasted_iota(jnp.int32, (BLOCK_ROWS, BLOCK_ROWS), 0)
    col_ids = lax.broadcasted_iota(jnp.int32, (BLOCK_ROWS, BLOCK_ROWS), 1)
    lower = row_ids >= col_ids

    with jax.named_scope("drops"):
        lower_twice = jnp.concatenate([row_ids, row_ids], axis=1) >= jnp.concatenate([col_ids, col_ids], axis=1)
        ones = jnp.ones((2 * BLOCK_ROWS, DK), BF16)
        for b in range(blocks):
            drop = extra[:, block_of(b)]
            drop_high = drop.astype(BF16).astype(F32)
            drop_low = drop - drop_high
            for h in range(heads):
                pair = jnp.concatenate([drop_high[h:h + 1], drop_low[h:h + 1]], axis=1)
                wide = jnp.where(lower_twice, jnp.broadcast_to(pair, (BLOCK_ROWS, 2 * BLOCK_ROWS)), 0.0)
                e_buf[block_of(b), head_of(h)] = dot(wide.astype(BF16), ones)
        wide_rows = lax.broadcasted_iota(jnp.int32, (BLOCK_ROWS, 2 * BLOCK_ROWS), 0) + BLOCK_ROWS
        wide_cols = lax.broadcasted_iota(jnp.int32, (BLOCK_ROWS, 2 * BLOCK_ROWS), 1)
        back = wide_rows - wide_cols
        for j in range(groups):
            window = jnp.left_shift(jnp.int32(2), tp * groups + j)
            share = 1.0 / window.astype(F32)
            inside = (back >= 0) & (back < window)
            bands[j] = (jnp.where(inside, share, 0.0) - jnp.where(back == 0, 1.0, 0.0)).astype(BF16)
        state[...] = jnp.zeros_like(state)

    with jax.named_scope("entry"):
        pl.semaphore_wait(barrier, 1 + x_at + z_at)
    each(0, x_at, lambda k: greet(row0 + k))
    each(0, z_at, lambda k: greet(k * row_n + x_at))
    with jax.named_scope("x_in"):
        for i in range(2):
            x_in(i).wait()
            x_out(i).start()
    with jax.named_scope("w01"):
        for i in (0, 1):
            w_wait(w_buf.at[i, OWN], i)

    tri = jnp.where(lower, 1.0, 0.0).astype(BF16)
    tri_twice = jnp.concatenate([tri, tri], axis=1)

    def proj(i, c):
        rows = rows_of(c)
        return dot(x_buf[OWN, rows, :], w_buf[i, OWN]) + dot(x_buf[PEER, rows, :], w_buf[i, PEER])

    class Post:
        def __init__(self, c):
            self.blocks = [c * per + j for j in range(per)]
            self.weight, self.split, self.total = {}, {}, {}
            self.down, self.half = {}, {}

        def logs(self):
            open_part = 1.0 - bound[...]
            for b in self.blocks:
                f_in = f_buf[block_of(b), :].astype(F32)
                weight = open_part * (0.5 - 0.5 * jnp.tanh(0.5 * f_in))
                keep = jnp.log(1.0 - weight)
                high = keep.astype(BF16)
                low = (keep - high.astype(F32)).astype(BF16)
                self.weight[b], self.split[b] = weight, jnp.concatenate([high, low], axis=0)

        def sums(self):
            for b in self.blocks:
                self.total[b] = dot(tri_twice, self.split[b]) + e_buf[block_of(b), :]

        def exps(self):
            for b in self.blocks:
                total = self.total[b]
                middle = 0.5 * total[BLOCK_ROWS - 1:BLOCK_ROWS]
                e_buf[block_of(b), :] = jnp.exp(total - middle)
                down = (self.weight[b] * jnp.exp(middle - total)).astype(BF16)
                u_buf[block_of(b), :] = down
                half = jnp.exp(middle)
                half_buf[b] = jnp.broadcast_to(half, (8, chans))
                self.down[b], self.half[b] = down, half

        def states(self):
            for b in self.blocks:
                for h in range(heads):
                    lanes = head_of(h)
                    hh = self.half[b][:, lanes]
                    term = dot(v_buf[block_of(b), lanes], self.down[b][:, lanes], TN) * hh
                    t_buf[b, :, lanes] = term
                    state[:, lanes] = hh * hh * state[:, lanes] + term

    def put_pool(c):
        p_buf[BLOCK_ROWS + c * rows_x:BLOCK_ROWS + (c + 1) * rows_x, :] = proj(2, c).astype(BF16)

    with jax.named_scope("own"):
        for c in (0, 1):
            own = x_buf[OWN, rows_of(c), :]
            for i in (0, 1):
                r_buf[rows_of(c), i * chans:(i + 1) * chans] = dot(own, w_buf[i, OWN])
    with jax.named_scope("x_in2"):
        x_in(2).wait()
        x_out(2).start()

    def rest(i, c):
        return (r_buf[rows_of(c), i * chans:(i + 1) * chans] + dot(x_buf[PEER, rows_of(c), :], w_buf[i, PEER])).astype(BF16)

    with jax.named_scope("x_recv0"):
        x_out(0).wait_recv()
        w_wait(w_buf.at[0:2, PEER], 2)
        for copy in smalls[1:]:
            copy.wait()
    for i in (2, 3, 4):
        for side in (OWN, PEER):
            w_in(i, side).start()
    with jax.named_scope("first0"):
        f_buf[rows_of(0), :] = rest(0, 0)
        v_buf[rows_of(0), :] = rest(1, 0)
    with jax.named_scope("x_recv1"):
        x_out(1).wait_recv()
    for c in range(1, chunks):
        if c == 2:
            with jax.named_scope("x_recv2"):
                x_out(2).wait_recv()
            for i in range(2):
                wo_in(i).start()
                wo_out(i).start()

            @pl.when(leads)
            def _():
                with jax.named_scope("lead"):
                    pl.semaphore_wait(ready, later)
                greet(sp - 1)

        with jax.named_scope("first"):
            post = Post(c - 1)
            post.logs()
            f_buf[rows_of(c), :] = rest(0, c) if c == 1 else proj(0, c).astype(BF16)
            post.sums()
            v_buf[rows_of(c), :] = rest(1, c) if c == 1 else proj(1, c).astype(BF16)
            post.exps()
            post.states()

    with jax.named_scope("w2"):
        w_wait(w_buf.at[2], 3)
    with jax.named_scope("second0"):
        post = Post(chunks - 1)
        post.logs()
        put_pool(chunks - 1)
        post.sums()
        put_pool(chunks - 2)
        post.exps()
        post.states()
        log_half = half_buf[0, 0:1]
        for b in range(1, blocks):
            log_half = log_half * half_buf[b, 0:1]
        keep_all = jnp.broadcast_to(log_half * log_half, (HALO, chans)).astype(BF16)
        for h in range(heads):
            mine_out[h, 0:DK, :] = state[:, head_of(h)].astype(BF16)
            mine_out[h, DK:DK + HALO, :] = keep_all[:, head_of(h)]

    @pl.when(jnp.logical_not(leads) & (sp + 1 < n_sp))
    def _():
        with jax.named_scope("later"):
            pl.semaphore_wait(ready, later)

    for step in range(1, row_n):
        mine_to(lax.rem(x_at + step, row_n), x_at).start()
    row_in[x_at] = mine_out[x_at]

    @pl.when(sp + 1 < n_sp)
    def _():
        h_out(sp + 1).start()

    with jax.named_scope("second"):
        for c in range(chunks - 2):
            put_pool(c)

    with jax.named_scope("w34"):
        w_wait(w_buf.at[3:5], 4)

    def part_of(ref, at):
        return ref[at, 0:DK, :].astype(F32), ref[at, DK:DK + HALO, :].astype(F32)[0:1]

    def fold_row():
        with jax.named_scope("row_recv"):
            some(row_in, row_n - 1, m_send, m_recv).wait_recv()
        total, kept = part_of(row_in, 0)
        for k in range(1, row_n):
            term, keep = part_of(row_in, k)
            total = keep * total + term
            kept = kept * keep
        total_out[0:DK, :] = total.astype(BF16)
        total_out[DK:DK + HALO, :] = jnp.broadcast_to(kept, (HALO, DK)).astype(BF16)
        each(z_at + 1, col_n, lambda k: total_to(k, z_at).start())

    def fold_column():
        state[:, 0:DK] = jnp.zeros((DK, DK), F32)
        with jax.named_scope("col_recv"):
            when_equal(z_at, range(1, col_n), lambda n: some(total_in, n, r_send, r_recv).wait_recv())

        def take(k):
            term, keep = part_of(total_in, k)
            state[:, 0:DK] = keep * state[:, 0:DK] + term

        each(0, z_at, take)
        total = state[:, 0:DK]
        for k in range(row_n):
            start_out[k] = total.astype(BF16)
            if k + 1 < row_n:
                term, keep = part_of(row_in, k)
                total = keep * total + term
        for step in range(1, row_n):
            k = lax.rem(x_at + step, row_n)

            @pl.when(row0 + k > 0)
            def _():
                start_to(k, x_at).start()

        start_in[x_at] = start_out[x_at]

    count = lax.broadcasted_iota(jnp.int32, (BLOCK_ROWS, LANES), 0) + (sp * length + 1)

    class Third:
        def __init__(self, c):
            self.c, self.rows = c, rows_of(c)
            self.blocks = [c * per + k for k in range(per)]

        def query(self):
            q_in = proj(3, self.c).astype(BF16).astype(F32)
            q_buf[self.rows, :] = (q_in * half_sigmoid(q_in) * e_buf[self.rows, :]).astype(BF16)

        def band(self):
            for b in self.blocks:
                near = p_buf[b * BLOCK_ROWS:(b + 2) * BLOCK_ROWS, :]
                for j in range(groups):
                    lanes = slice(j * GROUP_CH, (j + 1) * GROUP_CH)
                    if b:
                        a_buf[OWN, block_of(b), lanes] = dot(bands[j], near[:, lanes]).astype(BF16)
                        continue
                    window = jnp.left_shift(jnp.int32(2), tp * groups + j)
                    inside = jnp.where((back >= 0) & (back < window), 1.0, 0.0).astype(BF16)
                    share = 1.0 / jnp.minimum(count, window).astype(F32)
                    share = jnp.concatenate([share] * (GROUP_CH // LANES), axis=1)
                    sums = dot(inside, near[:, lanes])
                    a_buf[OWN, block_of(b), lanes] = (sums * share - near[BLOCK_ROWS:, lanes].astype(F32)).astype(BF16)

        def gates(self):
            g_buf[self.rows, :] = proj(4, self.c).astype(BF16)

        def mixed(self):
            for j in range(groups):
                lanes = slice(j * GROUP_CH, (j + 1) * GROUP_CH)
                a_buf[OWN, self.rows, lanes] = (dot(a_buf[OWN, self.rows, lanes], mix[j]) * scale[:, lanes]).astype(BF16)

        def score(self):
            for b in self.blocks:
                for h in range(heads):
                    up, down = q_buf[block_of(b), head_of(h)], u_buf[block_of(b), head_of(h)]
                    f_buf[block_of(b), head_of(h)] = jnp.where(lower, dot(up, down, NT), 0.0).astype(BF16)

        def inner(self):
            for b in self.blocks:
                for h in range(heads):
                    at = block_of(b), head_of(h)
                    e_buf[at] = dot(f_buf[at], v_buf[at])

    parts = [Third(c) for c in range(chunks)]
    early = x_at >= row_n // 2

    def fold_at(stage, who):
        @pl.when(who)
        def _():
            stage()

    for c in reversed(range(chunks)):
        if c == chunks - 2:
            fold_at(fold_row, early)
        if c == chunks - 3:
            pool_out(0).start()
            fold_at(fold_column, early)
            fold_at(fold_row, jnp.logical_not(early))
        if c == 0:
            fold_at(fold_column, jnp.logical_not(early))

            @pl.when(sp > 0)
            def _():
                with jax.named_scope("halo_recv"):
                    h_out(sp).wait_recv()
                p_buf[BLOCK_ROWS - HALO:BLOCK_ROWS, :] = halo_in[...]

        with jax.named_scope("third"):
            parts[c].query()
            if c + 1 < chunks:
                parts[c + 1].inner()
            parts[c].band()
            parts[c].gates()
            parts[c].mixed()
            parts[c].score()
    pool_out(1).start()

    with jax.named_scope("wo"):
        pltpu.make_async_copy(wo_buf.at[OWN], wo_buf.at[OWN], wo_loc).wait()
        to_peer(wo_buf.at[OWN], wo_buf.at[PEER], wo_send, wo_recv).wait_recv()
        pool_out(0).wait_recv()

    pool_at, rec_at = slice(0, pool_w), slice(pool_w, pool_w + chans)

    def pool_part(c):
        rows = rows_of(c)
        r_buf[rows, :] = (
            dot(a_buf[OWN, rows, pool_at], wo_buf[OWN, pool_at]) + dot(a_buf[PEER, rows, pool_at], wo_buf[PEER, pool_at])
            + ALPHA * x_buf[OWN, rows, :].astype(F32))

    with jax.named_scope("pool"):
        pool_part(chunks - 1)
        parts[0].inner()
        pool_part(chunks - 2)

    @pl.when(sp > 0)
    def _():
        with jax.named_scope("start_recv"):
            some(start_in, row_n - 1, b_send, b_recv).wait_recv()

    @pl.when(sp > 0)
    def _():
        for h in range(heads):
            state[:, head_of(h)] = start_in[h].astype(F32)

    @pl.when(sp == 0)
    def _():
        state[...] = jnp.zeros_like(state)

    def fourth(c):
        for k in range(per):
            b = c * per + k
            half = half_buf[b, 0:1]
            before = state[...] * half
            carried = before.astype(BF16)
            state[...] = before * half + t_buf[b]
            for h in range(heads):
                lanes = head_of(h)
                raw = e_buf[block_of(b), lanes] + dot(q_buf[block_of(b), lanes], carried[:, lanes], NT)
                power = jnp.mean(raw * raw, axis=-1, keepdims=True)
                gate = g_buf[block_of(b), lanes].astype(F32)
                rec = raw * lax.rsqrt(power + EPS_RMS) * gain[...] * (gate * half_sigmoid(gate))
                a_buf[OWN, block_of(b), pool_w + h * DK:pool_w + (h + 1) * DK] = rec.astype(BF16)

    def rec_part(side, c):
        r_buf[rows_of(c), :] += dot(a_buf[side, rows_of(c), rec_at], wo_buf[side, rec_at])

    with jax.named_scope("fourth"):
        fourth(0)
        with jax.named_scope("pool_recv"):
            pool_out(1).wait_recv()
        pool_part(1)
        fourth(1)
        pool_part(0)
        rec_out(0).start()
    with jax.named_scope("fourth2"):
        fourth(2)
        rec_part(OWN, 0)
        rec_out(1).start()
        fourth(3)
        rec_part(OWN, 1)
        rec_out(2).start()

    def fold(x):
        acc = x[:, :LANES]
        for k in range(1, feats // LANES):
            acc = acc + x[:, k * LANES:(k + 1) * LANES]
        return acc

    first_half = lax.broadcasted_iota(jnp.int32, (rows_x, LANES), 1) < LANES // 2

    def fifth(c):
        rows = rows_of(c)
        resid = r_buf[rows, :] + dot(a_buf[PEER, rows, rec_at], wo_buf[PEER, rec_at])
        r_buf[rows, :] = resid
        sums, squares = fold(resid), fold(resid * resid)
        sums = sums + pltpu.roll(sums, LANES // 2, 1)
        squares = squares + pltpu.roll(squares, LANES // 2, 1)
        stat_own[rows, :] = jnp.where(first_half, sums, squares)

    with jax.named_scope("fifth"):
        rec_out(0).wait_recv()
        fifth(0)
        fifth(1)
        rec_part(OWN, 2)
        s_out(0).start()
    with jax.named_scope("fifth2"):
        rec_out(1).wait_recv()
        fifth(2)
        rec_part(OWN, 3)
        rec_out(2).wait_recv()
        fifth(3)
        s_out(1).start()

    with jax.named_scope("sent"):
        to_peer(x_buf.at[OWN], x_buf.at[PEER], x_send, x_recv.at[0]).wait_send()
        to_peer(a_buf.at[OWN], a_buf.at[PEER], a_send, a_recv.at[0]).wait_send()
        to_peer(wo_buf.at[OWN], wo_buf.at[PEER], wo_send, wo_recv).wait_send()
        some(mine_out, row_n - 1, m_send, m_recv).wait_send()
        when_equal(col_n - 1 - z_at, range(1, col_n), lambda n: some(total_in, n, r_send, r_recv).wait_send())
        starts = jnp.where((z_at > 0) | (x_at == 0), row_n - 1, row_n - 2)
        when_equal(starts, (row_n - 2, row_n - 1), lambda n: some(start_out, n, b_send, b_recv).wait_send())

        @pl.when(sp + 1 < n_sp)
        def _():
            h_out(sp + 1).wait_send()

    with jax.named_scope("tail"):
        for i in range(2):
            s_out(i).wait_recv()
        stats[...] = stat_own[...] + stat_peer[...]
        to_peer(stat_own, stat_peer, s_send, s_recv.at[0]).wait_send()


def finish(width, rows, resid, stats, gain, bias, out, o_buf, o_sem):
    pieces = resid.shape[0] // rows

    def leave(c):
        part = pl.ds(c * rows, rows)
        return pltpu.make_async_copy(o_buf.at[part], out.at[0, part], o_sem.at[c])

    first_half = lax.broadcasted_iota(jnp.int32, (rows, LANES), 1) < LANES // 2
    for c in range(pieces):
        part = slice(c * rows, (c + 1) * rows)
        both = stats[part, :]
        mean = jnp.sum(jnp.where(first_half, both, 0.0), axis=1, keepdims=True) / width
        square = jnp.sum(jnp.where(first_half, 0.0, both), axis=1, keepdims=True) / width
        inv = lax.rsqrt(square - mean * mean + EPS_NORM)
        o_buf[part, :] = ((resid[part, :] - mean) * inv * gain[...] + bias[...]).astype(BF16)
        leave(c).start()
    for c in range(pieces):
        leave(c).wait()


def solution(mesh):
    n_sp, n_tp = mesh.shape["sp"], mesh.shape["tp"]

    def local(stream, w_pool, w_query, w_forget, w_value, w_gate, mix, scale, bound, extra,
              gain, wo_pool, wo_rec, norm_gain, norm_bias):
        length, feats = stream.shape[1], stream.shape[2]
        chans, pool_w = bound.shape[0], scale.shape[0]
        heads = chans // DK
        blocks = length // BLOCK_ROWS
        rows_x = 256
        chunks = length // rows_x
        hbm = pl.BlockSpec(memory_space=pl.ANY)
        vmem = pl.BlockSpec(memory_space=pltpu.VMEM)
        dma = pltpu.SemaphoreType.DMA
        scratch = [
            pltpu.VMEM((n_tp, length, feats), BF16),
            pltpu.VMEM((5, n_tp, feats, chans), BF16),
            pltpu.VMEM((n_tp, pool_w + chans, feats), BF16),
            pltpu.VMEM((n_tp, length, pool_w + chans), BF16),
            pltpu.VMEM((length, chans), BF16),
            pltpu.VMEM((length, chans), BF16),
            pltpu.VMEM((length, chans), F32),
            pltpu.VMEM((blocks, DK, chans), F32),
            pltpu.VMEM((BLOCK_ROWS + length, pool_w), BF16),
            pltpu.VMEM((length, chans), BF16),
            pltpu.VMEM((length, chans), BF16),
            pltpu.VMEM((length, chans), BF16),
            pltpu.VMEM((blocks, 8, chans), F32),
            pltpu.VMEM((DK, chans), F32),
            pltpu.VMEM((heads, DK + HALO, DK), BF16),
            pltpu.VMEM((heads, DK + HALO, DK), BF16),
            pltpu.VMEM((DK + HALO, DK), BF16),
            pltpu.VMEM((n_sp // heads, DK + HALO, DK), BF16),
            pltpu.VMEM((heads, DK, DK), BF16),
            pltpu.VMEM((heads, DK, DK), BF16),
            pltpu.VMEM((HALO, pool_w), BF16),
            pltpu.VMEM((length, LANES), F32),
            pltpu.VMEM((length, LANES), F32),
            pltpu.VMEM((mix.shape[0], BLOCK_ROWS, 2 * BLOCK_ROWS), BF16),
            pltpu.VMEM(mix.shape, BF16),
            pltpu.VMEM((1, pool_w), F32),
            pltpu.VMEM((1, chans), F32),
            pltpu.VMEM((heads, length), F32),
            pltpu.VMEM((1, DK), F32),
            dma((3,)), dma, dma((3,)), dma((5,)), dma, dma, dma, dma, dma((5,)),
            dma, dma, dma, dma, dma, dma, dma, dma, dma, dma((2,)), dma((5,)), pltpu.SemaphoreType.REGULAR,
        ]
        row = lambda x: x.reshape(1, -1)
        resid, stats = pl.pallas_call(
            functools.partial(mixer, n_sp, n_tp, rows_x),
            out_shape=(pltpu.VMEM((length, feats), F32), pltpu.VMEM((length, LANES), F32)),
            in_specs=[hbm] * 13,
            out_specs=(vmem, vmem),
            scratch_shapes=scratch,
            compiler_params=pltpu.CompilerParams(
                collective_id=0, has_side_effects=True, vmem_limit_bytes=LIMIT),
            name="mixer",
        )(stream, w_pool, w_query, w_forget, w_value, w_gate, mix, row(scale), row(bound), extra.T,
          row(gain), wo_pool, wo_rec)
        piece = 128
        pieces = length // piece
        return pl.pallas_call(
            functools.partial(finish, n_tp * feats, piece),
            out_shape=jax.ShapeDtypeStruct(stream.shape, BF16),
            in_specs=[vmem] * 4,
            out_specs=hbm,
            scratch_shapes=[pltpu.VMEM((length, feats), BF16), dma((pieces,))],
            compiler_params=pltpu.CompilerParams(vmem_limit_bytes=16 * 1024 * 1024),
            name="finish",
        )(resid, stats, row(norm_gain), row(norm_bias))

    placed = (
        P("fs", "sp", "tp"), P(None, "tp"), P(None, "tp"), P(None, "tp"), P(None, "tp"),
        P(None, "tp"), P("tp", None, None), P("tp"), P("tp"), P("sp", "tp"), P(),
        P("tp", None), P("tp", None), P("tp"), P("tp"),
    )
    return jax.shard_map(
        local, mesh=mesh, in_specs=placed, out_specs=P("fs", "sp", "tp"), check_vma=False
    )
```

```python
import functools

import jax
import jax.numpy as jnp
from jax import lax
from jax.experimental import pallas as pl
from jax.experimental.pallas import tpu as pltpu
from jax.sharding import PartitionSpec as P

DK = 128
BLOCK_ROWS = 128
GROUP_CH = 256
HALO = 16
LANES = 128

LIMIT = 56 * 1024 * 1024
ALPHA = 2.0**0.25
EPS_RMS = 1e-06
EPS_NORM = 1e-05
F32 = jnp.float32
BF16 = jnp.bfloat16
NT = (((1,), (1,)), ((), ()))
TN = (((0,), (0,)), ((), ()))
OWN, PEER = 0, 1


def dot(a, b, dims=None):
    if dims is None:
        return jnp.dot(a, b, preferred_element_type=F32)
    return lax.dot_general(a, b, dims, preferred_element_type=F32)


def half_sigmoid(x):
    return 0.5 + 0.5 * jnp.tanh(0.5 * x)


def mixer(
    n_sp, n_tp, rows_x,
    stream, w_pool, w_query, w_forget, w_value, w_gate,
    mix_in, scale_in, bound_in, extra_in, gain_in, wo_pool, wo_rec,
    r_buf, stats,
    x_buf, w_buf, wo_buf, a_buf, v_buf, u_buf, e_buf, t_buf, p_buf, q_buf, g_buf, f_buf,
    half_buf, state, mine_out, row_in, total_out, total_in, start_out, start_in, halo_in,
    stat_own, stat_peer, bands,
    mix, scale, bound, extra, gain,
    x_loc, x_send, x_recv, w_sem, wo_loc, wo_send, wo_recv, a_send, a_recv,
    m_send, m_recv, r_send, r_recv, b_send, b_recv, h_send, h_recv, s_send, s_recv, small_sem, ready,
):
    sp, tp = lax.axis_index("sp"), lax.axis_index("tp")
    peer = 1 - tp
    length, feats = stream.shape[1], stream.shape[2]
    chans = bound.shape[1]
    heads = chans // DK
    pool_w = scale.shape[1]
    groups = mix.shape[0]
    chunks = length // rows_x
    blocks = length // BLOCK_ROWS
    per = rows_x // BLOCK_ROWS
    row_n = heads
    col_n = n_sp // row_n
    x_at, z_at = lax.rem(sp, row_n), lax.div(sp, row_n)
    row0 = z_at * row_n
    mesh_id = pl.DeviceIdType.MESH

    def rows_of(c):
        return slice(c * rows_x, (c + 1) * rows_x)

    def block_of(b):
        return slice(b * BLOCK_ROWS, (b + 1) * BLOCK_ROWS)

    def head_of(h):
        return slice(h * DK, (h + 1) * DK)

    x_pieces = ((0, length // 2), (length // 2, length // 2))
    pool_pieces = ((2 * rows_x, length - 2 * rows_x), (rows_x, rows_x), (0, rows_x))
    rec_pieces = ((0, 2 * rows_x),) + tuple((c * rows_x, rows_x) for c in range(2, chunks))
    stat_pieces = rec_pieces

    def to_peer(src, dst, send, recv):
        return pltpu.make_async_remote_copy(
            src, dst, send, recv, device_id={"tp": peer}, device_id_type=mesh_id)

    def to_sp(src, dst, send, recv, k):
        return pltpu.make_async_remote_copy(
            src, dst, send, recv, device_id={"sp": k}, device_id_type=mesh_id)

    def x_in(i):
        rows = pl.ds(*x_pieces[i])
        return pltpu.make_async_copy(stream.at[0, rows], x_buf.at[OWN, rows], x_loc.at[i])

    def x_out(i):
        rows = pl.ds(*x_pieces[i])
        return to_peer(x_buf.at[OWN, rows], x_buf.at[PEER, rows], x_send, x_recv.at[i])

    my_cols = pl.ds(pl.multiple_of(tp * feats, LANES), feats)
    peer_cols = pl.ds(pl.multiple_of(peer * feats, LANES), feats)
    wo_places = ((wo_pool, pl.ds(0, pool_w)), (wo_rec, pl.ds(pool_w, chans)))

    w_groups = {(0, OWN): 0, (1, OWN): 1, (0, PEER): 2, (1, PEER): 2, (2, OWN): 3, (2, PEER): 3}

    def w_in(i, side):
        src = (w_forget, w_value, w_pool, w_query, w_gate)[i]
        return pltpu.make_async_copy(
            src.at[my_cols if side == OWN else peer_cols], w_buf.at[i, side], w_sem.at[w_groups.get((i, side), 4)])

    def w_wait(ref, group):
        pltpu.make_async_copy(ref, ref, w_sem.at[group]).wait()

    def wo_in(i):
        src, place = wo_places[i]
        return pltpu.make_async_copy(src.at[:, my_cols], wo_buf.at[OWN, place], wo_loc)

    def wo_out(i):
        src, place = wo_places[i]
        return to_peer(src.at[:, peer_cols], wo_buf.at[PEER, place], wo_send, wo_recv)

    def pool_out(i):
        rows, cols = pl.ds(*pool_pieces[i]), wo_places[0][1]
        return to_peer(a_buf.at[OWN, rows, cols], a_buf.at[PEER, rows, cols], a_send, a_recv.at[i])

    def rec_out(i):
        rows, cols = pl.ds(*rec_pieces[i]), wo_places[1][1]
        return to_peer(a_buf.at[OWN, rows, cols], a_buf.at[PEER, rows, cols], a_send, a_recv.at[len(pool_pieces) + i])

    def mine_to(k, slot):
        return to_sp(mine_out.at[k], row_in.at[slot], m_send, m_recv, row0 + k)

    def total_to(k, slot):
        return to_sp(total_out, total_in.at[slot], r_send, r_recv, k * row_n + x_at)

    def start_to(k, slot):
        return to_sp(start_out.at[k], start_in.at[slot], b_send, b_recv, row0 + k)

    def some(ref, count, send, recv):
        return to_sp(ref.at[0:count], ref.at[0:count], send, recv, row0)

    def when_equal(value, counts, do):
        for n in counts:
            @pl.when(value == n)
            def _():
                do(n)

    def h_out(k):
        return to_sp(p_buf.at[pl.ds(BLOCK_ROWS + length - HALO, HALO)], halo_in, h_send, h_recv, k)

    def s_out(i):
        rows = pl.ds(*stat_pieces[i])
        return to_peer(stat_own.at[rows], stat_peer.at[rows], s_send, s_recv.at[i])

    def greet(k):
        pl.semaphore_signal(ready, inc=1, device_id={"sp": k}, device_id_type=mesh_id)

    def each(low, high, do):
        def step(k, _):
            do(k)
            return 0

        lax.fori_loop(low, high, step, 0)

    smalls = [
        pltpu.make_async_copy(src, dst, small_sem.at[i])
        for i, (src, dst) in enumerate(
            ((extra_in, extra), (bound_in, bound), (mix_in, mix), (scale_in, scale), (gain_in, gain)))
    ]

    x_in(0).start()
    smalls[0].start()
    x_in(1).start()
    w_in(0, OWN).start()

    barrier = pltpu.get_barrier_semaphore()
    pl.semaphore_signal(barrier, inc=1, device_id={"tp": peer}, device_id_type=mesh_id)

    def hail(k):
        pl.semaphore_signal(barrier, inc=1, device_id={"sp": k}, device_id_type=mesh_id)

    each(x_at + 1, row_n, lambda k: hail(row0 + k))
    each(z_at + 1, col_n, lambda k: hail(k * row_n + x_at))
    leads = (x_at == 0) & (z_at > 0)
    ends = (x_at == row_n - 1) & (z_at < col_n - 1)
    later = (row_n - 1 - x_at) + (col_n - 1 - z_at) + jnp.where(ends, 1, 0)
    p_buf[0:BLOCK_ROWS, :] = jnp.zeros((BLOCK_ROWS, pool_w), BF16)
    with jax.named_scope("extra"):
        smalls[0].wait()
    w_in(1, OWN).start()
    w_in(0, PEER).start()
    w_in(1, PEER).start()
    for copy in smalls[1:]:
        copy.start()

    row_ids = lax.broadcasted_iota(jnp.int32, (BLOCK_ROWS, BLOCK_ROWS), 0)
    col_ids = lax.broadcasted_iota(jnp.int32, (BLOCK_ROWS, BLOCK_ROWS), 1)
    lower = row_ids >= col_ids

    with jax.named_scope("drops"):
        lower_twice = jnp.concatenate([row_ids, row_ids], axis=1) >= jnp.concatenate([col_ids, col_ids], axis=1)
        ones = jnp.ones((2 * BLOCK_ROWS, DK), BF16)
        for b in range(blocks):
            drop = extra[:, block_of(b)]
            drop_high = drop.astype(BF16).astype(F32)
            drop_low = drop - drop_high
            for h in range(heads):
                pair = jnp.concatenate([drop_high[h:h + 1], drop_low[h:h + 1]], axis=1)
                wide = jnp.where(lower_twice, jnp.broadcast_to(pair, (BLOCK_ROWS, 2 * BLOCK_ROWS)), 0.0)
                e_buf[block_of(b), head_of(h)] = dot(wide.astype(BF16), ones)
        wide_rows = lax.broadcasted_iota(jnp.int32, (BLOCK_ROWS, 2 * BLOCK_ROWS), 0) + BLOCK_ROWS
        wide_cols = lax.broadcasted_iota(jnp.int32, (BLOCK_ROWS, 2 * BLOCK_ROWS), 1)
        back = wide_rows - wide_cols
        for j in range(groups):
            window = jnp.left_shift(jnp.int32(2), tp * groups + j)
            share = 1.0 / window.astype(F32)
            inside = (back >= 0) & (back < window)
            bands[j] = (jnp.where(inside, share, 0.0) - jnp.where(back == 0, 1.0, 0.0)).astype(BF16)
        state[...] = jnp.zeros_like(state)

    with jax.named_scope("entry"):
        pl.semaphore_wait(barrier, 1 + x_at + z_at)
    each(0, x_at, lambda k: greet(row0 + k))
    each(0, z_at, lambda k: greet(k * row_n + x_at))
    with jax.named_scope("x_in"):
        for i in range(2):
            x_in(i).wait()
            x_out(i).start()
    with jax.named_scope("w0"):
        w_wait(w_buf.at[0, OWN], 0)

    tri = jnp.where(lower, 1.0, 0.0).astype(BF16)
    tri_twice = jnp.concatenate([tri, tri], axis=1)

    def proj(i, c, part=slice(0, rows_x)):
        rows = slice(c * rows_x + part.start, c * rows_x + part.stop)
        return dot(x_buf[OWN, rows, :], w_buf[i, OWN]) + dot(x_buf[PEER, rows, :], w_buf[i, PEER])

    class Post:
        def __init__(self, c):
            self.blocks = [c * per + j for j in range(per)]
            self.weight, self.split, self.total = {}, {}, {}
            self.down, self.half = {}, {}

        def logs(self):
            open_part = 1.0 - bound[...]
            for b in self.blocks:
                f_in = f_buf[block_of(b), :].astype(F32)
                weight = open_part * (0.5 - 0.5 * jnp.tanh(0.5 * f_in))
                keep = jnp.log(1.0 - weight)
                high = keep.astype(BF16)
                low = (keep - high.astype(F32)).astype(BF16)
                self.weight[b], self.split[b] = weight, jnp.concatenate([high, low], axis=0)

        def sums(self):
            for b in self.blocks:
                self.total[b] = dot(tri_twice, self.split[b]) + e_buf[block_of(b), :]

        def exps(self):
            for b in self.blocks:
                total = self.total[b]
                middle = 0.5 * total[BLOCK_ROWS - 1:BLOCK_ROWS]
                e_buf[block_of(b), :] = jnp.exp(total - middle)
                down = (self.weight[b] * jnp.exp(middle - total)).astype(BF16)
                u_buf[block_of(b), :] = down
                half = jnp.exp(middle)
                half_buf[b] = jnp.broadcast_to(half, (8, chans))
                self.down[b], self.half[b] = down, half

        def states(self):
            for b in self.blocks:
                for h in range(heads):
                    lanes = head_of(h)
                    hh = self.half[b][:, lanes]
                    term = dot(v_buf[block_of(b), lanes], self.down[b][:, lanes], TN) * hh
                    t_buf[b, :, lanes] = term
                    state[:, lanes] = hh * hh * state[:, lanes] + term

    whole, upper, under = slice(0, rows_x), slice(0, rows_x // 2), slice(rows_x // 2, rows_x)

    def put_pool(c, part=whole):
        at = BLOCK_ROWS + c * rows_x
        p_buf[at + part.start:at + part.stop, :] = proj(2, c, part).astype(BF16)

    def own_half(i):
        for c in range(chunks):
            r_buf[rows_of(c), i * chans:(i + 1) * chans] = dot(x_buf[OWN, rows_of(c), :], w_buf[i, OWN])

    with jax.named_scope("own0"):
        own_half(0)
    with jax.named_scope("w1"):
        w_wait(w_buf.at[1, OWN], 1)
    with jax.named_scope("own1"):
        own_half(1)

    def rest(i, c):
        return (r_buf[rows_of(c), i * chans:(i + 1) * chans] + dot(x_buf[PEER, rows_of(c), :], w_buf[i, PEER])).astype(BF16)

    with jax.named_scope("x_recv0"):
        x_out(0).wait_recv()
        w_wait(w_buf.at[0:2, PEER], 2)
        for copy in smalls[1:]:
            copy.wait()
    for i in (2, 3, 4):
        for side in (OWN, PEER):
            w_in(i, side).start()
    for c in range(chunks):
        if c == 2:
            with jax.named_scope("x_recv1"):
                x_out(1).wait_recv()
            for i in range(2):
                wo_in(i).start()
                wo_out(i).start()

            @pl.when(leads)
            def _():
                with jax.named_scope("lead"):
                    pl.semaphore_wait(ready, later)
                greet(sp - 1)

        with jax.named_scope("first"):
            if c:
                post = Post(c - 1)
                post.logs()
            f_buf[rows_of(c), :] = rest(0, c)
            if c:
                post.sums()
            v_buf[rows_of(c), :] = rest(1, c)
            if c:
                post.exps()
                post.states()

    with jax.named_scope("w2"):
        w_wait(w_buf.at[2], 3)
    with jax.named_scope("second0"):
        post = Post(chunks - 1)
        post.logs()
        put_pool(chunks - 1)
        post.sums()
        put_pool(chunks - 2)
        post.exps()
        post.states()
        log_half = half_buf[0, 0:1]
        for b in range(1, blocks):
            log_half = log_half * half_buf[b, 0:1]
        keep_all = jnp.broadcast_to(log_half * log_half, (HALO, chans)).astype(BF16)
        for h in range(heads):
            mine_out[h, 0:DK, :] = state[:, head_of(h)].astype(BF16)
            mine_out[h, DK:DK + HALO, :] = keep_all[:, head_of(h)]

    @pl.when(jnp.logical_not(leads) & (sp + 1 < n_sp))
    def _():
        with jax.named_scope("later"):
            pl.semaphore_wait(ready, later)

    for step in range(1, row_n):
        mine_to(lax.rem(x_at + step, row_n), x_at).start()
    row_in[x_at] = mine_out[x_at]

    @pl.when(sp + 1 < n_sp)
    def _():
        h_out(sp + 1).start()

    with jax.named_scope("w34"):
        w_wait(w_buf.at[3:5], 4)
    with jax.named_scope("second"):
        for c in range(chunks - 2):
            put_pool(c)

    def part_of(ref, at):
        return ref[at, 0:DK, :].astype(F32), ref[at, DK:DK + HALO, :].astype(F32)[0:1]

    def fold_row():
        with jax.named_scope("row_recv"):
            some(row_in, row_n - 1, m_send, m_recv).wait_recv()
        total, kept = part_of(row_in, 0)
        for k in range(1, row_n):
            term, keep = part_of(row_in, k)
            total = keep * total + term
            kept = kept * keep
        total_out[0:DK, :] = total.astype(BF16)
        total_out[DK:DK + HALO, :] = jnp.broadcast_to(kept, (HALO, DK)).astype(BF16)
        each(z_at + 1, col_n, lambda k: total_to(k, z_at).start())

    def fold_column():
        state[:, 0:DK] = jnp.zeros((DK, DK), F32)
        with jax.named_scope("col_recv"):
            when_equal(z_at, range(1, col_n), lambda n: some(total_in, n, r_send, r_recv).wait_recv())

        def take(k):
            term, keep = part_of(total_in, k)
            state[:, 0:DK] = keep * state[:, 0:DK] + term

        each(0, z_at, take)
        total = state[:, 0:DK]
        for k in range(row_n):
            start_out[k] = total.astype(BF16)
            if k + 1 < row_n:
                term, keep = part_of(row_in, k)
                total = keep * total + term
        for step in range(1, row_n):
            k = lax.rem(x_at + step, row_n)

            @pl.when(row0 + k > 0)
            def _():
                start_to(k, x_at).start()

        start_in[x_at] = start_out[x_at]

    count = lax.broadcasted_iota(jnp.int32, (BLOCK_ROWS, LANES), 0) + (sp * length + 1)

    gains = jnp.concatenate([gain[...]] * heads, axis=1)

    class Third:
        def __init__(self, c):
            self.c, self.rows = c, rows_of(c)
            self.blocks = [c * per + k for k in range(per)]

        def query(self):
            q_in = proj(3, self.c).astype(BF16).astype(F32)
            q_buf[self.rows, :] = (q_in * half_sigmoid(q_in) * e_buf[self.rows, :]).astype(BF16)

        def band(self):
            for b in self.blocks:
                near = p_buf[b * BLOCK_ROWS:(b + 2) * BLOCK_ROWS, :]
                for j in range(groups):
                    lanes = slice(j * GROUP_CH, (j + 1) * GROUP_CH)
                    if b:
                        a_buf[OWN, block_of(b), lanes] = dot(bands[j], near[:, lanes]).astype(BF16)
                        continue
                    window = jnp.left_shift(jnp.int32(2), tp * groups + j)
                    inside = jnp.where((back >= 0) & (back < window), 1.0, 0.0).astype(BF16)
                    share = 1.0 / jnp.minimum(count, window).astype(F32)
                    share = jnp.concatenate([share] * (GROUP_CH // LANES), axis=1)
                    sums = dot(inside, near[:, lanes])
                    a_buf[OWN, block_of(b), lanes] = (sums * share - near[BLOCK_ROWS:, lanes].astype(F32)).astype(BF16)

        def gates(self, part):
            rows = slice(self.rows.start + part.start, self.rows.start + part.stop)
            gate = proj(4, self.c, part).astype(BF16).astype(F32)
            g_buf[rows, :] = gate * half_sigmoid(gate) * gains

        def mixed(self):
            for j in range(groups):
                lanes = slice(j * GROUP_CH, (j + 1) * GROUP_CH)
                a_buf[OWN, self.rows, lanes] = (dot(a_buf[OWN, self.rows, lanes], mix[j]) * scale[:, lanes]).astype(BF16)

        def score(self):
            for b in self.blocks:
                for h in range(heads):
                    up, down = q_buf[block_of(b), head_of(h)], u_buf[block_of(b), head_of(h)]
                    f_buf[block_of(b), head_of(h)] = jnp.where(lower, dot(up, down, NT), 0.0).astype(BF16)

        def inner(self):
            for b in self.blocks:
                for h in range(heads):
                    at = block_of(b), head_of(h)
                    e_buf[at] = dot(f_buf[at], v_buf[at])

    parts = [Third(c) for c in range(chunks)]
    early = x_at > 0

    def fold_at(stage, who):
        @pl.when(who)
        def _():
            stage()

    for c in reversed(range(chunks)):
        if c == 1:
            pool_out(0).start()
            fold_at(fold_row, early)
        if c == 0:
            pool_out(1).start()
            fold_at(fold_column, early)
            fold_at(fold_row, jnp.logical_not(early))

            @pl.when(sp > 0)
            def _():
                with jax.named_scope("halo_recv"):
                    h_out(sp).wait_recv()
                p_buf[BLOCK_ROWS - HALO:BLOCK_ROWS, :] = halo_in[...]

        with jax.named_scope("third"):
            parts[c].query()
            if c + 1 < chunks:
                parts[c + 1].inner()
            parts[c].band()
            parts[c].gates(whole)
            parts[c].mixed()
            parts[c].score()
    pool_out(2).start()
    fold_at(fold_column, jnp.logical_not(early))

    with jax.named_scope("wo"):
        pltpu.make_async_copy(wo_buf.at[OWN], wo_buf.at[OWN], wo_loc).wait()
        to_peer(wo_buf.at[OWN], wo_buf.at[PEER], wo_send, wo_recv).wait_recv()
        pool_out(0).wait_recv()

    pool_at, rec_at = slice(0, pool_w), slice(pool_w, pool_w + chans)

    def pool_part(c):
        rows = rows_of(c)
        r_buf[rows, :] = (
            dot(a_buf[OWN, rows, pool_at], wo_buf[OWN, pool_at]) + dot(a_buf[PEER, rows, pool_at], wo_buf[PEER, pool_at])
            + ALPHA * x_buf[OWN, rows, :].astype(F32))

    with jax.named_scope("pool"):
        pool_part(chunks - 1)
        parts[0].inner()
        pool_part(chunks - 2)
    with jax.named_scope("pool_recv"):
        pool_out(1).wait_recv()
    with jax.named_scope("pool"):
        pool_part(1)

    with jax.named_scope("pool_recv"):
        pool_out(2).wait_recv()

    @pl.when(sp > 0)
    def _():
        with jax.named_scope("start_recv"):
            some(start_in, row_n - 1, b_send, b_recv).wait_recv()

    @pl.when(sp > 0)
    def _():
        for h in range(heads):
            state[:, head_of(h)] = start_in[h].astype(F32)

    @pl.when(sp == 0)
    def _():
        state[...] = jnp.zeros_like(state)

    def fourth(c):
        for k in range(per):
            b = c * per + k
            half = half_buf[b, 0:1]
            before = state[...] * half
            carried = before.astype(BF16)
            state[...] = before * half + t_buf[b]
            for h in range(heads):
                lanes = head_of(h)
                raw = e_buf[block_of(b), lanes] + dot(q_buf[block_of(b), lanes], carried[:, lanes], NT)
                power = jnp.mean(raw * raw, axis=-1, keepdims=True)
                rec = raw * lax.rsqrt(power + EPS_RMS) * g_buf[block_of(b), lanes]
                a_buf[OWN, block_of(b), pool_w + h * DK:pool_w + (h + 1) * DK] = rec.astype(BF16)

    def rec_part(side, c):
        r_buf[rows_of(c), :] += dot(a_buf[side, rows_of(c), rec_at], wo_buf[side, rec_at])

    with jax.named_scope("fourth"):
        fourth(0)
        pool_part(0)
        fourth(1)
        rec_out(0).start()
    with jax.named_scope("fourth2"):
        fourth(2)
        rec_part(OWN, 0)
        rec_out(1).start()
        fourth(3)
        rec_part(OWN, 1)
        rec_out(2).start()

    def fold(x):
        acc = x[:, :LANES]
        for k in range(1, feats // LANES):
            acc = acc + x[:, k * LANES:(k + 1) * LANES]
        return acc

    first_half = lax.broadcasted_iota(jnp.int32, (rows_x, LANES), 1) < LANES // 2

    def fifth(c):
        rows = rows_of(c)
        resid = r_buf[rows, :] + dot(a_buf[PEER, rows, rec_at], wo_buf[PEER, rec_at])
        r_buf[rows, :] = resid
        sums, squares = fold(resid), fold(resid * resid)
        sums = sums + pltpu.roll(sums, LANES // 2, 1)
        squares = squares + pltpu.roll(squares, LANES // 2, 1)
        stat_own[rows, :] = jnp.where(first_half, sums, squares)

    with jax.named_scope("fifth"):
        rec_out(0).wait_recv()
        fifth(0)
        fifth(1)
        rec_part(OWN, 2)
        s_out(0).start()
    with jax.named_scope("fifth2"):
        rec_out(1).wait_recv()
        fifth(2)
        rec_part(OWN, 3)
        s_out(1).start()
    with jax.named_scope("fifth3"):
        rec_out(2).wait_recv()
        fifth(3)
        s_out(2).start()

    with jax.named_scope("sent"):
        to_peer(x_buf.at[OWN], x_buf.at[PEER], x_send, x_recv.at[0]).wait_send()
        to_peer(a_buf.at[OWN], a_buf.at[PEER], a_send, a_recv.at[0]).wait_send()
        to_peer(wo_buf.at[OWN], wo_buf.at[PEER], wo_send, wo_recv).wait_send()
        some(mine_out, row_n - 1, m_send, m_recv).wait_send()
        when_equal(col_n - 1 - z_at, range(1, col_n), lambda n: some(total_in, n, r_send, r_recv).wait_send())
        starts = jnp.where((z_at > 0) | (x_at == 0), row_n - 1, row_n - 2)
        when_equal(starts, (row_n - 2, row_n - 1), lambda n: some(start_out, n, b_send, b_recv).wait_send())

        @pl.when(sp + 1 < n_sp)
        def _():
            h_out(sp + 1).wait_send()

    with jax.named_scope("tail"):
        for i in range(len(stat_pieces)):
            s_out(i).wait_recv()
        stats[...] = stat_own[...] + stat_peer[...]
        to_peer(stat_own, stat_peer, s_send, s_recv.at[0]).wait_send()


def finish(width, rows, resid, stats, gain, bias, out, o_buf, o_sem):
    pieces = resid.shape[0] // rows

    def leave(c):
        part = pl.ds(c * rows, rows)
        return pltpu.make_async_copy(o_buf.at[part], out.at[0, part], o_sem.at[c])

    first_half = lax.broadcasted_iota(jnp.int32, (rows, LANES), 1) < LANES // 2
    for c in range(pieces):
        part = slice(c * rows, (c + 1) * rows)
        both = stats[part, :]
        mean = jnp.sum(jnp.where(first_half, both, 0.0), axis=1, keepdims=True) / width
        square = jnp.sum(jnp.where(first_half, 0.0, both), axis=1, keepdims=True) / width
        inv = lax.rsqrt(square - mean * mean + EPS_NORM)
        o_buf[part, :] = ((resid[part, :] - mean) * inv * gain[...] + bias[...]).astype(BF16)
        leave(c).start()
    for c in range(pieces):
        leave(c).wait()


def solution(mesh):
    n_sp, n_tp = mesh.shape["sp"], mesh.shape["tp"]

    def local(stream, w_pool, w_query, w_forget, w_value, w_gate, mix, scale, bound, extra,
              gain, wo_pool, wo_rec, norm_gain, norm_bias):
        length, feats = stream.shape[1], stream.shape[2]
        chans, pool_w = bound.shape[0], scale.shape[0]
        heads = chans // DK
        blocks = length // BLOCK_ROWS
        rows_x = 256
        chunks = length // rows_x
        hbm = pl.BlockSpec(memory_space=pl.ANY)
        vmem = pl.BlockSpec(memory_space=pltpu.VMEM)
        dma = pltpu.SemaphoreType.DMA
        scratch = [
            pltpu.VMEM((n_tp, length, feats), BF16),
            pltpu.VMEM((5, n_tp, feats, chans), BF16),
            pltpu.VMEM((n_tp, pool_w + chans, feats), BF16),
            pltpu.VMEM((n_tp, length, pool_w + chans), BF16),
            pltpu.VMEM((length, chans), BF16),
            pltpu.VMEM((length, chans), BF16),
            pltpu.VMEM((length, chans), F32),
            pltpu.VMEM((blocks, DK, chans), F32),
            pltpu.VMEM((BLOCK_ROWS + length, pool_w), BF16),
            pltpu.VMEM((length, chans), BF16),
            pltpu.VMEM((length, chans), F32),
            pltpu.VMEM((length, chans), BF16),
            pltpu.VMEM((blocks, 8, chans), F32),
            pltpu.VMEM((DK, chans), F32),
            pltpu.VMEM((heads, DK + HALO, DK), BF16),
            pltpu.VMEM((heads, DK + HALO, DK), BF16),
            pltpu.VMEM((DK + HALO, DK), BF16),
            pltpu.VMEM((n_sp // heads, DK + HALO, DK), BF16),
            pltpu.VMEM((heads, DK, DK), BF16),
            pltpu.VMEM((heads, DK, DK), BF16),
            pltpu.VMEM((HALO, pool_w), BF16),
            pltpu.VMEM((length, LANES), F32),
            pltpu.VMEM((length, LANES), F32),
            pltpu.VMEM((mix.shape[0], BLOCK_ROWS, 2 * BLOCK_ROWS), BF16),
            pltpu.VMEM(mix.shape, BF16),
            pltpu.VMEM((1, pool_w), F32),
            pltpu.VMEM((1, chans), F32),
            pltpu.VMEM((heads, length), F32),
            pltpu.VMEM((1, DK), F32),
            dma((2,)), dma, dma((2,)), dma((5,)), dma, dma, dma, dma, dma((6,)),
            dma, dma, dma, dma, dma, dma, dma, dma, dma, dma((3,)), dma((5,)), pltpu.SemaphoreType.REGULAR,
        ]
        row = lambda x: x.reshape(1, -1)
        resid, stats = pl.pallas_call(
            functools.partial(mixer, n_sp, n_tp, rows_x),
            out_shape=(pltpu.VMEM((length, feats), F32), pltpu.VMEM((length, LANES), F32)),
            in_specs=[hbm] * 13,
            out_specs=(vmem, vmem),
            scratch_shapes=scratch,
            compiler_params=pltpu.CompilerParams(
                collective_id=0, has_side_effects=True, vmem_limit_bytes=LIMIT),
            name="mixer",
        )(stream, w_pool, w_query, w_forget, w_value, w_gate, mix, row(scale), row(bound), extra.T,
          row(gain), wo_pool, wo_rec)
        piece = 128
        pieces = length // piece
        return pl.pallas_call(
            functools.partial(finish, n_tp * feats, piece),
            out_shape=jax.ShapeDtypeStruct(stream.shape, BF16),
            in_specs=[vmem] * 4,
            out_specs=hbm,
            scratch_shapes=[pltpu.VMEM((length, feats), BF16), dma((pieces,))],
            compiler_params=pltpu.CompilerParams(vmem_limit_bytes=16 * 1024 * 1024),
            name="finish",
        )(resid, stats, row(norm_gain), row(norm_bias))

    placed = (
        P("fs", "sp", "tp"), P(None, "tp"), P(None, "tp"), P(None, "tp"), P(None, "tp"),
        P(None, "tp"), P("tp", None, None), P("tp"), P("tp"), P("sp", "tp"), P(),
        P("tp", None), P("tp", None), P("tp"), P("tp"),
    )
    return jax.shard_map(
        local, mesh=mesh, in_specs=placed, out_specs=P("fs", "sp", "tp"), check_vma=False
    )
```

```python
import functools

import jax
import jax.numpy as jnp
from jax import lax
from jax.experimental import pallas as pl
from jax.experimental.pallas import tpu as pltpu
from jax.sharding import PartitionSpec as P

DK = 128
BLOCK_ROWS = 128
GROUP_CH = 256
HALO = 16
LANES = 128

LIMIT = 56 * 1024 * 1024
ALPHA = 2.0**0.25
EPS_RMS = 1e-06
EPS_NORM = 1e-05
F32 = jnp.float32
BF16 = jnp.bfloat16
NT = (((1,), (1,)), ((), ()))
TN = (((0,), (0,)), ((), ()))
OWN, PEER = 0, 1


def dot(a, b, dims=None):
    if dims is None:
        return jnp.dot(a, b, preferred_element_type=F32)
    return lax.dot_general(a, b, dims, preferred_element_type=F32)


def half_sigmoid(x):
    return 0.5 + 0.5 * jnp.tanh(0.5 * x)


def mixer(
    n_sp, n_tp, rows_x,
    stream, w_pool, w_query, w_forget, w_value, w_gate,
    mix_in, scale_in, bound_in, extra_in, gain_in, wo_pool, wo_rec,
    r_buf, stats,
    x_buf, w_buf, wo_buf, a_buf, v_buf, u_buf, e_buf, t_buf, p_buf, q_buf, g_buf, f_buf,
    half_buf, state, mine_out, row_in, total_out, total_in, start_out, start_in, halo_in,
    stat_own, stat_peer, bands,
    mix, scale, bound, extra, gain,
    x_loc, x_send, x_recv, w_sem, wo_loc, wo_send, wo_recv, a_send, a_recv,
    m_send, m_recv, r_send, r_recv, b_send, b_recv, h_send, h_recv, s_send, s_recv, small_sem, ready,
):
    sp, tp = lax.axis_index("sp"), lax.axis_index("tp")
    peer = 1 - tp
    length, feats = stream.shape[1], stream.shape[2]
    chans = bound.shape[1]
    heads = chans // DK
    pool_w = scale.shape[1]
    groups = mix.shape[0]
    chunks = length // rows_x
    blocks = length // BLOCK_ROWS
    per = rows_x // BLOCK_ROWS
    row_n = heads
    col_n = n_sp // row_n
    x_at, z_at = lax.rem(sp, row_n), lax.div(sp, row_n)
    row0 = z_at * row_n
    mesh_id = pl.DeviceIdType.MESH

    def rows_of(c):
        return slice(c * rows_x, (c + 1) * rows_x)

    def block_of(b):
        return slice(b * BLOCK_ROWS, (b + 1) * BLOCK_ROWS)

    def head_of(h):
        return slice(h * DK, (h + 1) * DK)

    x_pieces = ((0, length // 2), (length // 2, length // 2))
    pool_pieces = ((2 * rows_x, length - 2 * rows_x), (rows_x, rows_x), (0, rows_x))
    rec_pieces = tuple((c * rows_x, rows_x) for c in range(chunks))
    stat_pieces = ((0, length - rows_x), (length - rows_x, rows_x))

    def to_peer(src, dst, send, recv):
        return pltpu.make_async_remote_copy(
            src, dst, send, recv, device_id={"tp": peer}, device_id_type=mesh_id)

    def to_sp(src, dst, send, recv, k):
        return pltpu.make_async_remote_copy(
            src, dst, send, recv, device_id={"sp": k}, device_id_type=mesh_id)

    def x_in(i):
        rows = pl.ds(*x_pieces[i])
        return pltpu.make_async_copy(stream.at[0, rows], x_buf.at[OWN, rows], x_loc.at[i])

    def x_out(i):
        rows = pl.ds(*x_pieces[i])
        return to_peer(x_buf.at[OWN, rows], x_buf.at[PEER, rows], x_send, x_recv.at[i])

    my_cols = pl.ds(pl.multiple_of(tp * feats, LANES), feats)
    peer_cols = pl.ds(pl.multiple_of(peer * feats, LANES), feats)
    wo_places = ((wo_pool, pl.ds(0, pool_w)), (wo_rec, pl.ds(pool_w, chans)))

    w_groups = {(0, OWN): 0, (1, OWN): 1, (0, PEER): 2, (1, PEER): 2, (2, OWN): 3, (2, PEER): 3}

    def w_in(i, side):
        src = (w_forget, w_value, w_pool, w_query, w_gate)[i]
        return pltpu.make_async_copy(
            src.at[my_cols if side == OWN else peer_cols], w_buf.at[i, side], w_sem.at[w_groups.get((i, side), 4)])

    def w_wait(ref, group):
        pltpu.make_async_copy(ref, ref, w_sem.at[group]).wait()

    def wo_in(i):
        src, place = wo_places[i]
        return pltpu.make_async_copy(src.at[:, my_cols], wo_buf.at[OWN, place], wo_loc)

    def wo_out(i):
        src, place = wo_places[i]
        return to_peer(src.at[:, peer_cols], wo_buf.at[PEER, place], wo_send, wo_recv)

    def pool_out(i):
        rows, cols = pl.ds(*pool_pieces[i]), wo_places[0][1]
        return to_peer(a_buf.at[OWN, rows, cols], a_buf.at[PEER, rows, cols], a_send, a_recv.at[i])

    def rec_out(i):
        rows, cols = pl.ds(*rec_pieces[i]), wo_places[1][1]
        return to_peer(a_buf.at[OWN, rows, cols], a_buf.at[PEER, rows, cols], a_send, a_recv.at[len(pool_pieces) + i])

    def mine_to(k, slot):
        return to_sp(mine_out.at[k], row_in.at[slot], m_send, m_recv, row0 + k)

    def total_to(k, slot):
        return to_sp(total_out, total_in.at[slot], r_send, r_recv, k * row_n + x_at)

    def start_to(k, slot):
        return to_sp(start_out.at[k], start_in.at[slot], b_send, b_recv, row0 + k)

    def some(ref, count, send, recv):
        return to_sp(ref.at[0:count], ref.at[0:count], send, recv, row0)

    def when_equal(value, counts, do):
        for n in counts:
            @pl.when(value == n)
            def _():
                do(n)

    def h_out(k):
        return to_sp(p_buf.at[pl.ds(BLOCK_ROWS + length - HALO, HALO)], halo_in, h_send, h_recv, k)

    def s_out(i):
        rows = pl.ds(*stat_pieces[i])
        return to_peer(stat_own.at[rows], stat_peer.at[rows], s_send, s_recv.at[i])

    def greet(k):
        pl.semaphore_signal(ready, inc=1, device_id={"sp": k}, device_id_type=mesh_id)

    def each(low, high, do):
        def step(k, _):
            do(k)
            return 0

        lax.fori_loop(low, high, step, 0)

    smalls = [
        pltpu.make_async_copy(src, dst, small_sem.at[i])
        for i, (src, dst) in enumerate(
            ((extra_in, extra), (bound_in, bound), (mix_in, mix), (scale_in, scale), (gain_in, gain)))
    ]

    smalls[0].start()
    x_in(0).start()
    w_in(0, OWN).start()
    x_in(1).start()

    barrier = pltpu.get_barrier_semaphore()
    pl.semaphore_signal(barrier, inc=1, device_id={"tp": peer}, device_id_type=mesh_id)

    def hail(k):
        pl.semaphore_signal(barrier, inc=1, device_id={"sp": k}, device_id_type=mesh_id)

    each(x_at + 1, row_n, lambda k: hail(row0 + k))
    each(z_at + 1, col_n, lambda k: hail(k * row_n + x_at))
    leads = (x_at == 0) & (z_at > 0)
    ends = (x_at == row_n - 1) & (z_at < col_n - 1)
    later = (row_n - 1 - x_at) + (col_n - 1 - z_at) + jnp.where(ends, 1, 0)
    p_buf[0:BLOCK_ROWS, :] = jnp.zeros((BLOCK_ROWS, pool_w), BF16)

    row_ids = lax.broadcasted_iota(jnp.int32, (BLOCK_ROWS, BLOCK_ROWS), 0)
    col_ids = lax.broadcasted_iota(jnp.int32, (BLOCK_ROWS, BLOCK_ROWS), 1)
    lower = row_ids >= col_ids

    state[...] = jnp.zeros_like(state)
    with jax.named_scope("entry"):
        pl.semaphore_wait(barrier, 1 + x_at + z_at)
    with jax.named_scope("x_in"):
        x_in(0).wait()
        x_out(0).start()
    w_in(1, OWN).start()
    w_in(0, PEER).start()
    w_in(1, PEER).start()
    for copy in smalls[1:]:
        copy.start()
    each(0, x_at, lambda k: greet(row0 + k))
    each(0, z_at, lambda k: greet(k * row_n + x_at))
    wide_rows = lax.broadcasted_iota(jnp.int32, (BLOCK_ROWS, 2 * BLOCK_ROWS), 0) + BLOCK_ROWS
    wide_cols = lax.broadcasted_iota(jnp.int32, (BLOCK_ROWS, 2 * BLOCK_ROWS), 1)
    back = wide_rows - wide_cols
    with jax.named_scope("bands"):
        for j in range(groups):
            window = jnp.left_shift(jnp.int32(2), tp * groups + j)
            share = 1.0 / window.astype(F32)
            inside = (back >= 0) & (back < window)
            bands[j] = (jnp.where(inside, share, 0.0) - jnp.where(back == 0, 1.0, 0.0)).astype(BF16)

    with jax.named_scope("x_in1"):
        x_in(1).wait()
        x_out(1).start()
    with jax.named_scope("w0"):
        w_wait(w_buf.at[0, OWN], 0)

    tri = jnp.where(lower, 1.0, 0.0).astype(BF16)
    tri_twice = jnp.concatenate([tri, tri], axis=1)

    def proj(i, c, part=slice(0, rows_x)):
        rows = slice(c * rows_x + part.start, c * rows_x + part.stop)
        return dot(x_buf[OWN, rows, :], w_buf[i, OWN]) + dot(x_buf[PEER, rows, :], w_buf[i, PEER])

    class Post:
        def __init__(self, c):
            self.blocks = [c * per + j for j in range(per)]
            self.weight, self.split, self.total = {}, {}, {}
            self.down, self.half = {}, {}

        def logs(self):
            open_part = 1.0 - bound[...]
            for b in self.blocks:
                f_in = f_buf[block_of(b), :].astype(F32)
                weight = open_part * (0.5 - 0.5 * jnp.tanh(0.5 * f_in))
                drop = jnp.concatenate([extra[:, block_of(b)], jnp.zeros((8 - heads, BLOCK_ROWS), F32)], axis=0).T
                drop = jnp.concatenate(
                    [jnp.broadcast_to(drop[:, h:h + 1], (BLOCK_ROWS, DK)) for h in range(heads)], axis=1)
                keep = jnp.log(1.0 - weight) + drop
                high = keep.astype(BF16)
                low = (keep - high.astype(F32)).astype(BF16)
                self.weight[b], self.split[b] = weight, jnp.concatenate([high, low], axis=0)

        def sums(self):
            for b in self.blocks:
                self.total[b] = dot(tri_twice, self.split[b])

        def exps(self):
            for b in self.blocks:
                total = self.total[b]
                middle = 0.5 * total[BLOCK_ROWS - 1:BLOCK_ROWS]
                e_buf[block_of(b), :] = jnp.exp(total - middle)
                down = (self.weight[b] * jnp.exp(middle - total)).astype(BF16)
                u_buf[block_of(b), :] = down
                half = jnp.exp(middle)
                half_buf[b] = jnp.broadcast_to(half, (8, chans))
                self.down[b], self.half[b] = down, half

        def states(self):
            for b in self.blocks:
                for h in range(heads):
                    lanes = head_of(h)
                    hh = self.half[b][:, lanes]
                    term = dot(v_buf[block_of(b), lanes], self.down[b][:, lanes], TN) * hh
                    t_buf[b, :, lanes] = term
                    state[:, lanes] = hh * hh * state[:, lanes] + term

    whole, upper, under = slice(0, rows_x), slice(0, rows_x // 2), slice(rows_x // 2, rows_x)

    def put_pool(c, part=whole):
        at = BLOCK_ROWS + c * rows_x
        p_buf[at + part.start:at + part.stop, :] = proj(2, c, part).astype(BF16)

    def own_half(i, some_chunks):
        for c in some_chunks:
            r_buf[rows_of(c), i * chans:(i + 1) * chans] = dot(x_buf[OWN, rows_of(c), :], w_buf[i, OWN])

    with jax.named_scope("own0"):
        own_half(0, range(chunks))
    with jax.named_scope("w1"):
        w_wait(w_buf.at[1, OWN], 1)
    for side in (OWN, PEER):
        w_in(2, side).start()
    with jax.named_scope("own1"):
        own_half(1, range(chunks))

    def rest(i, c):
        return (r_buf[rows_of(c), i * chans:(i + 1) * chans] + dot(x_buf[PEER, rows_of(c), :], w_buf[i, PEER])).astype(BF16)

    with jax.named_scope("x_recv0"):
        x_out(0).wait_recv()
        w_wait(w_buf.at[0:2, PEER], 2)
        for copy in smalls:
            copy.wait()
    for i in (3, 4):
        for side in (OWN, PEER):
            w_in(i, side).start()
    posts = [Post(c) for c in range(chunks)]

    def forget(c):
        f_buf[rows_of(c), :] = rest(0, c)

    def value(c):
        v_buf[rows_of(c), :] = rest(1, c)

    with jax.named_scope("first"):
        forget(0)
        posts[0].logs()
        forget(1)
        posts[0].sums()
        value(0)
        posts[0].exps()
    with jax.named_scope("x_recv1"):
        x_out(1).wait_recv()
        w_wait(w_buf.at[2], 3)
    for i in range(2):
        wo_in(i).start()
        wo_out(i).start()

    @pl.when(leads)
    def _():
        with jax.named_scope("lead"):
            pl.semaphore_wait(ready, later)
        greet(sp - 1)

    with jax.named_scope("first2"):
        posts[1].logs()
        forget(2)
        posts[0].states()
        posts[1].sums()
        value(1)
        posts[1].exps()
        posts[2].logs()
        forget(3)
        posts[1].states()
        posts[2].sums()
        value(2)
        posts[2].exps()
        posts[3].logs()
        posts[2].states()
        posts[3].sums()
        value(3)
        posts[3].exps()
        put_pool(3, under)
        posts[3].states()
        log_half = half_buf[0, 0:1]
        for b in range(1, blocks):
            log_half = log_half * half_buf[b, 0:1]
        keep_all = jnp.broadcast_to(log_half * log_half, (HALO, chans)).astype(BF16)
        for h in range(heads):
            mine_out[h, 0:DK, :] = state[:, head_of(h)].astype(BF16)
            mine_out[h, DK:DK + HALO, :] = keep_all[:, head_of(h)]

    @pl.when(jnp.logical_not(leads) & (sp + 1 < n_sp))
    def _():
        with jax.named_scope("later"):
            pl.semaphore_wait(ready, later)

    for step in range(1, row_n):
        mine_to(lax.rem(x_at + step, row_n), x_at).start()
    row_in[x_at] = mine_out[x_at]

    @pl.when(sp + 1 < n_sp)
    def _():
        h_out(sp + 1).start()

    with jax.named_scope("w34"):
        w_wait(w_buf.at[3:5], 4)
    with jax.named_scope("second"):
        put_pool(3, upper)
        for c in reversed(range(chunks - 1)):
            put_pool(c)

    def part_of(ref, at):
        return ref[at, 0:DK, :].astype(F32), ref[at, DK:DK + HALO, :].astype(F32)[0:1]

    def fold_row():
        with jax.named_scope("row_recv"):
            some(row_in, row_n - 1, m_send, m_recv).wait_recv()
        total, kept = part_of(row_in, 0)
        for k in range(1, row_n):
            term, keep = part_of(row_in, k)
            total = keep * total + term
            kept = kept * keep
        total_out[0:DK, :] = total.astype(BF16)
        total_out[DK:DK + HALO, :] = jnp.broadcast_to(kept, (HALO, DK)).astype(BF16)
        each(z_at + 1, col_n, lambda k: total_to(k, z_at).start())

    def fold_column():
        state[:, 0:DK] = jnp.zeros((DK, DK), F32)
        with jax.named_scope("col_recv"):
            when_equal(z_at, range(1, col_n), lambda n: some(total_in, n, r_send, r_recv).wait_recv())

        def take(k):
            term, keep = part_of(total_in, k)
            state[:, 0:DK] = keep * state[:, 0:DK] + term

        each(0, z_at, take)
        total = state[:, 0:DK]
        for k in range(row_n):
            start_out[k] = total.astype(BF16)
            if k + 1 < row_n:
                term, keep = part_of(row_in, k)
                total = keep * total + term
        for step in range(1, row_n):
            k = lax.rem(x_at + step, row_n)

            @pl.when(row0 + k > 0)
            def _():
                start_to(k, x_at).start()

        start_in[x_at] = start_out[x_at]

    count = lax.broadcasted_iota(jnp.int32, (BLOCK_ROWS, LANES), 0) + (sp * length + 1)

    gains = jnp.concatenate([gain[...]] * heads, axis=1)

    class Third:
        def __init__(self, c):
            self.c, self.rows = c, rows_of(c)
            self.blocks = [c * per + k for k in range(per)]

        def query(self):
            q_in = proj(3, self.c).astype(BF16).astype(F32)
            q_buf[self.rows, :] = (q_in * half_sigmoid(q_in) * e_buf[self.rows, :]).astype(BF16)

        def band(self):
            for b in self.blocks:
                near = p_buf[b * BLOCK_ROWS:(b + 2) * BLOCK_ROWS, :]
                for j in range(groups):
                    lanes = slice(j * GROUP_CH, (j + 1) * GROUP_CH)
                    if b:
                        a_buf[OWN, block_of(b), lanes] = dot(bands[j], near[:, lanes]).astype(BF16)
                        continue
                    window = jnp.left_shift(jnp.int32(2), tp * groups + j)
                    inside = jnp.where((back >= 0) & (back < window), 1.0, 0.0).astype(BF16)
                    share = 1.0 / jnp.minimum(count, window).astype(F32)
                    share = jnp.concatenate([share] * (GROUP_CH // LANES), axis=1)
                    sums = dot(inside, near[:, lanes])
                    a_buf[OWN, block_of(b), lanes] = (sums * share - near[BLOCK_ROWS:, lanes].astype(F32)).astype(BF16)

        def gates(self, part):
            rows = slice(self.rows.start + part.start, self.rows.start + part.stop)
            gate = proj(4, self.c, part).astype(BF16).astype(F32)
            g_buf[rows, :] = gate * half_sigmoid(gate) * gains

        def mixed(self):
            for j in range(groups):
                lanes = slice(j * GROUP_CH, (j + 1) * GROUP_CH)
                a_buf[OWN, self.rows, lanes] = (dot(a_buf[OWN, self.rows, lanes], mix[j]) * scale[:, lanes]).astype(BF16)

        def score(self):
            for b in self.blocks:
                for h in range(heads):
                    up, down = q_buf[block_of(b), head_of(h)], u_buf[block_of(b), head_of(h)]
                    f_buf[block_of(b), head_of(h)] = jnp.where(lower, dot(up, down, NT), 0.0).astype(BF16)

        def inner(self):
            for b in self.blocks:
                for h in range(heads):
                    at = block_of(b), head_of(h)
                    e_buf[at] = dot(f_buf[at], v_buf[at])

    parts = [Third(c) for c in range(chunks)]
    early = x_at >= row_n // 2

    def fold_at(stage, who):
        @pl.when(who)
        def _():
            stage()

    for c in reversed(range(chunks)):
        if c == 2:
            fold_at(fold_row, early)
        if c == 1:
            pool_out(0).start()
            fold_at(fold_row, jnp.logical_not(early))
        if c == 0:
            pool_out(1).start()
            fold_at(fold_column, x_at > 0)

            @pl.when(sp > 0)
            def _():
                with jax.named_scope("halo_recv"):
                    h_out(sp).wait_recv()
                p_buf[BLOCK_ROWS - HALO:BLOCK_ROWS, :] = halo_in[...]

        with jax.named_scope("third"):
            parts[c].query()
            if c + 1 < chunks:
                parts[c + 1].inner()
            parts[c].band()
            parts[c].gates(whole)
            parts[c].mixed()
            parts[c].score()
    pool_out(2).start()
    fold_at(fold_column, x_at == 0)

    with jax.named_scope("wo"):
        pltpu.make_async_copy(wo_buf.at[OWN], wo_buf.at[OWN], wo_loc).wait()
        to_peer(wo_buf.at[OWN], wo_buf.at[PEER], wo_send, wo_recv).wait_recv()
        pool_out(0).wait_recv()

    pool_at, rec_at = slice(0, pool_w), slice(pool_w, pool_w + chans)

    def pool_part(c):
        rows = rows_of(c)
        r_buf[rows, :] = (
            dot(a_buf[OWN, rows, pool_at], wo_buf[OWN, pool_at]) + dot(a_buf[PEER, rows, pool_at], wo_buf[PEER, pool_at])
            + ALPHA * x_buf[OWN, rows, :].astype(F32))

    with jax.named_scope("pool"):
        pool_part(chunks - 1)
        parts[0].inner()
        pool_part(chunks - 2)
    with jax.named_scope("pool_recv"):
        pool_out(1).wait_recv()
        pool_out(2).wait_recv()
    with jax.named_scope("pool"):
        pool_part(1)
        pool_part(0)

    @pl.when(sp > 0)
    def _():
        with jax.named_scope("start_recv"):
            some(start_in, row_n - 1, b_send, b_recv).wait_recv()

    @pl.when(sp > 0)
    def _():
        for h in range(heads):
            state[:, head_of(h)] = start_in[h].astype(F32)

    @pl.when(sp == 0)
    def _():
        state[...] = jnp.zeros_like(state)

    def fourth(c):
        for k in range(per):
            b = c * per + k
            half = half_buf[b, 0:1]
            before = state[...] * half
            carried = before.astype(BF16)
            state[...] = before * half + t_buf[b]
            for h in range(heads):
                lanes = head_of(h)
                raw = e_buf[block_of(b), lanes] + dot(q_buf[block_of(b), lanes], carried[:, lanes], NT)
                power = jnp.mean(raw * raw, axis=-1, keepdims=True)
                rec = raw * lax.rsqrt(power + EPS_RMS) * g_buf[block_of(b), lanes]
                a_buf[OWN, block_of(b), pool_w + h * DK:pool_w + (h + 1) * DK] = rec.astype(BF16)

    def rec_part(side, c):
        r_buf[rows_of(c), :] += dot(a_buf[side, rows_of(c), rec_at], wo_buf[side, rec_at])

    with jax.named_scope("fourth"):
        fourth(0)
        fourth(1)
        rec_out(0).start()
        rec_out(1).start()
    with jax.named_scope("fourth2"):
        fourth(2)
        rec_part(OWN, 0)
        rec_out(2).start()
        fourth(3)
        rec_part(OWN, 1)
        rec_out(3).start()

    def fold(x):
        acc = x[:, :LANES]
        for k in range(1, feats // LANES):
            acc = acc + x[:, k * LANES:(k + 1) * LANES]
        return acc

    first_half = lax.broadcasted_iota(jnp.int32, (rows_x, LANES), 1) < LANES // 2

    def fifth(c):
        rows = rows_of(c)
        resid = r_buf[rows, :] + dot(a_buf[PEER, rows, rec_at], wo_buf[PEER, rec_at])
        r_buf[rows, :] = resid
        sums, squares = fold(resid), fold(resid * resid)
        sums = sums + pltpu.roll(sums, LANES // 2, 1)
        squares = squares + pltpu.roll(squares, LANES // 2, 1)
        stat_own[rows, :] = jnp.where(first_half, sums, squares)

    with jax.named_scope("fifth"):
        rec_part(OWN, 2)
        rec_part(OWN, 3)
        for c in range(3):
            with jax.named_scope("rec_recv"):
                rec_out(c).wait_recv()
        for c in range(3):
            fifth(c)
        s_out(0).start()
    with jax.named_scope("fifth3"):
        with jax.named_scope("rec_recv"):
            rec_out(3).wait_recv()
        fifth(3)
        s_out(1).start()

    with jax.named_scope("sent"):
        to_peer(x_buf.at[OWN], x_buf.at[PEER], x_send, x_recv.at[0]).wait_send()
        to_peer(a_buf.at[OWN], a_buf.at[PEER], a_send, a_recv.at[0]).wait_send()
        to_peer(wo_buf.at[OWN], wo_buf.at[PEER], wo_send, wo_recv).wait_send()
        some(mine_out, row_n - 1, m_send, m_recv).wait_send()
        when_equal(col_n - 1 - z_at, range(1, col_n), lambda n: some(total_in, n, r_send, r_recv).wait_send())
        starts = jnp.where((z_at > 0) | (x_at == 0), row_n - 1, row_n - 2)
        when_equal(starts, (row_n - 2, row_n - 1), lambda n: some(start_out, n, b_send, b_recv).wait_send())

        @pl.when(sp + 1 < n_sp)
        def _():
            h_out(sp + 1).wait_send()

    with jax.named_scope("tail"):
        for i in range(len(stat_pieces)):
            s_out(i).wait_recv()
        stats[...] = stat_own[...] + stat_peer[...]
        to_peer(stat_own, stat_peer, s_send, s_recv.at[0]).wait_send()


def finish(width, rows, resid, stats, gain, bias, out, o_buf, o_sem):
    pieces = resid.shape[0] // rows

    def leave(c):
        part = pl.ds(c * rows, rows)
        return pltpu.make_async_copy(o_buf.at[part], out.at[0, part], o_sem.at[c])

    half = rows // 2
    first_half = lax.broadcasted_iota(jnp.int32, (half, LANES), 1) < LANES // 2
    for c in range(pieces):
        for k in range(2):
            part = slice(c * rows + k * half, c * rows + (k + 1) * half)
            both = stats[part, :]
            mean = jnp.sum(jnp.where(first_half, both, 0.0), axis=1, keepdims=True) * (1.0 / width)
            square = jnp.sum(jnp.where(first_half, 0.0, both), axis=1, keepdims=True) * (1.0 / width)
            inv = lax.rsqrt(square - mean * mean + EPS_NORM)
            shift = -mean * inv
            o_buf[part, :] = ((resid[part, :] * inv + shift) * gain[...] + bias[...]).astype(BF16)
        leave(c).start()
    for c in range(pieces):
        leave(c).wait()


def solution(mesh):
    n_sp, n_tp = mesh.shape["sp"], mesh.shape["tp"]

    def local(stream, w_pool, w_query, w_forget, w_value, w_gate, mix, scale, bound, extra,
              gain, wo_pool, wo_rec, norm_gain, norm_bias):
        length, feats = stream.shape[1], stream.shape[2]
        chans, pool_w = bound.shape[0], scale.shape[0]
        heads = chans // DK
        blocks = length // BLOCK_ROWS
        rows_x = 256
        chunks = length // rows_x
        hbm = pl.BlockSpec(memory_space=pl.ANY)
        vmem = pl.BlockSpec(memory_space=pltpu.VMEM)
        dma = pltpu.SemaphoreType.DMA
        scratch = [
            pltpu.VMEM((n_tp, length, feats), BF16),
            pltpu.VMEM((5, n_tp, feats, chans), BF16),
            pltpu.VMEM((n_tp, pool_w + chans, feats), BF16),
            pltpu.VMEM((n_tp, length, pool_w + chans), BF16),
            pltpu.VMEM((length, chans), BF16),
            pltpu.VMEM((length, chans), BF16),
            pltpu.VMEM((length, chans), F32),
            pltpu.VMEM((blocks, DK, chans), F32),
            pltpu.VMEM((BLOCK_ROWS + length, pool_w), BF16),
            pltpu.VMEM((length, chans), BF16),
            pltpu.VMEM((length, chans), F32),
            pltpu.VMEM((length, chans), BF16),
            pltpu.VMEM((blocks, 8, chans), F32),
            pltpu.VMEM((DK, chans), F32),
            pltpu.VMEM((heads, DK + HALO, DK), BF16),
            pltpu.VMEM((heads, DK + HALO, DK), BF16),
            pltpu.VMEM((DK + HALO, DK), BF16),
            pltpu.VMEM((n_sp // heads, DK + HALO, DK), BF16),
            pltpu.VMEM((heads, DK, DK), BF16),
            pltpu.VMEM((heads, DK, DK), BF16),
            pltpu.VMEM((HALO, pool_w), BF16),
            pltpu.VMEM((length, LANES), F32),
            pltpu.VMEM((length, LANES), F32),
            pltpu.VMEM((mix.shape[0], BLOCK_ROWS, 2 * BLOCK_ROWS), BF16),
            pltpu.VMEM(mix.shape, BF16),
            pltpu.VMEM((1, pool_w), F32),
            pltpu.VMEM((1, chans), F32),
            pltpu.VMEM((heads, length), F32),
            pltpu.VMEM((1, DK), F32),
            dma((2,)), dma, dma((2,)), dma((5,)), dma, dma, dma, dma, dma((7,)),
            dma, dma, dma, dma, dma, dma, dma, dma, dma, dma((2,)), dma((5,)), pltpu.SemaphoreType.REGULAR,
        ]
        row = lambda x: x.reshape(1, -1)
        resid, stats = pl.pallas_call(
            functools.partial(mixer, n_sp, n_tp, rows_x),
            out_shape=(pltpu.VMEM((length, feats), F32), pltpu.VMEM((length, LANES), F32)),
            in_specs=[hbm] * 13,
            out_specs=(vmem, vmem),
            scratch_shapes=scratch,
            compiler_params=pltpu.CompilerParams(
                collective_id=0, has_side_effects=True, vmem_limit_bytes=LIMIT),
            name="mixer",
        )(stream, w_pool, w_query, w_forget, w_value, w_gate, mix, row(scale), row(bound), extra.T,
          row(gain), wo_pool, wo_rec)
        piece = 128
        pieces = length // piece
        return pl.pallas_call(
            functools.partial(finish, n_tp * feats, piece),
            out_shape=jax.ShapeDtypeStruct(stream.shape, BF16),
            in_specs=[vmem] * 4,
            out_specs=hbm,
            scratch_shapes=[pltpu.VMEM((length, feats), BF16), dma((pieces,))],
            compiler_params=pltpu.CompilerParams(vmem_limit_bytes=16 * 1024 * 1024),
            name="finish",
        )(resid, stats, row(norm_gain), row(norm_bias))

    placed = (
        P("fs", "sp", "tp"), P(None, "tp"), P(None, "tp"), P(None, "tp"), P(None, "tp"),
        P(None, "tp"), P("tp", None, None), P("tp"), P("tp"), P("sp", "tp"), P(),
        P("tp", None), P("tp", None), P("tp"), P("tp"),
    )
    return jax.shard_map(
        local, mesh=mesh, in_specs=placed, out_specs=P("fs", "sp", "tp"), check_vma=False
    )
```

```python
import functools

import jax
import jax.numpy as jnp
from jax import lax
from jax.experimental import pallas as pl
from jax.experimental.pallas import tpu as pltpu
from jax.sharding import PartitionSpec as P

DK = 128
BLOCK_ROWS = 128
GROUP_CH = 256
HALO = 16
LANES = 128

LIMIT = 56 * 1024 * 1024
ALPHA = 2.0**0.25
EPS_RMS = 1e-06
EPS_NORM = 1e-05
F32 = jnp.float32
BF16 = jnp.bfloat16
NT = (((1,), (1,)), ((), ()))
TN = (((0,), (0,)), ((), ()))
OWN, PEER = 0, 1


def dot(a, b, dims=None):
    if dims is None:
        return jnp.dot(a, b, preferred_element_type=F32)
    return lax.dot_general(a, b, dims, preferred_element_type=F32)


def half_sigmoid(x):
    return 0.5 + 0.5 * jnp.tanh(0.5 * x)


def mixer(
    n_sp, n_tp, rows_x,
    stream, w_pool, w_query, w_forget, w_value, w_gate,
    mix_in, scale_in, bound_in, extra_in, gain_in, wo_pool, wo_rec,
    r_buf, stats,
    x_buf, w_buf, wo_buf, a_buf, v_buf, u_buf, e_buf, t_buf, p_buf, q_buf, g_buf, f_buf,
    half_buf, state, mine_out, row_in, total_out, total_in, start_out, start_in, halo_in,
    stat_own, stat_peer, bands,
    mix, scale, bound, extra, gain,
    x_loc, x_send, x_recv, w_sem, wo_loc, wo_send, wo_recv, a_send, a_recv,
    m_send, m_recv, r_send, r_recv, b_send, b_recv, h_send, h_recv, s_send, s_recv, small_sem, ready,
):
    sp, tp = lax.axis_index("sp"), lax.axis_index("tp")
    peer = 1 - tp
    length, feats = stream.shape[1], stream.shape[2]
    chans = bound.shape[1]
    heads = chans // DK
    pool_w = scale.shape[1]
    groups = mix.shape[0]
    chunks = length // rows_x
    blocks = length // BLOCK_ROWS
    per = rows_x // BLOCK_ROWS
    row_n = heads
    col_n = n_sp // row_n
    x_at, z_at = lax.rem(sp, row_n), lax.div(sp, row_n)
    row0 = z_at * row_n
    mesh_id = pl.DeviceIdType.MESH

    def rows_of(c):
        return slice(c * rows_x, (c + 1) * rows_x)

    def block_of(b):
        return slice(b * BLOCK_ROWS, (b + 1) * BLOCK_ROWS)

    def head_of(h):
        return slice(h * DK, (h + 1) * DK)

    x_pieces = ((0, length // 2), (length // 2, length // 2))
    pool_pieces = ((2 * rows_x, length - 2 * rows_x), (rows_x, rows_x), (0, rows_x))
    rec_pieces = tuple((c * rows_x, rows_x) for c in range(chunks))
    stat_pieces = ((0, length - rows_x), (length - rows_x, rows_x))

    def to_peer(src, dst, send, recv):
        return pltpu.make_async_remote_copy(
            src, dst, send, recv, device_id={"tp": peer}, device_id_type=mesh_id)

    def to_sp(src, dst, send, recv, k):
        return pltpu.make_async_remote_copy(
            src, dst, send, recv, device_id={"sp": k}, device_id_type=mesh_id)

    def x_in(i):
        rows = pl.ds(*x_pieces[i])
        return pltpu.make_async_copy(stream.at[0, rows], x_buf.at[OWN, rows], x_loc.at[i])

    def x_out(i):
        rows = pl.ds(*x_pieces[i])
        return to_peer(x_buf.at[OWN, rows], x_buf.at[PEER, rows], x_send, x_recv.at[i])

    my_cols = pl.ds(pl.multiple_of(tp * feats, LANES), feats)
    peer_cols = pl.ds(pl.multiple_of(peer * feats, LANES), feats)
    wo_places = ((wo_pool, pl.ds(0, pool_w)), (wo_rec, pl.ds(pool_w, chans)))

    w_groups = {(0, OWN): 0, (1, OWN): 1, (0, PEER): 2, (1, PEER): 2, (2, OWN): 3, (2, PEER): 3}

    def w_in(i, side):
        src = (w_forget, w_value, w_pool, w_query, w_gate)[i]
        return pltpu.make_async_copy(
            src.at[my_cols if side == OWN else peer_cols], w_buf.at[i, side], w_sem.at[w_groups.get((i, side), 4)])

    def w_wait(ref, group):
        pltpu.make_async_copy(ref, ref, w_sem.at[group]).wait()

    def wo_in(i):
        src, place = wo_places[i]
        return pltpu.make_async_copy(src.at[:, my_cols], wo_buf.at[OWN, place], wo_loc)

    def wo_out(i):
        src, place = wo_places[i]
        return to_peer(src.at[:, peer_cols], wo_buf.at[PEER, place], wo_send, wo_recv)

    def pool_out(i):
        rows, cols = pl.ds(*pool_pieces[i]), wo_places[0][1]
        return to_peer(a_buf.at[OWN, rows, cols], a_buf.at[PEER, rows, cols], a_send, a_recv.at[i])

    def rec_out(i):
        rows, cols = pl.ds(*rec_pieces[i]), wo_places[1][1]
        return to_peer(a_buf.at[OWN, rows, cols], a_buf.at[PEER, rows, cols], a_send, a_recv.at[len(pool_pieces) + i])

    def mine_to(k, slot):
        return to_sp(mine_out.at[k], row_in.at[slot], m_send, m_recv, row0 + k)

    def total_to(k, slot):
        return to_sp(total_out, total_in.at[slot], r_send, r_recv, k * row_n + x_at)

    def start_to(k, slot):
        return to_sp(start_out.at[k], start_in.at[slot], b_send, b_recv, row0 + k)

    def some(ref, count, send, recv):
        return to_sp(ref.at[0:count], ref.at[0:count], send, recv, row0)

    def when_equal(value, counts, do):
        for n in counts:
            @pl.when(value == n)
            def _():
                do(n)

    def h_out(k):
        return to_sp(p_buf.at[pl.ds(BLOCK_ROWS + length - HALO, HALO)], halo_in, h_send, h_recv, k)

    def s_out(i):
        rows = pl.ds(*stat_pieces[i])
        return to_peer(stat_own.at[rows], stat_peer.at[rows], s_send, s_recv.at[i])

    def greet(k):
        pl.semaphore_signal(ready, inc=1, device_id={"sp": k}, device_id_type=mesh_id)

    def each(low, high, do):
        def step(k, _):
            do(k)
            return 0

        lax.fori_loop(low, high, step, 0)

    smalls = [
        pltpu.make_async_copy(src, dst, small_sem.at[i])
        for i, (src, dst) in enumerate(
            ((extra_in, extra), (bound_in, bound), (mix_in, mix), (scale_in, scale), (gain_in, gain)))
    ]

    smalls[0].start()
    x_in(0).start()
    w_in(0, OWN).start()
    x_in(1).start()

    barrier = pltpu.get_barrier_semaphore()
    pl.semaphore_signal(barrier, inc=1, device_id={"tp": peer}, device_id_type=mesh_id)

    def hail(k):
        pl.semaphore_signal(barrier, inc=1, device_id={"sp": k}, device_id_type=mesh_id)

    each(x_at + 1, row_n, lambda k: hail(row0 + k))
    each(z_at + 1, col_n, lambda k: hail(k * row_n + x_at))
    leads = (x_at == 0) & (z_at > 0)
    ends = (x_at == row_n - 1) & (z_at < col_n - 1)
    later = (row_n - 1 - x_at) + (col_n - 1 - z_at) + jnp.where(ends, 1, 0)
    p_buf[0:BLOCK_ROWS, :] = jnp.zeros((BLOCK_ROWS, pool_w), BF16)

    row_ids = lax.broadcasted_iota(jnp.int32, (BLOCK_ROWS, BLOCK_ROWS), 0)
    col_ids = lax.broadcasted_iota(jnp.int32, (BLOCK_ROWS, BLOCK_ROWS), 1)
    lower = row_ids >= col_ids

    state[...] = jnp.zeros_like(state)
    with jax.named_scope("entry"):
        pl.semaphore_wait(barrier, 1 + x_at + z_at)
    with jax.named_scope("x_in"):
        x_in(0).wait()
        x_out(0).start()
    w_in(1, OWN).start()
    w_in(0, PEER).start()
    w_in(1, PEER).start()
    for copy in smalls[1:]:
        copy.start()
    each(0, x_at, lambda k: greet(row0 + k))
    each(0, z_at, lambda k: greet(k * row_n + x_at))
    wide_rows = lax.broadcasted_iota(jnp.int32, (BLOCK_ROWS, 2 * BLOCK_ROWS), 0) + BLOCK_ROWS
    wide_cols = lax.broadcasted_iota(jnp.int32, (BLOCK_ROWS, 2 * BLOCK_ROWS), 1)
    back = wide_rows - wide_cols
    with jax.named_scope("bands"):
        for j in range(groups):
            window = jnp.left_shift(jnp.int32(2), tp * groups + j)
            share = 1.0 / window.astype(F32)
            inside = (back >= 0) & (back < window)
            bands[j] = (jnp.where(inside, share, 0.0) - jnp.where(back == 0, 1.0, 0.0)).astype(BF16)

    with jax.named_scope("x_in1"):
        x_in(1).wait()
        x_out(1).start()
    with jax.named_scope("w0"):
        w_wait(w_buf.at[0, OWN], 0)

    tri = jnp.where(lower, 1.0, 0.0).astype(BF16)
    tri_twice = jnp.concatenate([tri, tri], axis=1)

    def proj(i, c, part=slice(0, rows_x)):
        rows = slice(c * rows_x + part.start, c * rows_x + part.stop)
        return dot(x_buf[OWN, rows, :], w_buf[i, OWN]) + dot(x_buf[PEER, rows, :], w_buf[i, PEER])

    class Post:
        def __init__(self, c):
            self.blocks = [c * per + j for j in range(per)]
            self.weight, self.split, self.total = {}, {}, {}
            self.down, self.half = {}, {}

        def logs(self):
            open_part = 1.0 - bound[...]
            for b in self.blocks:
                f_in = f_buf[block_of(b), :].astype(F32)
                weight = open_part * (0.5 - 0.5 * jnp.tanh(0.5 * f_in))
                drop = jnp.concatenate([extra[:, block_of(b)], jnp.zeros((8 - heads, BLOCK_ROWS), F32)], axis=0).T
                drop = jnp.concatenate(
                    [jnp.broadcast_to(drop[:, h:h + 1], (BLOCK_ROWS, DK)) for h in range(heads)], axis=1)
                keep = jnp.log(1.0 - weight) + drop
                high = keep.astype(BF16)
                low = (keep - high.astype(F32)).astype(BF16)
                self.weight[b], self.split[b] = weight, jnp.concatenate([high, low], axis=0)

        def sums(self):
            for b in self.blocks:
                self.total[b] = dot(tri_twice, self.split[b])

        def exps(self):
            for b in self.blocks:
                total = self.total[b]
                middle = 0.5 * total[BLOCK_ROWS - 1:BLOCK_ROWS]
                e_buf[block_of(b), :] = jnp.exp(total - middle)
                down = (self.weight[b] * jnp.exp(middle - total)).astype(BF16)
                u_buf[block_of(b), :] = down
                half = jnp.exp(middle)
                half_buf[b] = jnp.broadcast_to(half, (8, chans))
                self.down[b], self.half[b] = down, half

        def states(self):
            for b in self.blocks:
                for h in range(heads):
                    lanes = head_of(h)
                    hh = self.half[b][:, lanes]
                    term = dot(v_buf[block_of(b), lanes], self.down[b][:, lanes], TN) * hh
                    t_buf[b, :, lanes] = term
                    state[:, lanes] = hh * hh * state[:, lanes] + term

    whole, upper, under = slice(0, rows_x), slice(0, rows_x // 2), slice(rows_x // 2, rows_x)

    def put_pool(c, part=whole):
        at = BLOCK_ROWS + c * rows_x
        p_buf[at + part.start:at + part.stop, :] = proj(2, c, part).astype(BF16)

    def own_half(i, some_chunks):
        for c in some_chunks:
            r_buf[rows_of(c), i * chans:(i + 1) * chans] = dot(x_buf[OWN, rows_of(c), :], w_buf[i, OWN])

    with jax.named_scope("own0"):
        own_half(0, range(chunks))
    with jax.named_scope("w1"):
        w_wait(w_buf.at[1, OWN], 1)
    for side in (OWN, PEER):
        w_in(2, side).start()
    with jax.named_scope("own1"):
        own_half(1, range(chunks))

    def rest(i, c):
        return (r_buf[rows_of(c), i * chans:(i + 1) * chans] + dot(x_buf[PEER, rows_of(c), :], w_buf[i, PEER])).astype(BF16)

    with jax.named_scope("x_recv0"):
        x_out(0).wait_recv()
        w_wait(w_buf.at[0:2, PEER], 2)
        for copy in smalls:
            copy.wait()
    for i in (3, 4):
        for side in (OWN, PEER):
            w_in(i, side).start()
    posts = [Post(c) for c in range(chunks)]

    def forget(c):
        f_buf[rows_of(c), :] = rest(0, c)

    def value(c):
        v_buf[rows_of(c), :] = rest(1, c)

    with jax.named_scope("first"):
        forget(0)
        posts[0].logs()
        forget(1)
        posts[0].sums()
        value(0)
        posts[0].exps()
    with jax.named_scope("x_recv1"):
        x_out(1).wait_recv()
        w_wait(w_buf.at[2], 3)
    for i in range(2):
        wo_in(i).start()
        wo_out(i).start()

    @pl.when(leads)
    def _():
        with jax.named_scope("lead"):
            pl.semaphore_wait(ready, later)
        greet(sp - 1)

    with jax.named_scope("first2"):
        posts[1].logs()
        forget(2)
        posts[0].states()
        posts[1].sums()
        value(1)
        posts[1].exps()
        posts[2].logs()
        forget(3)
        posts[1].states()
        posts[2].sums()
        value(2)
        posts[2].exps()
        posts[3].logs()
        posts[2].states()
        posts[3].sums()
        value(3)
        posts[3].exps()
        put_pool(3, under)
        posts[3].states()
        log_half = half_buf[0, 0:1]
        for b in range(1, blocks):
            log_half = log_half * half_buf[b, 0:1]
        keep_all = jnp.broadcast_to(log_half * log_half, (HALO, chans)).astype(BF16)
        for h in range(heads):
            mine_out[h, 0:DK, :] = state[:, head_of(h)].astype(BF16)
            mine_out[h, DK:DK + HALO, :] = keep_all[:, head_of(h)]

    @pl.when(jnp.logical_not(leads) & (sp + 1 < n_sp))
    def _():
        with jax.named_scope("later"):
            pl.semaphore_wait(ready, later)

    for k in range(row_n):
        @pl.when(x_at != k)
        def _():
            mine_to(k, x_at).start()
    row_in[x_at] = mine_out[x_at]

    @pl.when(sp + 1 < n_sp)
    def _():
        h_out(sp + 1).start()

    with jax.named_scope("w34"):
        w_wait(w_buf.at[3:5], 4)
    with jax.named_scope("second"):
        put_pool(3, upper)
        for c in reversed(range(chunks - 1)):
            put_pool(c)

    def part_of(ref, at):
        return ref[at, 0:DK, :].astype(F32), ref[at, DK:DK + HALO, :].astype(F32)[0:1]

    def fold_row():
        with jax.named_scope("row_recv"):
            some(row_in, row_n - 1, m_send, m_recv).wait_recv()
        total, kept = part_of(row_in, 0)
        for k in range(1, row_n):
            term, keep = part_of(row_in, k)
            total = keep * total + term
            kept = kept * keep
        total_out[0:DK, :] = total.astype(BF16)
        total_out[DK:DK + HALO, :] = jnp.broadcast_to(kept, (HALO, DK)).astype(BF16)
        each(z_at + 1, col_n, lambda k: total_to(k, z_at).start())

    def fold_column():
        state[:, 0:DK] = jnp.zeros((DK, DK), F32)
        with jax.named_scope("col_recv"):
            when_equal(z_at, range(1, col_n), lambda n: some(total_in, n, r_send, r_recv).wait_recv())

        def take(k):
            term, keep = part_of(total_in, k)
            state[:, 0:DK] = keep * state[:, 0:DK] + term

        each(0, z_at, take)
        total = state[:, 0:DK]
        for k in range(row_n):
            start_out[k] = total.astype(BF16)
            if k + 1 < row_n:
                term, keep = part_of(row_in, k)
                total = keep * total + term
        for k in range(row_n):
            @pl.when((x_at != k) & (row0 + k > 0))
            def _():
                start_to(k, x_at).start()

        start_in[x_at] = start_out[x_at]

    count = lax.broadcasted_iota(jnp.int32, (BLOCK_ROWS, LANES), 0) + (sp * length + 1)

    gains = jnp.concatenate([gain[...]] * heads, axis=1)

    class Third:
        def __init__(self, c):
            self.c, self.rows = c, rows_of(c)
            self.blocks = [c * per + k for k in range(per)]

        def query(self):
            q_in = proj(3, self.c).astype(BF16).astype(F32)
            q_buf[self.rows, :] = (q_in * half_sigmoid(q_in) * e_buf[self.rows, :]).astype(BF16)

        def band(self):
            for b in self.blocks:
                near = p_buf[b * BLOCK_ROWS:(b + 2) * BLOCK_ROWS, :]
                for j in range(groups):
                    lanes = slice(j * GROUP_CH, (j + 1) * GROUP_CH)
                    if b:
                        a_buf[OWN, block_of(b), lanes] = dot(bands[j], near[:, lanes]).astype(BF16)
                        continue
                    window = jnp.left_shift(jnp.int32(2), tp * groups + j)
                    inside = jnp.where((back >= 0) & (back < window), 1.0, 0.0).astype(BF16)
                    share = 1.0 / jnp.minimum(count, window).astype(F32)
                    share = jnp.concatenate([share] * (GROUP_CH // LANES), axis=1)
                    sums = dot(inside, near[:, lanes])
                    a_buf[OWN, block_of(b), lanes] = (sums * share - near[BLOCK_ROWS:, lanes].astype(F32)).astype(BF16)

        def gates(self, part):
            rows = slice(self.rows.start + part.start, self.rows.start + part.stop)
            gate = proj(4, self.c, part).astype(BF16).astype(F32)
            g_buf[rows, :] = gate * half_sigmoid(gate) * gains

        def mixed(self):
            for j in range(groups):
                lanes = slice(j * GROUP_CH, (j + 1) * GROUP_CH)
                a_buf[OWN, self.rows, lanes] = (dot(a_buf[OWN, self.rows, lanes], mix[j]) * scale[:, lanes]).astype(BF16)

        def score(self):
            for b in self.blocks:
                for h in range(heads):
                    up, down = q_buf[block_of(b), head_of(h)], u_buf[block_of(b), head_of(h)]
                    f_buf[block_of(b), head_of(h)] = jnp.where(lower, dot(up, down, NT), 0.0).astype(BF16)

        def inner(self):
            for b in self.blocks:
                for h in range(heads):
                    at = block_of(b), head_of(h)
                    e_buf[at] = dot(f_buf[at], v_buf[at])

    parts = [Third(c) for c in range(chunks)]
    early = x_at >= row_n // 2

    def fold_at(stage, who):
        @pl.when(who)
        def _():
            stage()

    for c in reversed(range(chunks)):
        if c == 2:
            fold_at(fold_row, early)
        if c == 1:
            pool_out(0).start()
            fold_at(fold_row, jnp.logical_not(early))
            fold_at(fold_column, early)
        if c == 0:
            pool_out(1).start()
            fold_at(fold_column, x_at == 1)

            @pl.when(sp > 0)
            def _():
                with jax.named_scope("halo_recv"):
                    h_out(sp).wait_recv()
                p_buf[BLOCK_ROWS - HALO:BLOCK_ROWS, :] = halo_in[...]

        with jax.named_scope("third"):
            parts[c].query()
            if c + 1 < chunks:
                parts[c + 1].inner()
            parts[c].band()
            parts[c].gates(whole)
            parts[c].mixed()
            parts[c].score()
    pool_out(2).start()
    fold_at(fold_column, x_at == 0)

    with jax.named_scope("wo"):
        pltpu.make_async_copy(wo_buf.at[OWN], wo_buf.at[OWN], wo_loc).wait()
        to_peer(wo_buf.at[OWN], wo_buf.at[PEER], wo_send, wo_recv).wait_recv()
        pool_out(0).wait_recv()

    pool_at, rec_at = slice(0, pool_w), slice(pool_w, pool_w + chans)

    def pool_part(c):
        rows = rows_of(c)
        r_buf[rows, :] = (
            dot(a_buf[OWN, rows, pool_at], wo_buf[OWN, pool_at]) + dot(a_buf[PEER, rows, pool_at], wo_buf[PEER, pool_at])
            + ALPHA * x_buf[OWN, rows, :].astype(F32))

    with jax.named_scope("pool"):
        pool_part(chunks - 1)
        parts[0].inner()
        pool_part(chunks - 2)
    with jax.named_scope("pool_recv"):
        pool_out(1).wait_recv()
        pool_out(2).wait_recv()
    with jax.named_scope("pool"):
        pool_part(1)
        pool_part(0)

    @pl.when(sp > 0)
    def _():
        with jax.named_scope("start_recv"):
            some(start_in, row_n - 1, b_send, b_recv).wait_recv()

    @pl.when(sp > 0)
    def _():
        for h in range(heads):
            state[:, head_of(h)] = start_in[h].astype(F32)

    @pl.when(sp == 0)
    def _():
        state[...] = jnp.zeros_like(state)

    def fourth(c):
        for k in range(per):
            b = c * per + k
            half = half_buf[b, 0:1]
            before = state[...] * half
            carried = before.astype(BF16)
            state[...] = before * half + t_buf[b]
            for h in range(heads):
                lanes = head_of(h)
                raw = e_buf[block_of(b), lanes] + dot(q_buf[block_of(b), lanes], carried[:, lanes], NT)
                power = jnp.mean(raw * raw, axis=-1, keepdims=True)
                rec = raw * lax.rsqrt(power + EPS_RMS) * g_buf[block_of(b), lanes]
                a_buf[OWN, block_of(b), pool_w + h * DK:pool_w + (h + 1) * DK] = rec.astype(BF16)

    def rec_part(side, c):
        r_buf[rows_of(c), :] += dot(a_buf[side, rows_of(c), rec_at], wo_buf[side, rec_at])

    with jax.named_scope("fourth"):
        fourth(0)
        fourth(1)
        rec_out(0).start()
        rec_out(1).start()
    with jax.named_scope("fourth2"):
        fourth(2)
        rec_part(OWN, 0)
        rec_out(2).start()
        fourth(3)
        rec_part(OWN, 1)
        rec_out(3).start()

    def fold(x):
        acc = x[:, :LANES]
        for k in range(1, feats // LANES):
            acc = acc + x[:, k * LANES:(k + 1) * LANES]
        return acc

    first_half = lax.broadcasted_iota(jnp.int32, (rows_x, LANES), 1) < LANES // 2

    def fifth(c):
        rows = rows_of(c)
        resid = r_buf[rows, :] + dot(a_buf[PEER, rows, rec_at], wo_buf[PEER, rec_at])
        r_buf[rows, :] = resid
        sums, squares = fold(resid), fold(resid * resid)
        sums = sums + pltpu.roll(sums, LANES // 2, 1)
        squares = squares + pltpu.roll(squares, LANES // 2, 1)
        stat_own[rows, :] = jnp.where(first_half, sums, squares)

    with jax.named_scope("fifth"):
        rec_part(OWN, 2)
        rec_part(OWN, 3)
        for c in range(3):
            with jax.named_scope("rec_recv"):
                rec_out(c).wait_recv()
        for c in range(3):
            fifth(c)
        s_out(0).start()
    with jax.named_scope("fifth3"):
        with jax.named_scope("rec_recv"):
            rec_out(3).wait_recv()
        fifth(3)
        s_out(1).start()

    with jax.named_scope("sent"):
        to_peer(x_buf.at[OWN], x_buf.at[PEER], x_send, x_recv.at[0]).wait_send()
        to_peer(a_buf.at[OWN], a_buf.at[PEER], a_send, a_recv.at[0]).wait_send()
        to_peer(wo_buf.at[OWN], wo_buf.at[PEER], wo_send, wo_recv).wait_send()
        some(mine_out, row_n - 1, m_send, m_recv).wait_send()
        when_equal(col_n - 1 - z_at, range(1, col_n), lambda n: some(total_in, n, r_send, r_recv).wait_send())
        starts = jnp.where((z_at > 0) | (x_at == 0), row_n - 1, row_n - 2)
        when_equal(starts, (row_n - 2, row_n - 1), lambda n: some(start_out, n, b_send, b_recv).wait_send())

        @pl.when(sp + 1 < n_sp)
        def _():
            h_out(sp + 1).wait_send()

    with jax.named_scope("tail"):
        for i in range(len(stat_pieces)):
            s_out(i).wait_recv()
        stats[...] = stat_own[...] + stat_peer[...]
        to_peer(stat_own, stat_peer, s_send, s_recv.at[0]).wait_send()


def finish(width, rows, resid, stats, gain, bias, out, o_buf, o_sem):
    pieces = resid.shape[0] // rows

    def leave(c):
        part = pl.ds(c * rows, rows)
        return pltpu.make_async_copy(o_buf.at[part], out.at[0, part], o_sem.at[c])

    half = rows // 2
    first_half = lax.broadcasted_iota(jnp.int32, (half, LANES), 1) < LANES // 2
    for c in range(pieces):
        for k in range(2):
            part = slice(c * rows + k * half, c * rows + (k + 1) * half)
            both = stats[part, :]
            mean = jnp.sum(jnp.where(first_half, both, 0.0), axis=1, keepdims=True) * (1.0 / width)
            square = jnp.sum(jnp.where(first_half, 0.0, both), axis=1, keepdims=True) * (1.0 / width)
            inv = lax.rsqrt(square - mean * mean + EPS_NORM)
            shift = -mean * inv
            o_buf[part, :] = ((resid[part, :] * inv + shift) * gain[...] + bias[...]).astype(BF16)
        leave(c).start()
    for c in range(pieces):
        leave(c).wait()


def solution(mesh):
    n_sp, n_tp = mesh.shape["sp"], mesh.shape["tp"]

    def local(stream, w_pool, w_query, w_forget, w_value, w_gate, mix, scale, bound, extra,
              gain, wo_pool, wo_rec, norm_gain, norm_bias):
        length, feats = stream.shape[1], stream.shape[2]
        chans, pool_w = bound.shape[0], scale.shape[0]
        heads = chans // DK
        blocks = length // BLOCK_ROWS
        rows_x = 256
        chunks = length // rows_x
        hbm = pl.BlockSpec(memory_space=pl.ANY)
        vmem = pl.BlockSpec(memory_space=pltpu.VMEM)
        dma = pltpu.SemaphoreType.DMA
        scratch = [
            pltpu.VMEM((n_tp, length, feats), BF16),
            pltpu.VMEM((5, n_tp, feats, chans), BF16),
            pltpu.VMEM((n_tp, pool_w + chans, feats), BF16),
            pltpu.VMEM((n_tp, length, pool_w + chans), BF16),
            pltpu.VMEM((length, chans), BF16),
            pltpu.VMEM((length, chans), BF16),
            pltpu.VMEM((length, chans), F32),
            pltpu.VMEM((blocks, DK, chans), F32),
            pltpu.VMEM((BLOCK_ROWS + length, pool_w), BF16),
            pltpu.VMEM((length, chans), BF16),
            pltpu.VMEM((length, chans), F32),
            pltpu.VMEM((length, chans), BF16),
            pltpu.VMEM((blocks, 8, chans), F32),
            pltpu.VMEM((DK, chans), F32),
            pltpu.VMEM((heads, DK + HALO, DK), BF16),
            pltpu.VMEM((heads, DK + HALO, DK), BF16),
            pltpu.VMEM((DK + HALO, DK), BF16),
            pltpu.VMEM((n_sp // heads, DK + HALO, DK), BF16),
            pltpu.VMEM((heads, DK, DK), BF16),
            pltpu.VMEM((heads, DK, DK), BF16),
            pltpu.VMEM((HALO, pool_w), BF16),
            pltpu.VMEM((length, LANES), F32),
            pltpu.VMEM((length, LANES), F32),
            pltpu.VMEM((mix.shape[0], BLOCK_ROWS, 2 * BLOCK_ROWS), BF16),
            pltpu.VMEM(mix.shape, BF16),
            pltpu.VMEM((1, pool_w), F32),
            pltpu.VMEM((1, chans), F32),
            pltpu.VMEM((heads, length), F32),
            pltpu.VMEM((1, DK), F32),
            dma((2,)), dma, dma((2,)), dma((5,)), dma, dma, dma, dma, dma((7,)),
            dma, dma, dma, dma, dma, dma, dma, dma, dma, dma((2,)), dma((5,)), pltpu.SemaphoreType.REGULAR,
        ]
        row = lambda x: x.reshape(1, -1)
        resid, stats = pl.pallas_call(
            functools.partial(mixer, n_sp, n_tp, rows_x),
            out_shape=(pltpu.VMEM((length, feats), F32), pltpu.VMEM((length, LANES), F32)),
            in_specs=[hbm] * 13,
            out_specs=(vmem, vmem),
            scratch_shapes=scratch,
            compiler_params=pltpu.CompilerParams(
                collective_id=0, has_side_effects=True, vmem_limit_bytes=LIMIT),
            name="mixer",
        )(stream, w_pool, w_query, w_forget, w_value, w_gate, mix, row(scale), row(bound), extra.T,
          row(gain), wo_pool, wo_rec)
        piece = 128
        pieces = length // piece
        return pl.pallas_call(
            functools.partial(finish, n_tp * feats, piece),
            out_shape=jax.ShapeDtypeStruct(stream.shape, BF16),
            in_specs=[vmem] * 4,
            out_specs=hbm,
            scratch_shapes=[pltpu.VMEM((length, feats), BF16), dma((pieces,))],
            compiler_params=pltpu.CompilerParams(vmem_limit_bytes=16 * 1024 * 1024),
            name="finish",
        )(resid, stats, row(norm_gain), row(norm_bias))

    placed = (
        P("fs", "sp", "tp"), P(None, "tp"), P(None, "tp"), P(None, "tp"), P(None, "tp"),
        P(None, "tp"), P("tp", None, None), P("tp"), P("tp"), P("sp", "tp"), P(),
        P("tp", None), P("tp", None), P("tp"), P("tp"),
    )
    return jax.shard_map(
        local, mesh=mesh, in_specs=placed, out_specs=P("fs", "sp", "tp"), check_vma=False
    )
```

```python
import functools

import jax
import jax.numpy as jnp
from jax import lax
from jax.experimental import pallas as pl
from jax.experimental.pallas import tpu as pltpu
from jax.sharding import PartitionSpec as P

DK = 128
BLOCK_ROWS = 128
GROUP_CH = 256
HALO = 16
LANES = 128

LIMIT = 56 * 1024 * 1024
ALPHA = 2.0**0.25
EPS_RMS = 1e-06
EPS_NORM = 1e-05
F32 = jnp.float32
BF16 = jnp.bfloat16
NT = (((1,), (1,)), ((), ()))
TN = (((0,), (0,)), ((), ()))
OWN, PEER = 0, 1


def dot(a, b, dims=None):
    if dims is None:
        return jnp.dot(a, b, preferred_element_type=F32)
    return lax.dot_general(a, b, dims, preferred_element_type=F32)


def half_sigmoid(x):
    return 0.5 + 0.5 * jnp.tanh(0.5 * x)


def mixer(
    n_sp, n_tp, rows_x,
    stream, w_pool, w_query, w_forget, w_value, w_gate,
    mix_in, scale_in, bound_in, extra_in, gain_in, wo_pool, wo_rec,
    r_buf, stats,
    x_buf, w_buf, wo_buf, a_buf, v_buf, u_buf, e_buf, t_buf, p_buf, q_buf, g_buf, f_buf,
    half_buf, state, mine_out, row_in, total_out, total_in, start_out, start_in, halo_in,
    stat_own, stat_peer, bands,
    mix, scale, bound, extra, gain,
    x_loc, x_send, x_recv, w_sem, wo_loc, wo_send, wo_recv, a_send, a_recv,
    m_send, m_recv, r_send, r_recv, b_send, b_recv, h_send, h_recv, s_send, s_recv, small_sem, ready,
):
    sp, tp = lax.axis_index("sp"), lax.axis_index("tp")
    peer = 1 - tp
    length, feats = stream.shape[1], stream.shape[2]
    chans = bound.shape[1]
    heads = chans // DK
    pool_w = scale.shape[1]
    groups = mix.shape[0]
    chunks = length // rows_x
    blocks = length // BLOCK_ROWS
    per = rows_x // BLOCK_ROWS
    row_n = heads
    col_n = n_sp // row_n
    x_at, z_at = lax.rem(sp, row_n), lax.div(sp, row_n)
    row0 = z_at * row_n
    mesh_id = pl.DeviceIdType.MESH

    def rows_of(c):
        return slice(c * rows_x, (c + 1) * rows_x)

    def block_of(b):
        return slice(b * BLOCK_ROWS, (b + 1) * BLOCK_ROWS)

    def head_of(h):
        return slice(h * DK, (h + 1) * DK)

    x_pieces = ((0, length // 2), (length // 2, length // 2))
    pool_pieces = ((2 * rows_x, length - 2 * rows_x), (rows_x, rows_x), (0, rows_x))
    rec_pieces = tuple((c * rows_x, rows_x) for c in range(chunks))
    stat_pieces = ((0, length - rows_x), (length - rows_x, rows_x))

    def to_peer(src, dst, send, recv):
        return pltpu.make_async_remote_copy(
            src, dst, send, recv, device_id={"tp": peer}, device_id_type=mesh_id)

    def to_sp(src, dst, send, recv, k):
        return pltpu.make_async_remote_copy(
            src, dst, send, recv, device_id={"sp": k}, device_id_type=mesh_id)

    def x_in(i):
        rows = pl.ds(*x_pieces[i])
        return pltpu.make_async_copy(stream.at[0, rows], x_buf.at[OWN, rows], x_loc.at[i])

    def x_out(i):
        rows = pl.ds(*x_pieces[i])
        return to_peer(x_buf.at[OWN, rows], x_buf.at[PEER, rows], x_send, x_recv.at[i])

    my_cols = pl.ds(pl.multiple_of(tp * feats, LANES), feats)
    peer_cols = pl.ds(pl.multiple_of(peer * feats, LANES), feats)
    wo_places = ((wo_pool, pl.ds(0, pool_w)), (wo_rec, pl.ds(pool_w, chans)))

    w_groups = {(0, OWN): 0, (1, OWN): 1, (0, PEER): 2, (1, PEER): 2, (2, OWN): 3, (2, PEER): 3}

    def w_in(i, side):
        src = (w_forget, w_value, w_pool, w_query, w_gate)[i]
        return pltpu.make_async_copy(
            src.at[my_cols if side == OWN else peer_cols], w_buf.at[i, side], w_sem.at[w_groups.get((i, side), 4)])

    def w_wait(ref, group):
        pltpu.make_async_copy(ref, ref, w_sem.at[group]).wait()

    def wo_in(i):
        src, place = wo_places[i]
        return pltpu.make_async_copy(src.at[:, my_cols], wo_buf.at[OWN, place], wo_loc)

    def wo_out(i):
        src, place = wo_places[i]
        return to_peer(src.at[:, peer_cols], wo_buf.at[PEER, place], wo_send, wo_recv)

    def pool_out(i):
        rows, cols = pl.ds(*pool_pieces[i]), wo_places[0][1]
        return to_peer(a_buf.at[OWN, rows, cols], a_buf.at[PEER, rows, cols], a_send, a_recv.at[i])

    def rec_out(i):
        rows, cols = pl.ds(*rec_pieces[i]), wo_places[1][1]
        return to_peer(a_buf.at[OWN, rows, cols], a_buf.at[PEER, rows, cols], a_send, a_recv.at[len(pool_pieces) + i])

    def mine_to(k, slot):
        return to_sp(mine_out.at[k], row_in.at[slot], m_send, m_recv, row0 + k)

    def total_to(k, slot):
        return to_sp(total_out, total_in.at[slot], r_send, r_recv, k * row_n + x_at)

    def start_to(k, slot):
        return to_sp(start_out.at[k], start_in.at[slot], b_send, b_recv, row0 + k)

    def some(ref, count, send, recv):
        return to_sp(ref.at[0:count], ref.at[0:count], send, recv, row0)

    def when_equal(value, counts, do):
        for n in counts:
            @pl.when(value == n)
            def _():
                do(n)

    def h_out(k):
        return to_sp(p_buf.at[pl.ds(BLOCK_ROWS + length - HALO, HALO)], halo_in, h_send, h_recv, k)

    def s_out(i):
        rows = pl.ds(*stat_pieces[i])
        return to_peer(stat_own.at[rows], stat_peer.at[rows], s_send, s_recv.at[i])

    def greet(k):
        pl.semaphore_signal(ready, inc=1, device_id={"sp": k}, device_id_type=mesh_id)

    def each(low, high, do):
        def step(k, _):
            do(k)
            return 0

        lax.fori_loop(low, high, step, 0)

    smalls = [
        pltpu.make_async_copy(src, dst, small_sem.at[i])
        for i, (src, dst) in enumerate(
            ((extra_in, extra), (bound_in, bound), (mix_in, mix), (scale_in, scale), (gain_in, gain)))
    ]

    smalls[0].start()
    x_in(0).start()
    w_in(0, OWN).start()
    x_in(1).start()

    barrier = pltpu.get_barrier_semaphore()
    pl.semaphore_signal(barrier, inc=1, device_id={"tp": peer}, device_id_type=mesh_id)

    def hail(k):
        pl.semaphore_signal(barrier, inc=1, device_id={"sp": k}, device_id_type=mesh_id)

    each(x_at + 1, row_n, lambda k: hail(row0 + k))
    each(z_at + 1, col_n, lambda k: hail(k * row_n + x_at))
    leads = (x_at == 0) & (z_at > 0)
    ends = (x_at == row_n - 1) & (z_at < col_n - 1)
    later = (row_n - 1 - x_at) + (col_n - 1 - z_at) + jnp.where(ends, 1, 0)
    p_buf[0:BLOCK_ROWS, :] = jnp.zeros((BLOCK_ROWS, pool_w), BF16)

    row_ids = lax.broadcasted_iota(jnp.int32, (BLOCK_ROWS, BLOCK_ROWS), 0)
    col_ids = lax.broadcasted_iota(jnp.int32, (BLOCK_ROWS, BLOCK_ROWS), 1)
    lower = row_ids >= col_ids

    state[...] = jnp.zeros_like(state)
    with jax.named_scope("entry"):
        pl.semaphore_wait(barrier, 1 + x_at + z_at)
    with jax.named_scope("x_in"):
        x_in(0).wait()
        x_out(0).start()
    w_in(1, OWN).start()
    w_in(0, PEER).start()
    w_in(1, PEER).start()
    for copy in smalls[1:]:
        copy.start()
    each(0, x_at, lambda k: greet(row0 + k))
    each(0, z_at, lambda k: greet(k * row_n + x_at))
    wide_rows = lax.broadcasted_iota(jnp.int32, (BLOCK_ROWS, 2 * BLOCK_ROWS), 0) + BLOCK_ROWS
    wide_cols = lax.broadcasted_iota(jnp.int32, (BLOCK_ROWS, 2 * BLOCK_ROWS), 1)
    back = wide_rows - wide_cols
    with jax.named_scope("bands"):
        for j in range(groups):
            window = jnp.left_shift(jnp.int32(2), tp * groups + j)
            share = 1.0 / window.astype(F32)
            inside = (back >= 0) & (back < window)
            bands[j] = (jnp.where(inside, share, 0.0) - jnp.where(back == 0, 1.0, 0.0)).astype(BF16)

    with jax.named_scope("x_in1"):
        x_in(1).wait()
        x_out(1).start()
    with jax.named_scope("w0"):
        w_wait(w_buf.at[0, OWN], 0)

    tri = jnp.where(lower, 1.0, 0.0).astype(BF16)
    tri_twice = jnp.concatenate([tri, tri], axis=1)

    def proj(i, c, part=slice(0, rows_x)):
        rows = slice(c * rows_x + part.start, c * rows_x + part.stop)
        return dot(x_buf[OWN, rows, :], w_buf[i, OWN]) + dot(x_buf[PEER, rows, :], w_buf[i, PEER])

    class Post:
        def __init__(self, c):
            self.blocks = [c * per + j for j in range(per)]
            self.weight, self.split, self.total = {}, {}, {}
            self.down, self.half = {}, {}

        def logs(self):
            open_part = 1.0 - bound[...]
            for b in self.blocks:
                f_in = f_buf[block_of(b), :].astype(F32)
                weight = open_part * (0.5 - 0.5 * jnp.tanh(0.5 * f_in))
                drop = jnp.concatenate([extra[:, block_of(b)], jnp.zeros((8 - heads, BLOCK_ROWS), F32)], axis=0).T
                drop = jnp.concatenate(
                    [jnp.broadcast_to(drop[:, h:h + 1], (BLOCK_ROWS, DK)) for h in range(heads)], axis=1)
                keep = jnp.log(1.0 - weight) + drop
                high = keep.astype(BF16)
                low = (keep - high.astype(F32)).astype(BF16)
                self.weight[b], self.split[b] = weight, jnp.concatenate([high, low], axis=0)

        def sums(self):
            for b in self.blocks:
                self.total[b] = dot(tri_twice, self.split[b])

        def exps(self):
            for b in self.blocks:
                total = self.total[b]
                middle = 0.5 * total[BLOCK_ROWS - 1:BLOCK_ROWS]
                e_buf[block_of(b), :] = jnp.exp(total - middle)
                down = (self.weight[b] * jnp.exp(middle - total)).astype(BF16)
                u_buf[block_of(b), :] = down
                half = jnp.exp(middle)
                half_buf[b] = jnp.broadcast_to(half, (8, chans))
                self.down[b], self.half[b] = down, half

        def states(self):
            for b in self.blocks:
                for h in range(heads):
                    lanes = head_of(h)
                    hh = self.half[b][:, lanes]
                    term = dot(v_buf[block_of(b), lanes], self.down[b][:, lanes], TN) * hh
                    t_buf[b, :, lanes] = term
                    state[:, lanes] = hh * hh * state[:, lanes] + term

    whole, upper, under = slice(0, rows_x), slice(0, rows_x // 2), slice(rows_x // 2, rows_x)

    def put_pool(c, part=whole):
        at = BLOCK_ROWS + c * rows_x
        p_buf[at + part.start:at + part.stop, :] = proj(2, c, part).astype(BF16)

    def own_half(i, some_chunks):
        for c in some_chunks:
            r_buf[rows_of(c), i * chans:(i + 1) * chans] = dot(x_buf[OWN, rows_of(c), :], w_buf[i, OWN])

    with jax.named_scope("own0"):
        own_half(0, range(chunks))
    with jax.named_scope("w1"):
        w_wait(w_buf.at[1, OWN], 1)
    for side in (OWN, PEER):
        w_in(2, side).start()
    with jax.named_scope("own1"):
        own_half(1, range(chunks))

    def rest(i, c):
        return (r_buf[rows_of(c), i * chans:(i + 1) * chans] + dot(x_buf[PEER, rows_of(c), :], w_buf[i, PEER])).astype(BF16)

    with jax.named_scope("x_recv0"):
        x_out(0).wait_recv()
        w_wait(w_buf.at[0:2, PEER], 2)
        for copy in smalls:
            copy.wait()
    for i in (3, 4):
        for side in (OWN, PEER):
            w_in(i, side).start()
    posts = [Post(c) for c in range(chunks)]

    def forget(c):
        f_buf[rows_of(c), :] = rest(0, c)

    def value(c):
        v_buf[rows_of(c), :] = rest(1, c)

    with jax.named_scope("first"):
        forget(0)
        posts[0].logs()
        forget(1)
        posts[0].sums()
        value(0)
        posts[0].exps()
    with jax.named_scope("x_recv1"):
        x_out(1).wait_recv()
        w_wait(w_buf.at[2], 3)
    for i in range(2):
        wo_in(i).start()
        wo_out(i).start()

    @pl.when(leads)
    def _():
        with jax.named_scope("lead"):
            pl.semaphore_wait(ready, later)
        greet(sp - 1)

    with jax.named_scope("first2"):
        posts[1].logs()
        forget(2)
        posts[0].states()
        posts[1].sums()
        value(1)
        posts[1].exps()
        posts[2].logs()
        forget(3)
        posts[1].states()
        posts[2].sums()
        value(2)
        posts[2].exps()
        posts[3].logs()
        posts[2].states()
        posts[3].sums()
        value(3)
        posts[3].exps()
        put_pool(3, under)
        posts[3].states()
        log_half = half_buf[0, 0:1]
        for b in range(1, blocks):
            log_half = log_half * half_buf[b, 0:1]
        keep_all = jnp.broadcast_to(log_half * log_half, (HALO, chans)).astype(BF16)
        for h in range(heads):
            mine_out[h, 0:DK, :] = state[:, head_of(h)].astype(BF16)
            mine_out[h, DK:DK + HALO, :] = keep_all[:, head_of(h)]

    @pl.when(jnp.logical_not(leads) & (sp + 1 < n_sp))
    def _():
        with jax.named_scope("later"):
            pl.semaphore_wait(ready, later)

    for k in range(row_n):
        @pl.when(x_at != k)
        def _():
            mine_to(k, x_at).start()
    row_in[x_at] = mine_out[x_at]

    @pl.when(sp + 1 < n_sp)
    def _():
        h_out(sp + 1).start()

    with jax.named_scope("w34"):
        w_wait(w_buf.at[3:5], 4)
    with jax.named_scope("second"):
        put_pool(3, upper)
        for c in reversed(range(chunks - 1)):
            put_pool(c)

    def part_of(ref, at):
        return ref[at, 0:DK, :].astype(F32), ref[at, DK:DK + HALO, :].astype(F32)[0:1]

    def fold_row():
        with jax.named_scope("row_recv"):
            some(row_in, row_n - 1, m_send, m_recv).wait_recv()
        total, kept = part_of(row_in, 0)
        for k in range(1, row_n):
            term, keep = part_of(row_in, k)
            total = keep * total + term
            kept = kept * keep
        total_out[0:DK, :] = total.astype(BF16)
        total_out[DK:DK + HALO, :] = jnp.broadcast_to(kept, (HALO, DK)).astype(BF16)
        each(z_at + 1, col_n, lambda k: total_to(k, z_at).start())

    def fold_column():
        state[:, 0:DK] = jnp.zeros((DK, DK), F32)
        with jax.named_scope("col_recv"):
            when_equal(z_at, range(1, col_n), lambda n: some(total_in, n, r_send, r_recv).wait_recv())

        def take(k):
            term, keep = part_of(total_in, k)
            state[:, 0:DK] = keep * state[:, 0:DK] + term

        each(0, z_at, take)
        total = state[:, 0:DK]
        for k in range(row_n):
            start_out[k] = total.astype(BF16)
            if k + 1 < row_n:
                term, keep = part_of(row_in, k)
                total = keep * total + term
        for k in range(row_n):
            @pl.when((x_at != k) & (row0 + k > 0))
            def _():
                start_to(k, x_at).start()

        start_in[x_at] = start_out[x_at]

    count = lax.broadcasted_iota(jnp.int32, (BLOCK_ROWS, LANES), 0) + (sp * length + 1)

    gains = jnp.concatenate([gain[...]] * heads, axis=1)

    class Third:
        def __init__(self, c):
            self.c, self.rows = c, rows_of(c)
            self.blocks = [c * per + k for k in range(per)]

        def query(self):
            q_in = proj(3, self.c).astype(BF16).astype(F32)
            q_buf[self.rows, :] = (q_in * half_sigmoid(q_in) * e_buf[self.rows, :]).astype(BF16)

        def band(self):
            for b in self.blocks:
                near = p_buf[b * BLOCK_ROWS:(b + 2) * BLOCK_ROWS, :]
                for j in range(groups):
                    lanes = slice(j * GROUP_CH, (j + 1) * GROUP_CH)
                    if b:
                        a_buf[OWN, block_of(b), lanes] = dot(bands[j], near[:, lanes]).astype(BF16)
                        continue
                    window = jnp.left_shift(jnp.int32(2), tp * groups + j)
                    inside = jnp.where((back >= 0) & (back < window), 1.0, 0.0).astype(BF16)
                    share = 1.0 / jnp.minimum(count, window).astype(F32)
                    share = jnp.concatenate([share] * (GROUP_CH // LANES), axis=1)
                    sums = dot(inside, near[:, lanes])
                    a_buf[OWN, block_of(b), lanes] = (sums * share - near[BLOCK_ROWS:, lanes].astype(F32)).astype(BF16)

        def gates(self, part):
            rows = slice(self.rows.start + part.start, self.rows.start + part.stop)
            gate = proj(4, self.c, part).astype(BF16).astype(F32)
            g_buf[rows, :] = gate * half_sigmoid(gate) * gains

        def mixed(self):
            for j in range(groups):
                lanes = slice(j * GROUP_CH, (j + 1) * GROUP_CH)
                a_buf[OWN, self.rows, lanes] = (dot(a_buf[OWN, self.rows, lanes], mix[j]) * scale[:, lanes]).astype(BF16)

        def score(self):
            for b in self.blocks:
                for h in range(heads):
                    up, down = q_buf[block_of(b), head_of(h)], u_buf[block_of(b), head_of(h)]
                    f_buf[block_of(b), head_of(h)] = jnp.where(lower, dot(up, down, NT), 0.0).astype(BF16)

        def inner(self):
            for b in self.blocks:
                for h in range(heads):
                    at = block_of(b), head_of(h)
                    e_buf[at] = dot(f_buf[at], v_buf[at])

    parts = [Third(c) for c in range(chunks)]
    early = x_at >= row_n // 2

    def fold_at(stage, who):
        @pl.when(who)
        def _():
            stage()

    for c in reversed(range(chunks)):
        if c == 2:
            fold_at(fold_row, early)
        if c == 1:
            pool_out(0).start()
            fold_at(fold_row, jnp.logical_not(early))
            fold_at(fold_column, early)
        if c == 0:
            pool_out(1).start()
            fold_at(fold_column, x_at == 1)

            @pl.when(sp > 0)
            def _():
                with jax.named_scope("halo_recv"):
                    h_out(sp).wait_recv()
                p_buf[BLOCK_ROWS - HALO:BLOCK_ROWS, :] = halo_in[...]

        with jax.named_scope("third"):
            parts[c].query()
            if c + 1 < chunks:
                parts[c + 1].inner()
            parts[c].band()
            parts[c].gates(whole)
            parts[c].mixed()
            parts[c].score()
    pool_out(2).start()
    fold_at(fold_column, x_at == 0)

    with jax.named_scope("wo"):
        pltpu.make_async_copy(wo_buf.at[OWN], wo_buf.at[OWN], wo_loc).wait()
        to_peer(wo_buf.at[OWN], wo_buf.at[PEER], wo_send, wo_recv).wait_recv()
        pool_out(0).wait_recv()

    pool_at, rec_at = slice(0, pool_w), slice(pool_w, pool_w + chans)

    def pool_part(c):
        rows = rows_of(c)
        r_buf[rows, :] = (
            dot(a_buf[OWN, rows, pool_at], wo_buf[OWN, pool_at]) + dot(a_buf[PEER, rows, pool_at], wo_buf[PEER, pool_at])
            + ALPHA * x_buf[OWN, rows, :].astype(F32))

    with jax.named_scope("pool"):
        pool_part(chunks - 1)
        parts[0].inner()
        pool_part(chunks - 2)
    with jax.named_scope("pool_recv"):
        pool_out(1).wait_recv()
    with jax.named_scope("pool"):
        pool_part(1)

    @pl.when(sp > 0)
    def _():
        with jax.named_scope("start_recv"):
            some(start_in, row_n - 1, b_send, b_recv).wait_recv()

    @pl.when(sp > 0)
    def _():
        for h in range(heads):
            state[:, head_of(h)] = start_in[h].astype(F32)

    @pl.when(sp == 0)
    def _():
        state[...] = jnp.zeros_like(state)

    def fourth(c):
        for k in range(per):
            b = c * per + k
            half = half_buf[b, 0:1]
            before = state[...] * half
            carried = before.astype(BF16)
            state[...] = before * half + t_buf[b]
            for h in range(heads):
                lanes = head_of(h)
                raw = e_buf[block_of(b), lanes] + dot(q_buf[block_of(b), lanes], carried[:, lanes], NT)
                power = jnp.mean(raw * raw, axis=-1, keepdims=True)
                rec = raw * lax.rsqrt(power + EPS_RMS) * g_buf[block_of(b), lanes]
                a_buf[OWN, block_of(b), pool_w + h * DK:pool_w + (h + 1) * DK] = rec.astype(BF16)

    def rec_part(side, c):
        r_buf[rows_of(c), :] += dot(a_buf[side, rows_of(c), rec_at], wo_buf[side, rec_at])

    with jax.named_scope("fourth"):
        fourth(0)
        fourth(1)
        rec_out(0).start()
        rec_out(1).start()
    with jax.named_scope("fourth2"):
        fourth(2)
        rec_part(OWN, 1)
        rec_out(2).start()
        fourth(3)
        rec_part(OWN, 2)
        rec_out(3).start()

    def fold(x):
        acc = x[:, :LANES]
        for k in range(1, feats // LANES):
            acc = acc + x[:, k * LANES:(k + 1) * LANES]
        return acc

    first_half = lax.broadcasted_iota(jnp.int32, (rows_x, LANES), 1) < LANES // 2

    def fifth(c):
        rows = rows_of(c)
        resid = r_buf[rows, :] + dot(a_buf[PEER, rows, rec_at], wo_buf[PEER, rec_at])
        r_buf[rows, :] = resid
        sums, squares = fold(resid), fold(resid * resid)
        sums = sums + pltpu.roll(sums, LANES // 2, 1)
        squares = squares + pltpu.roll(squares, LANES // 2, 1)
        stat_own[rows, :] = jnp.where(first_half, sums, squares)

    with jax.named_scope("fifth"):
        pool_out(2).wait_recv()
        pool_part(0)
        rec_part(OWN, 0)
        rec_part(OWN, 3)
        for c in range(3):
            with jax.named_scope("rec_recv"):
                rec_out(c).wait_recv()
        for c in range(3):
            fifth(c)
        s_out(0).start()
    with jax.named_scope("fifth3"):
        with jax.named_scope("rec_recv"):
            rec_out(3).wait_recv()
        fifth(3)
        s_out(1).start()

    with jax.named_scope("sent"):
        to_peer(x_buf.at[OWN], x_buf.at[PEER], x_send, x_recv.at[0]).wait_send()
        to_peer(a_buf.at[OWN], a_buf.at[PEER], a_send, a_recv.at[0]).wait_send()
        to_peer(wo_buf.at[OWN], wo_buf.at[PEER], wo_send, wo_recv).wait_send()
        some(mine_out, row_n - 1, m_send, m_recv).wait_send()
        when_equal(col_n - 1 - z_at, range(1, col_n), lambda n: some(total_in, n, r_send, r_recv).wait_send())
        starts = jnp.where((z_at > 0) | (x_at == 0), row_n - 1, row_n - 2)
        when_equal(starts, (row_n - 2, row_n - 1), lambda n: some(start_out, n, b_send, b_recv).wait_send())

        @pl.when(sp + 1 < n_sp)
        def _():
            h_out(sp + 1).wait_send()

    with jax.named_scope("tail"):
        for i in range(len(stat_pieces)):
            s_out(i).wait_recv()
        stats[...] = stat_own[...] + stat_peer[...]
        to_peer(stat_own, stat_peer, s_send, s_recv.at[0]).wait_send()


def finish(width, rows, resid, stats, gain, bias, out, o_buf, o_sem):
    pieces = resid.shape[0] // rows

    def leave(c):
        part = pl.ds(c * rows, rows)
        return pltpu.make_async_copy(o_buf.at[part], out.at[0, part], o_sem.at[c])

    half = rows // 2
    first_half = lax.broadcasted_iota(jnp.int32, (half, LANES), 1) < LANES // 2
    for c in range(pieces):
        for k in range(2):
            part = slice(c * rows + k * half, c * rows + (k + 1) * half)
            both = stats[part, :]
            mean = jnp.sum(jnp.where(first_half, both, 0.0), axis=1, keepdims=True) * (1.0 / width)
            square = jnp.sum(jnp.where(first_half, 0.0, both), axis=1, keepdims=True) * (1.0 / width)
            inv = lax.rsqrt(square - mean * mean + EPS_NORM)
            shift = -mean * inv
            o_buf[part, :] = ((resid[part, :] * inv + shift) * gain[...] + bias[...]).astype(BF16)
        leave(c).start()
    for c in range(pieces):
        leave(c).wait()


def solution(mesh):
    n_sp, n_tp = mesh.shape["sp"], mesh.shape["tp"]

    def local(stream, w_pool, w_query, w_forget, w_value, w_gate, mix, scale, bound, extra,
              gain, wo_pool, wo_rec, norm_gain, norm_bias):
        length, feats = stream.shape[1], stream.shape[2]
        chans, pool_w = bound.shape[0], scale.shape[0]
        heads = chans // DK
        blocks = length // BLOCK_ROWS
        rows_x = 256
        chunks = length // rows_x
        hbm = pl.BlockSpec(memory_space=pl.ANY)
        vmem = pl.BlockSpec(memory_space=pltpu.VMEM)
        dma = pltpu.SemaphoreType.DMA
        scratch = [
            pltpu.VMEM((n_tp, length, feats), BF16),
            pltpu.VMEM((5, n_tp, feats, chans), BF16),
            pltpu.VMEM((n_tp, pool_w + chans, feats), BF16),
            pltpu.VMEM((n_tp, length, pool_w + chans), BF16),
            pltpu.VMEM((length, chans), BF16),
            pltpu.VMEM((length, chans), BF16),
            pltpu.VMEM((length, chans), F32),
            pltpu.VMEM((blocks, DK, chans), F32),
            pltpu.VMEM((BLOCK_ROWS + length, pool_w), BF16),
            pltpu.VMEM((length, chans), BF16),
            pltpu.VMEM((length, chans), F32),
            pltpu.VMEM((length, chans), BF16),
            pltpu.VMEM((blocks, 8, chans), F32),
            pltpu.VMEM((DK, chans), F32),
            pltpu.VMEM((heads, DK + HALO, DK), BF16),
            pltpu.VMEM((heads, DK + HALO, DK), BF16),
            pltpu.VMEM((DK + HALO, DK), BF16),
            pltpu.VMEM((n_sp // heads, DK + HALO, DK), BF16),
            pltpu.VMEM((heads, DK, DK), BF16),
            pltpu.VMEM((heads, DK, DK), BF16),
            pltpu.VMEM((HALO, pool_w), BF16),
            pltpu.VMEM((length, LANES), F32),
            pltpu.VMEM((length, LANES), F32),
            pltpu.VMEM((mix.shape[0], BLOCK_ROWS, 2 * BLOCK_ROWS), BF16),
            pltpu.VMEM(mix.shape, BF16),
            pltpu.VMEM((1, pool_w), F32),
            pltpu.VMEM((1, chans), F32),
            pltpu.VMEM((heads, length), F32),
            pltpu.VMEM((1, DK), F32),
            dma((2,)), dma, dma((2,)), dma((5,)), dma, dma, dma, dma, dma((7,)),
            dma, dma, dma, dma, dma, dma, dma, dma, dma, dma((2,)), dma((5,)), pltpu.SemaphoreType.REGULAR,
        ]
        row = lambda x: x.reshape(1, -1)
        resid, stats = pl.pallas_call(
            functools.partial(mixer, n_sp, n_tp, rows_x),
            out_shape=(pltpu.VMEM((length, feats), F32), pltpu.VMEM((length, LANES), F32)),
            in_specs=[hbm] * 13,
            out_specs=(vmem, vmem),
            scratch_shapes=scratch,
            compiler_params=pltpu.CompilerParams(
                collective_id=0, has_side_effects=True, vmem_limit_bytes=LIMIT),
            name="mixer",
        )(stream, w_pool, w_query, w_forget, w_value, w_gate, mix, row(scale), row(bound), extra.T,
          row(gain), wo_pool, wo_rec)
        piece = 128
        pieces = length // piece
        return pl.pallas_call(
            functools.partial(finish, n_tp * feats, piece),
            out_shape=jax.ShapeDtypeStruct(stream.shape, BF16),
            in_specs=[vmem] * 4,
            out_specs=hbm,
            scratch_shapes=[pltpu.VMEM((length, feats), BF16), dma((pieces,))],
            compiler_params=pltpu.CompilerParams(vmem_limit_bytes=16 * 1024 * 1024),
            name="finish",
        )(resid, stats, row(norm_gain), row(norm_bias))

    placed = (
        P("fs", "sp", "tp"), P(None, "tp"), P(None, "tp"), P(None, "tp"), P(None, "tp"),
        P(None, "tp"), P("tp", None, None), P("tp"), P("tp"), P("sp", "tp"), P(),
        P("tp", None), P("tp", None), P("tp"), P("tp"),
    )
    return jax.shard_map(
        local, mesh=mesh, in_specs=placed, out_specs=P("fs", "sp", "tp"), check_vma=False
    )
```

```python
import functools

import jax
import jax.numpy as jnp
from jax import lax
from jax.experimental import pallas as pl
from jax.experimental.pallas import tpu as pltpu
from jax.sharding import PartitionSpec as P

DK = 128
BLOCK_ROWS = 128
GROUP_CH = 256
HALO = 16
LANES = 128

LIMIT = 56 * 1024 * 1024
ALPHA = 2.0**0.25
EPS_RMS = 1e-06
EPS_NORM = 1e-05
F32 = jnp.float32
BF16 = jnp.bfloat16
NT = (((1,), (1,)), ((), ()))
TN = (((0,), (0,)), ((), ()))
OWN, PEER = 0, 1


def dot(a, b, dims=None):
    if dims is None:
        return jnp.dot(a, b, preferred_element_type=F32)
    return lax.dot_general(a, b, dims, preferred_element_type=F32)


def half_sigmoid(x):
    return 0.5 + 0.5 * jnp.tanh(0.5 * x)


def mixer(
    n_sp, n_tp, rows_x,
    stream, w_pool, w_query, w_forget, w_value, w_gate,
    mix_in, scale_in, bound_in, extra_in, gain_in, wo_pool, wo_rec,
    r_buf, stats,
    x_buf, w_buf, wo_buf, a_buf, v_buf, u_buf, e_buf, t_buf, p_buf, q_buf, g_buf, f_buf,
    half_buf, state, mine_out, row_in, total_out, total_in, start_out, start_in, halo_in,
    stat_own, stat_peer, bands,
    mix, scale, bound, extra, gain,
    x_loc, x_send, x_recv, w_sem, wo_loc, wo_send, wo_recv, a_send, a_recv,
    m_send, m_recv, r_send, r_recv, b_send, b_recv, h_send, h_recv, s_send, s_recv, small_sem, ready,
):
    sp, tp = lax.axis_index("sp"), lax.axis_index("tp")
    peer = 1 - tp
    length, feats = stream.shape[1], stream.shape[2]
    chans = bound.shape[1]
    heads = chans // DK
    pool_w = scale.shape[1]
    groups = mix.shape[0]
    chunks = length // rows_x
    blocks = length // BLOCK_ROWS
    per = rows_x // BLOCK_ROWS
    row_n = heads
    col_n = n_sp // row_n
    x_at, z_at = lax.rem(sp, row_n), lax.div(sp, row_n)
    row0 = z_at * row_n
    mesh_id = pl.DeviceIdType.MESH

    def rows_of(c):
        return slice(c * rows_x, (c + 1) * rows_x)

    def block_of(b):
        return slice(b * BLOCK_ROWS, (b + 1) * BLOCK_ROWS)

    def head_of(h):
        return slice(h * DK, (h + 1) * DK)

    x_pieces = ((0, length // 2), (length // 2, length // 2))
    pool_pieces = ((2 * rows_x, length - 2 * rows_x), (rows_x, rows_x), (0, rows_x))
    rec_pieces = tuple((c * rows_x, rows_x) for c in range(chunks))
    stat_pieces = ((0, length - rows_x), (length - rows_x, rows_x))

    def to_peer(src, dst, send, recv):
        return pltpu.make_async_remote_copy(
            src, dst, send, recv, device_id={"tp": peer}, device_id_type=mesh_id)

    def to_sp(src, dst, send, recv, k):
        return pltpu.make_async_remote_copy(
            src, dst, send, recv, device_id={"sp": k}, device_id_type=mesh_id)

    def x_in(i):
        rows = pl.ds(*x_pieces[i])
        return pltpu.make_async_copy(stream.at[0, rows], x_buf.at[OWN, rows], x_loc.at[i])

    def x_out(i):
        rows = pl.ds(*x_pieces[i])
        return to_peer(x_buf.at[OWN, rows], x_buf.at[PEER, rows], x_send, x_recv.at[i])

    my_cols = pl.ds(pl.multiple_of(tp * feats, LANES), feats)
    peer_cols = pl.ds(pl.multiple_of(peer * feats, LANES), feats)
    wo_places = ((wo_pool, pl.ds(0, pool_w)), (wo_rec, pl.ds(pool_w, chans)))

    w_groups = {(0, OWN): 0, (1, OWN): 1, (0, PEER): 2, (1, PEER): 2, (2, OWN): 3, (2, PEER): 3}

    def w_in(i, side):
        src = (w_forget, w_value, w_pool, w_query, w_gate)[i]
        return pltpu.make_async_copy(
            src.at[my_cols if side == OWN else peer_cols], w_buf.at[i, side], w_sem.at[w_groups.get((i, side), 4)])

    def w_wait(ref, group):
        pltpu.make_async_copy(ref, ref, w_sem.at[group]).wait()

    def wo_in(i):
        src, place = wo_places[i]
        return pltpu.make_async_copy(src.at[:, my_cols], wo_buf.at[OWN, place], wo_loc)

    def wo_out(i):
        src, place = wo_places[i]
        return to_peer(src.at[:, peer_cols], wo_buf.at[PEER, place], wo_send, wo_recv)

    def pool_out(i):
        rows, cols = pl.ds(*pool_pieces[i]), wo_places[0][1]
        return to_peer(a_buf.at[OWN, rows, cols], a_buf.at[PEER, rows, cols], a_send, a_recv.at[i])

    def rec_out(i):
        rows, cols = pl.ds(*rec_pieces[i]), wo_places[1][1]
        return to_peer(a_buf.at[OWN, rows, cols], a_buf.at[PEER, rows, cols], a_send, a_recv.at[len(pool_pieces) + i])

    def mine_to(k, slot):
        return to_sp(mine_out.at[k], row_in.at[slot], m_send, m_recv, row0 + k)

    def total_to(k, slot):
        return to_sp(total_out, total_in.at[slot], r_send, r_recv, k * row_n + x_at)

    def start_to(k, slot):
        return to_sp(start_out.at[k], start_in.at[slot], b_send, b_recv, row0 + k)

    def some(ref, count, send, recv):
        return to_sp(ref.at[0:count], ref.at[0:count], send, recv, row0)

    def when_equal(value, counts, do):
        for n in counts:
            @pl.when(value == n)
            def _():
                do(n)

    def h_out(k):
        return to_sp(p_buf.at[pl.ds(BLOCK_ROWS + length - HALO, HALO)], halo_in, h_send, h_recv, k)

    def s_out(i):
        rows = pl.ds(*stat_pieces[i])
        return to_peer(stat_own.at[rows], stat_peer.at[rows], s_send, s_recv.at[i])

    def greet(k):
        pl.semaphore_signal(ready, inc=1, device_id={"sp": k}, device_id_type=mesh_id)

    def each(low, high, do):
        def step(k, _):
            do(k)
            return 0

        lax.fori_loop(low, high, step, 0)

    smalls = [
        pltpu.make_async_copy(src, dst, small_sem.at[i])
        for i, (src, dst) in enumerate(
            ((extra_in, extra), (bound_in, bound), (mix_in, mix), (scale_in, scale), (gain_in, gain)))
    ]

    smalls[0].start()
    x_in(0).start()
    w_in(0, OWN).start()

    barrier = pltpu.get_barrier_semaphore()
    pl.semaphore_signal(barrier, inc=1, device_id={"tp": peer}, device_id_type=mesh_id)

    def hail(k):
        pl.semaphore_signal(barrier, inc=1, device_id={"sp": k}, device_id_type=mesh_id)

    each(x_at + 1, row_n, lambda k: hail(row0 + k))
    each(z_at + 1, col_n, lambda k: hail(k * row_n + x_at))
    leads = (x_at == 0) & (z_at > 0)
    ends = (x_at == row_n - 1) & (z_at < col_n - 1)
    later = (row_n - 1 - x_at) + (col_n - 1 - z_at) + jnp.where(ends, 1, 0)
    p_buf[0:BLOCK_ROWS, :] = jnp.zeros((BLOCK_ROWS, pool_w), BF16)

    row_ids = lax.broadcasted_iota(jnp.int32, (BLOCK_ROWS, BLOCK_ROWS), 0)
    col_ids = lax.broadcasted_iota(jnp.int32, (BLOCK_ROWS, BLOCK_ROWS), 1)
    lower = row_ids >= col_ids

    state[...] = jnp.zeros_like(state)
    with jax.named_scope("entry"):
        pl.semaphore_wait(barrier, 1 + x_at + z_at)
    with jax.named_scope("x_in"):
        x_in(0).wait()
        x_out(0).start()
    x_in(1).start()
    w_in(1, OWN).start()
    w_in(0, PEER).start()
    w_in(1, PEER).start()
    for copy in smalls[1:]:
        copy.start()
    each(0, x_at, lambda k: greet(row0 + k))
    each(0, z_at, lambda k: greet(k * row_n + x_at))
    wide_rows = lax.broadcasted_iota(jnp.int32, (BLOCK_ROWS, 2 * BLOCK_ROWS), 0) + BLOCK_ROWS
    wide_cols = lax.broadcasted_iota(jnp.int32, (BLOCK_ROWS, 2 * BLOCK_ROWS), 1)
    back = wide_rows - wide_cols
    with jax.named_scope("bands"):
        for j in range(groups):
            window = jnp.left_shift(jnp.int32(2), tp * groups + j)
            share = 1.0 / window.astype(F32)
            inside = (back >= 0) & (back < window)
            bands[j] = (jnp.where(inside, share, 0.0) - jnp.where(back == 0, 1.0, 0.0)).astype(BF16)

    with jax.named_scope("w0"):
        w_wait(w_buf.at[0, OWN], 0)

    tri = jnp.where(lower, 1.0, 0.0).astype(BF16)
    tri_twice = jnp.concatenate([tri, tri], axis=1)

    def proj(i, c, part=slice(0, rows_x)):
        rows = slice(c * rows_x + part.start, c * rows_x + part.stop)
        return dot(x_buf[OWN, rows, :], w_buf[i, OWN]) + dot(x_buf[PEER, rows, :], w_buf[i, PEER])

    class Post:
        def __init__(self, c):
            self.blocks = [c * per + j for j in range(per)]
            self.weight, self.split, self.total = {}, {}, {}
            self.down, self.half = {}, {}

        def logs(self):
            open_part = 1.0 - bound[...]
            for b in self.blocks:
                f_in = f_buf[block_of(b), :].astype(F32)
                weight = open_part * (0.5 - 0.5 * jnp.tanh(0.5 * f_in))
                drop = jnp.concatenate([extra[:, block_of(b)], jnp.zeros((8 - heads, BLOCK_ROWS), F32)], axis=0).T
                drop = jnp.concatenate(
                    [jnp.broadcast_to(drop[:, h:h + 1], (BLOCK_ROWS, DK)) for h in range(heads)], axis=1)
                keep = jnp.log(1.0 - weight) + drop
                high = keep.astype(BF16)
                low = (keep - high.astype(F32)).astype(BF16)
                self.weight[b], self.split[b] = weight, jnp.concatenate([high, low], axis=0)

        def sums(self):
            for b in self.blocks:
                self.total[b] = dot(tri_twice, self.split[b])

        def exps(self):
            for b in self.blocks:
                total = self.total[b]
                middle = 0.5 * total[BLOCK_ROWS - 1:BLOCK_ROWS]
                e_buf[block_of(b), :] = jnp.exp(total - middle)
                down = (self.weight[b] * jnp.exp(middle - total)).astype(BF16)
                u_buf[block_of(b), :] = down
                half = jnp.exp(middle)
                half_buf[b] = jnp.broadcast_to(half, (8, chans))
                self.down[b], self.half[b] = down, half

        def states(self):
            for b in self.blocks:
                for h in range(heads):
                    lanes = head_of(h)
                    hh = self.half[b][:, lanes]
                    term = dot(v_buf[block_of(b), lanes], self.down[b][:, lanes], TN) * hh
                    t_buf[b, :, lanes] = term
                    state[:, lanes] = hh * hh * state[:, lanes] + term

    whole, upper, under = slice(0, rows_x), slice(0, rows_x // 2), slice(rows_x // 2, rows_x)

    def put_pool(c, part=whole):
        at = BLOCK_ROWS + c * rows_x
        p_buf[at + part.start:at + part.stop, :] = proj(2, c, part).astype(BF16)

    def own_half(i, some_chunks):
        for c in some_chunks:
            r_buf[rows_of(c), i * chans:(i + 1) * chans] = dot(x_buf[OWN, rows_of(c), :], w_buf[i, OWN])

    with jax.named_scope("own0"):
        own_half(0, range(chunks // 2))
    with jax.named_scope("x_in1"):
        x_in(1).wait()
        x_out(1).start()
    with jax.named_scope("own0"):
        own_half(0, range(chunks // 2, chunks))
    with jax.named_scope("w1"):
        w_wait(w_buf.at[1, OWN], 1)
    for side in (OWN, PEER):
        w_in(2, side).start()
    with jax.named_scope("own1"):
        own_half(1, range(chunks))

    def rest(i, c):
        return (r_buf[rows_of(c), i * chans:(i + 1) * chans] + dot(x_buf[PEER, rows_of(c), :], w_buf[i, PEER])).astype(BF16)

    with jax.named_scope("x_recv0"):
        x_out(0).wait_recv()
        w_wait(w_buf.at[0:2, PEER], 2)
        for copy in smalls:
            copy.wait()
    for i in (3, 4):
        for side in (OWN, PEER):
            w_in(i, side).start()
    posts = [Post(c) for c in range(chunks)]

    def forget(c):
        f_buf[rows_of(c), :] = rest(0, c)

    def value(c):
        v_buf[rows_of(c), :] = rest(1, c)

    with jax.named_scope("first"):
        forget(0)
        posts[0].logs()
        forget(1)
        posts[0].sums()
        value(0)
        posts[0].exps()
    with jax.named_scope("x_recv1"):
        x_out(1).wait_recv()
        w_wait(w_buf.at[2], 3)
    for i in range(2):
        wo_in(i).start()
        wo_out(i).start()

    @pl.when(leads)
    def _():
        with jax.named_scope("lead"):
            pl.semaphore_wait(ready, later)
        greet(sp - 1)

    with jax.named_scope("first2"):
        posts[1].logs()
        forget(2)
        posts[0].states()
        posts[1].sums()
        value(1)
        posts[1].exps()
        posts[2].logs()
        forget(3)
        posts[1].states()
        posts[2].sums()
        value(2)
        posts[2].exps()
        posts[3].logs()
        posts[2].states()
        posts[3].sums()
        value(3)
        posts[3].exps()
        put_pool(3, under)
        posts[3].states()
        log_half = half_buf[0, 0:1]
        for b in range(1, blocks):
            log_half = log_half * half_buf[b, 0:1]
        keep_all = jnp.broadcast_to(log_half * log_half, (HALO, chans)).astype(BF16)
        for h in range(heads):
            mine_out[h, 0:DK, :] = state[:, head_of(h)].astype(BF16)
            mine_out[h, DK:DK + HALO, :] = keep_all[:, head_of(h)]

    @pl.when(jnp.logical_not(leads) & (sp + 1 < n_sp))
    def _():
        with jax.named_scope("later"):
            pl.semaphore_wait(ready, later)

    for k in range(row_n):
        @pl.when(x_at != k)
        def _():
            mine_to(k, x_at).start()
    row_in[x_at] = mine_out[x_at]

    @pl.when(sp + 1 < n_sp)
    def _():
        h_out(sp + 1).start()

    with jax.named_scope("w34"):
        w_wait(w_buf.at[3:5], 4)
    with jax.named_scope("second"):
        put_pool(3, upper)
        for c in reversed(range(chunks - 1)):
            put_pool(c)

    def part_of(ref, at):
        return ref[at, 0:DK, :].astype(F32), ref[at, DK:DK + HALO, :].astype(F32)[0:1]

    def fold_row():
        with jax.named_scope("row_recv"):
            some(row_in, row_n - 1, m_send, m_recv).wait_recv()
        total, kept = part_of(row_in, 0)
        for k in range(1, row_n):
            term, keep = part_of(row_in, k)
            total = keep * total + term
            kept = kept * keep
        total_out[0:DK, :] = total.astype(BF16)
        total_out[DK:DK + HALO, :] = jnp.broadcast_to(kept, (HALO, DK)).astype(BF16)
        each(z_at + 1, col_n, lambda k: total_to(k, z_at).start())

    def fold_column():
        state[:, 0:DK] = jnp.zeros((DK, DK), F32)
        with jax.named_scope("col_recv"):
            when_equal(z_at, range(1, col_n), lambda n: some(total_in, n, r_send, r_recv).wait_recv())

        def take(k):
            term, keep = part_of(total_in, k)
            state[:, 0:DK] = keep * state[:, 0:DK] + term

        each(0, z_at, take)
        total = state[:, 0:DK]
        for k in range(row_n):
            start_out[k] = total.astype(BF16)
            if k + 1 < row_n:
                term, keep = part_of(row_in, k)
                total = keep * total + term
        for k in range(row_n):
            @pl.when((x_at != k) & (row0 + k > 0))
            def _():
                start_to(k, x_at).start()

        start_in[x_at] = start_out[x_at]

    count = lax.broadcasted_iota(jnp.int32, (BLOCK_ROWS, LANES), 0) + (sp * length + 1)

    gains = jnp.concatenate([gain[...]] * heads, axis=1)

    class Third:
        def __init__(self, c):
            self.c, self.rows = c, rows_of(c)
            self.blocks = [c * per + k for k in range(per)]

        def query(self):
            q_in = proj(3, self.c).astype(BF16).astype(F32)
            q_buf[self.rows, :] = (q_in * half_sigmoid(q_in) * e_buf[self.rows, :]).astype(BF16)

        def band(self):
            for b in self.blocks:
                near = p_buf[b * BLOCK_ROWS:(b + 2) * BLOCK_ROWS, :]
                for j in range(groups):
                    lanes = slice(j * GROUP_CH, (j + 1) * GROUP_CH)
                    if b:
                        a_buf[OWN, block_of(b), lanes] = dot(bands[j], near[:, lanes]).astype(BF16)
                        continue
                    window = jnp.left_shift(jnp.int32(2), tp * groups + j)
                    inside = jnp.where((back >= 0) & (back < window), 1.0, 0.0).astype(BF16)
                    share = 1.0 / jnp.minimum(count, window).astype(F32)
                    share = jnp.concatenate([share] * (GROUP_CH // LANES), axis=1)
                    sums = dot(inside, near[:, lanes])
                    a_buf[OWN, block_of(b), lanes] = (sums * share - near[BLOCK_ROWS:, lanes].astype(F32)).astype(BF16)

        def gates(self, part):
            rows = slice(self.rows.start + part.start, self.rows.start + part.stop)
            gate = proj(4, self.c, part).astype(BF16).astype(F32)
            g_buf[rows, :] = gate * half_sigmoid(gate) * gains

        def mixed(self):
            for j in range(groups):
                lanes = slice(j * GROUP_CH, (j + 1) * GROUP_CH)
                a_buf[OWN, self.rows, lanes] = (dot(a_buf[OWN, self.rows, lanes], mix[j]) * scale[:, lanes]).astype(BF16)

        def score(self):
            for b in self.blocks:
                for h in range(heads):
                    up, down = q_buf[block_of(b), head_of(h)], u_buf[block_of(b), head_of(h)]
                    f_buf[block_of(b), head_of(h)] = jnp.where(lower, dot(up, down, NT), 0.0).astype(BF16)

        def inner(self):
            for b in self.blocks:
                for h in range(heads):
                    at = block_of(b), head_of(h)
                    e_buf[at] = dot(f_buf[at], v_buf[at])

    parts = [Third(c) for c in range(chunks)]
    early = x_at >= row_n // 2

    def fold_at(stage, who):
        @pl.when(who)
        def _():
            stage()

    for c in reversed(range(chunks)):
        if c == 2:
            fold_at(fold_row, early)
        if c == 1:
            pool_out(0).start()
            fold_at(fold_row, jnp.logical_not(early))
            fold_at(fold_column, early)
        if c == 0:
            pool_out(1).start()
            fold_at(fold_column, x_at == 1)

            @pl.when(sp > 0)
            def _():
                with jax.named_scope("halo_recv"):
                    h_out(sp).wait_recv()
                p_buf[BLOCK_ROWS - HALO:BLOCK_ROWS, :] = halo_in[...]

        with jax.named_scope("third"):
            parts[c].query()
            if c + 1 < chunks:
                parts[c + 1].inner()
            parts[c].band()
            parts[c].gates(whole)
            parts[c].mixed()
            parts[c].score()
    pool_out(2).start()
    fold_at(fold_column, x_at == 0)

    with jax.named_scope("wo"):
        pltpu.make_async_copy(wo_buf.at[OWN], wo_buf.at[OWN], wo_loc).wait()
        to_peer(wo_buf.at[OWN], wo_buf.at[PEER], wo_send, wo_recv).wait_recv()
        pool_out(0).wait_recv()

    pool_at, rec_at = slice(0, pool_w), slice(pool_w, pool_w + chans)

    def pool_part(c):
        rows = rows_of(c)
        r_buf[rows, :] = (
            dot(a_buf[OWN, rows, pool_at], wo_buf[OWN, pool_at]) + dot(a_buf[PEER, rows, pool_at], wo_buf[PEER, pool_at])
            + ALPHA * x_buf[OWN, rows, :].astype(F32))

    with jax.named_scope("pool"):
        pool_part(chunks - 1)
        parts[0].inner()
        pool_part(chunks - 2)
    with jax.named_scope("pool_recv"):
        pool_out(1).wait_recv()
        pool_out(2).wait_recv()
    with jax.named_scope("pool"):
        pool_part(1)
        pool_part(0)

    @pl.when(sp > 0)
    def _():
        with jax.named_scope("start_recv"):
            some(start_in, row_n - 1, b_send, b_recv).wait_recv()

    @pl.when(sp > 0)
    def _():
        for h in range(heads):
            state[:, head_of(h)] = start_in[h].astype(F32)

    @pl.when(sp == 0)
    def _():
        state[...] = jnp.zeros_like(state)

    def fourth(c):
        for k in range(per):
            b = c * per + k
            half = half_buf[b, 0:1]
            before = state[...] * half
            carried = before.astype(BF16)
            state[...] = before * half + t_buf[b]
            for h in range(heads):
                lanes = head_of(h)
                raw = e_buf[block_of(b), lanes] + dot(q_buf[block_of(b), lanes], carried[:, lanes], NT)
                power = jnp.mean(raw * raw, axis=-1, keepdims=True)
                rec = raw * lax.rsqrt(power + EPS_RMS) * g_buf[block_of(b), lanes]
                a_buf[OWN, block_of(b), pool_w + h * DK:pool_w + (h + 1) * DK] = rec.astype(BF16)

    def rec_part(side, c):
        r_buf[rows_of(c), :] += dot(a_buf[side, rows_of(c), rec_at], wo_buf[side, rec_at])

    with jax.named_scope("fourth"):
        fourth(0)
        fourth(1)
        rec_out(0).start()
        rec_out(1).start()
    with jax.named_scope("fourth2"):
        fourth(2)
        rec_part(OWN, 0)
        rec_out(2).start()
        fourth(3)
        rec_part(OWN, 1)
        rec_out(3).start()

    def fold(x):
        acc = x[:, :LANES]
        for k in range(1, feats // LANES):
            acc = acc + x[:, k * LANES:(k + 1) * LANES]
        return acc

    first_half = lax.broadcasted_iota(jnp.int32, (rows_x, LANES), 1) < LANES // 2

    def fifth(c):
        rows = rows_of(c)
        resid = r_buf[rows, :] + dot(a_buf[PEER, rows, rec_at], wo_buf[PEER, rec_at])
        r_buf[rows, :] = resid
        sums, squares = fold(resid), fold(resid * resid)
        sums = sums + pltpu.roll(sums, LANES // 2, 1)
        squares = squares + pltpu.roll(squares, LANES // 2, 1)
        stat_own[rows, :] = jnp.where(first_half, sums, squares)

    with jax.named_scope("fifth"):
        rec_part(OWN, 2)
        rec_part(OWN, 3)
        for c in range(3):
            with jax.named_scope("rec_recv"):
                rec_out(c).wait_recv()
        for c in range(3):
            fifth(c)
        s_out(0).start()
    with jax.named_scope("fifth3"):
        with jax.named_scope("rec_recv"):
            rec_out(3).wait_recv()
        fifth(3)
        s_out(1).start()

    with jax.named_scope("sent"):
        to_peer(x_buf.at[OWN], x_buf.at[PEER], x_send, x_recv.at[0]).wait_send()
        to_peer(a_buf.at[OWN], a_buf.at[PEER], a_send, a_recv.at[0]).wait_send()
        to_peer(wo_buf.at[OWN], wo_buf.at[PEER], wo_send, wo_recv).wait_send()
        some(mine_out, row_n - 1, m_send, m_recv).wait_send()
        when_equal(col_n - 1 - z_at, range(1, col_n), lambda n: some(total_in, n, r_send, r_recv).wait_send())
        starts = jnp.where((z_at > 0) | (x_at == 0), row_n - 1, row_n - 2)
        when_equal(starts, (row_n - 2, row_n - 1), lambda n: some(start_out, n, b_send, b_recv).wait_send())

        @pl.when(sp + 1 < n_sp)
        def _():
            h_out(sp + 1).wait_send()

    with jax.named_scope("tail"):
        for i, (start, n) in enumerate(stat_pieces):
            s_out(i).wait_recv()
            stats[start:start + n, :] = stat_own[start:start + n, :] + stat_peer[start:start + n, :]
        to_peer(stat_own, stat_peer, s_send, s_recv.at[0]).wait_send()


def finish(width, rows, resid, stats, gain, bias, out, o_buf, o_sem):
    pieces = resid.shape[0] // rows

    def leave(c):
        part = pl.ds(c * rows, rows)
        return pltpu.make_async_copy(o_buf.at[part], out.at[0, part], o_sem.at[c])

    half = rows // 2
    first_half = lax.broadcasted_iota(jnp.int32, (half, LANES), 1) < LANES // 2
    for c in range(pieces):
        for k in range(2):
            part = slice(c * rows + k * half, c * rows + (k + 1) * half)
            both = stats[part, :]
            mean = jnp.sum(jnp.where(first_half, both, 0.0), axis=1, keepdims=True) * (1.0 / width)
            square = jnp.sum(jnp.where(first_half, 0.0, both), axis=1, keepdims=True) * (1.0 / width)
            inv = lax.rsqrt(square - mean * mean + EPS_NORM)
            shift = -mean * inv
            o_buf[part, :] = ((resid[part, :] * inv + shift) * gain[...] + bias[...]).astype(BF16)
        leave(c).start()
    for c in range(pieces):
        leave(c).wait()


def solution(mesh):
    n_sp, n_tp = mesh.shape["sp"], mesh.shape["tp"]

    def local(stream, w_pool, w_query, w_forget, w_value, w_gate, mix, scale, bound, extra,
              gain, wo_pool, wo_rec, norm_gain, norm_bias):
        length, feats = stream.shape[1], stream.shape[2]
        chans, pool_w = bound.shape[0], scale.shape[0]
        heads = chans // DK
        blocks = length // BLOCK_ROWS
        rows_x = 256
        chunks = length // rows_x
        hbm = pl.BlockSpec(memory_space=pl.ANY)
        vmem = pl.BlockSpec(memory_space=pltpu.VMEM)
        dma = pltpu.SemaphoreType.DMA
        scratch = [
            pltpu.VMEM((n_tp, length, feats), BF16),
            pltpu.VMEM((5, n_tp, feats, chans), BF16),
            pltpu.VMEM((n_tp, pool_w + chans, feats), BF16),
            pltpu.VMEM((n_tp, length, pool_w + chans), BF16),
            pltpu.VMEM((length, chans), BF16),
            pltpu.VMEM((length, chans), BF16),
            pltpu.VMEM((length, chans), F32),
            pltpu.VMEM((blocks, DK, chans), F32),
            pltpu.VMEM((BLOCK_ROWS + length, pool_w), BF16),
            pltpu.VMEM((length, chans), BF16),
            pltpu.VMEM((length, chans), F32),
            pltpu.VMEM((length, chans), BF16),
            pltpu.VMEM((blocks, 8, chans), F32),
            pltpu.VMEM((DK, chans), F32),
            pltpu.VMEM((heads, DK + HALO, DK), BF16),
            pltpu.VMEM((heads, DK + HALO, DK), BF16),
            pltpu.VMEM((DK + HALO, DK), BF16),
            pltpu.VMEM((n_sp // heads, DK + HALO, DK), BF16),
            pltpu.VMEM((heads, DK, DK), BF16),
            pltpu.VMEM((heads, DK, DK), BF16),
            pltpu.VMEM((HALO, pool_w), BF16),
            pltpu.VMEM((length, LANES), F32),
            pltpu.VMEM((length, LANES), F32),
            pltpu.VMEM((mix.shape[0], BLOCK_ROWS, 2 * BLOCK_ROWS), BF16),
            pltpu.VMEM(mix.shape, BF16),
            pltpu.VMEM((1, pool_w), F32),
            pltpu.VMEM((1, chans), F32),
            pltpu.VMEM((heads, length), F32),
            pltpu.VMEM((1, DK), F32),
            dma((2,)), dma, dma((2,)), dma((5,)), dma, dma, dma, dma, dma((7,)),
            dma, dma, dma, dma, dma, dma, dma, dma, dma, dma((2,)), dma((5,)), pltpu.SemaphoreType.REGULAR,
        ]
        row = lambda x: x.reshape(1, -1)
        resid, stats = pl.pallas_call(
            functools.partial(mixer, n_sp, n_tp, rows_x),
            out_shape=(pltpu.VMEM((length, feats), F32), pltpu.VMEM((length, LANES), F32)),
            in_specs=[hbm] * 13,
            out_specs=(vmem, vmem),
            scratch_shapes=scratch,
            compiler_params=pltpu.CompilerParams(
                collective_id=0, has_side_effects=True, vmem_limit_bytes=LIMIT),
            name="mixer",
        )(stream, w_pool, w_query, w_forget, w_value, w_gate, mix, row(scale), row(bound), extra.T,
          row(gain), wo_pool, wo_rec)
        piece = 128
        pieces = length // piece
        return pl.pallas_call(
            functools.partial(finish, n_tp * feats, piece),
            out_shape=jax.ShapeDtypeStruct(stream.shape, BF16),
            in_specs=[vmem] * 4,
            out_specs=hbm,
            scratch_shapes=[pltpu.VMEM((length, feats), BF16), dma((pieces,))],
            compiler_params=pltpu.CompilerParams(vmem_limit_bytes=16 * 1024 * 1024),
            name="finish",
        )(resid, stats, row(norm_gain), row(norm_bias))

    placed = (
        P("fs", "sp", "tp"), P(None, "tp"), P(None, "tp"), P(None, "tp"), P(None, "tp"),
        P(None, "tp"), P("tp", None, None), P("tp"), P("tp"), P("sp", "tp"), P(),
        P("tp", None), P("tp", None), P("tp"), P("tp"),
    )
    return jax.shard_map(
        local, mesh=mesh, in_specs=placed, out_specs=P("fs", "sp", "tp"), check_vma=False
    )
```

```python
import functools

import jax
import jax.numpy as jnp
from jax import lax
from jax.experimental import pallas as pl
from jax.experimental.pallas import tpu as pltpu
from jax.sharding import PartitionSpec as P

DK = 128
BLOCK_ROWS = 128
GROUP_CH = 256
HALO = 16
LANES = 128

LIMIT = 56 * 1024 * 1024
ALPHA = 2.0**0.25
EPS_RMS = 1e-06
EPS_NORM = 1e-05
F32 = jnp.float32
BF16 = jnp.bfloat16
NT = (((1,), (1,)), ((), ()))
TN = (((0,), (0,)), ((), ()))
OWN, PEER = 0, 1


def dot(a, b, dims=None):
    if dims is None:
        return jnp.dot(a, b, preferred_element_type=F32)
    return lax.dot_general(a, b, dims, preferred_element_type=F32)


def half_sigmoid(x):
    return 0.5 + 0.5 * jnp.tanh(0.5 * x)


def mixer(
    n_sp, n_tp, rows_x,
    stream, w_pool, w_query, w_forget, w_value, w_gate,
    mix_in, scale_in, bound_in, extra_in, gain_in, wo_pool, wo_rec,
    r_buf, stats,
    x_buf, w_buf, wo_buf, a_buf, v_buf, u_buf, e_buf, t_buf, p_buf, q_buf, g_buf, f_buf,
    half_buf, state, mine_out, row_in, total_out, total_in, start_out, start_in, halo_in,
    stat_own, stat_peer, bands,
    mix, scale, bound, extra, gain,
    x_loc, x_send, x_recv, w_sem, wo_loc, wo_send, wo_recv, a_send, a_recv,
    m_send, m_recv, r_send, r_recv, b_send, b_recv, h_send, h_recv, s_send, s_recv, small_sem, ready,
):
    sp, tp = lax.axis_index("sp"), lax.axis_index("tp")
    peer = 1 - tp
    length, feats = stream.shape[1], stream.shape[2]
    chans = bound.shape[1]
    heads = chans // DK
    pool_w = scale.shape[1]
    groups = mix.shape[0]
    chunks = length // rows_x
    blocks = length // BLOCK_ROWS
    per = rows_x // BLOCK_ROWS
    row_n = heads
    col_n = n_sp // row_n
    x_at, z_at = lax.rem(sp, row_n), lax.div(sp, row_n)
    row0 = z_at * row_n
    mesh_id = pl.DeviceIdType.MESH

    def rows_of(c):
        return slice(c * rows_x, (c + 1) * rows_x)

    def block_of(b):
        return slice(b * BLOCK_ROWS, (b + 1) * BLOCK_ROWS)

    def head_of(h):
        return slice(h * DK, (h + 1) * DK)

    x_pieces = ((0, length // 2), (length // 2, length // 2))
    pool_pieces = ((2 * rows_x, length - 2 * rows_x), (rows_x, rows_x), (0, rows_x))
    rec_pieces = tuple((c * rows_x, rows_x) for c in range(chunks))
    stat_pieces = ((0, length - rows_x), (length - rows_x, rows_x))

    def to_peer(src, dst, send, recv):
        return pltpu.make_async_remote_copy(
            src, dst, send, recv, device_id={"tp": peer}, device_id_type=mesh_id)

    def to_sp(src, dst, send, recv, k):
        return pltpu.make_async_remote_copy(
            src, dst, send, recv, device_id={"sp": k}, device_id_type=mesh_id)

    def x_in(i):
        rows = pl.ds(*x_pieces[i])
        return pltpu.make_async_copy(stream.at[0, rows], x_buf.at[OWN, rows], x_loc.at[i])

    def x_out(i):
        rows = pl.ds(*x_pieces[i])
        return to_peer(x_buf.at[OWN, rows], x_buf.at[PEER, rows], x_send, x_recv.at[i])

    my_cols = pl.ds(pl.multiple_of(tp * feats, LANES), feats)
    peer_cols = pl.ds(pl.multiple_of(peer * feats, LANES), feats)
    wo_places = ((wo_pool, pl.ds(0, pool_w)), (wo_rec, pl.ds(pool_w, chans)))

    w_groups = {(0, OWN): 0, (1, OWN): 1, (0, PEER): 2, (1, PEER): 2, (2, OWN): 3, (2, PEER): 3}

    def w_in(i, side):
        src = (w_forget, w_value, w_pool, w_query, w_gate)[i]
        return pltpu.make_async_copy(
            src.at[my_cols if side == OWN else peer_cols], w_buf.at[i, side], w_sem.at[w_groups.get((i, side), 4)])

    def w_wait(ref, group):
        pltpu.make_async_copy(ref, ref, w_sem.at[group]).wait()

    def wo_in(i):
        src, place = wo_places[i]
        return pltpu.make_async_copy(src.at[:, my_cols], wo_buf.at[OWN, place], wo_loc)

    def wo_out(i):
        src, place = wo_places[i]
        return to_peer(src.at[:, peer_cols], wo_buf.at[PEER, place], wo_send, wo_recv)

    def pool_out(i):
        rows, cols = pl.ds(*pool_pieces[i]), wo_places[0][1]
        return to_peer(a_buf.at[OWN, rows, cols], a_buf.at[PEER, rows, cols], a_send, a_recv.at[i])

    def rec_out(i):
        rows, cols = pl.ds(*rec_pieces[i]), wo_places[1][1]
        return to_peer(a_buf.at[OWN, rows, cols], a_buf.at[PEER, rows, cols], a_send, a_recv.at[len(pool_pieces) + i])

    def mine_to(k, slot):
        return to_sp(mine_out.at[k], row_in.at[slot], m_send, m_recv, row0 + k)

    def total_to(k, slot):
        return to_sp(total_out, total_in.at[slot], r_send, r_recv, k * row_n + x_at)

    def start_to(k, slot):
        return to_sp(start_out.at[k], start_in.at[slot], b_send, b_recv, row0 + k)

    def some(ref, count, send, recv):
        return to_sp(ref.at[0:count], ref.at[0:count], send, recv, row0)

    def when_equal(value, counts, do):
        for n in counts:
            @pl.when(value == n)
            def _():
                do(n)

    def h_out(k):
        return to_sp(p_buf.at[pl.ds(BLOCK_ROWS + length - HALO, HALO)], halo_in, h_send, h_recv, k)

    def s_out(i):
        rows = pl.ds(*stat_pieces[i])
        return to_peer(stat_own.at[rows], stat_peer.at[rows], s_send, s_recv.at[i])

    def greet(k):
        pl.semaphore_signal(ready, inc=1, device_id={"sp": k}, device_id_type=mesh_id)

    def each(low, high, do):
        def step(k, _):
            do(k)
            return 0

        lax.fori_loop(low, high, step, 0)

    smalls = [
        pltpu.make_async_copy(src, dst, small_sem.at[i])
        for i, (src, dst) in enumerate(
            ((extra_in, extra), (bound_in, bound), (mix_in, mix), (scale_in, scale), (gain_in, gain)))
    ]

    smalls[0].start()
    x_in(0).start()
    w_in(0, OWN).start()
    x_in(1).start()

    barrier = pltpu.get_barrier_semaphore()
    pl.semaphore_signal(barrier, inc=1, device_id={"tp": peer}, device_id_type=mesh_id)

    def hail(k):
        pl.semaphore_signal(barrier, inc=1, device_id={"sp": k}, device_id_type=mesh_id)

    each(x_at + 1, row_n, lambda k: hail(row0 + k))
    each(z_at + 1, col_n, lambda k: hail(k * row_n + x_at))
    leads = (x_at == 0) & (z_at > 0)
    ends = (x_at == row_n - 1) & (z_at < col_n - 1)
    later = (row_n - 1 - x_at) + (col_n - 1 - z_at) + jnp.where(ends, 1, 0)
    p_buf[0:BLOCK_ROWS, :] = jnp.zeros((BLOCK_ROWS, pool_w), BF16)

    row_ids = lax.broadcasted_iota(jnp.int32, (BLOCK_ROWS, BLOCK_ROWS), 0)
    col_ids = lax.broadcasted_iota(jnp.int32, (BLOCK_ROWS, BLOCK_ROWS), 1)
    lower = row_ids >= col_ids

    state[...] = jnp.zeros_like(state)
    with jax.named_scope("entry"):
        pl.semaphore_wait(barrier, 1 + x_at + z_at)
    with jax.named_scope("x_in"):
        x_in(0).wait()
        x_out(0).start()
    w_in(1, OWN).start()
    w_in(0, PEER).start()
    w_in(1, PEER).start()
    for copy in smalls[1:]:
        copy.start()
    each(0, x_at, lambda k: greet(row0 + k))
    each(0, z_at, lambda k: greet(k * row_n + x_at))
    wide_rows = lax.broadcasted_iota(jnp.int32, (BLOCK_ROWS, 2 * BLOCK_ROWS), 0) + BLOCK_ROWS
    wide_cols = lax.broadcasted_iota(jnp.int32, (BLOCK_ROWS, 2 * BLOCK_ROWS), 1)
    back = wide_rows - wide_cols
    with jax.named_scope("bands"):
        for j in range(groups):
            window = jnp.left_shift(jnp.int32(2), tp * groups + j)
            share = 1.0 / window.astype(F32)
            inside = (back >= 0) & (back < window)
            bands[j] = (jnp.where(inside, share, 0.0) - jnp.where(back == 0, 1.0, 0.0)).astype(BF16)

    with jax.named_scope("x_in1"):
        x_in(1).wait()
        x_out(1).start()
    with jax.named_scope("w0"):
        w_wait(w_buf.at[0, OWN], 0)

    tri = jnp.where(lower, 1.0, 0.0).astype(BF16)
    tri_twice = jnp.concatenate([tri, tri], axis=1)

    def proj(i, c, part=slice(0, rows_x)):
        rows = slice(c * rows_x + part.start, c * rows_x + part.stop)
        return dot(x_buf[OWN, rows, :], w_buf[i, OWN]) + dot(x_buf[PEER, rows, :], w_buf[i, PEER])

    class Post:
        def __init__(self, c):
            self.blocks = [c * per + j for j in range(per)]
            self.weight, self.split, self.total = {}, {}, {}
            self.down, self.half = {}, {}

        def logs(self):
            open_part = 1.0 - bound[...]
            for b in self.blocks:
                f_in = f_buf[block_of(b), :].astype(F32)
                weight = open_part * (0.5 - 0.5 * jnp.tanh(0.5 * f_in))
                drop = jnp.concatenate([extra[:, block_of(b)], jnp.zeros((8 - heads, BLOCK_ROWS), F32)], axis=0).T
                drop = jnp.concatenate(
                    [jnp.broadcast_to(drop[:, h:h + 1], (BLOCK_ROWS, DK)) for h in range(heads)], axis=1)
                keep = jnp.log(1.0 - weight) + drop
                high = keep.astype(BF16)
                low = (keep - high.astype(F32)).astype(BF16)
                self.weight[b], self.split[b] = weight, jnp.concatenate([high, low], axis=0)

        def sums(self):
            for b in self.blocks:
                self.total[b] = dot(tri_twice, self.split[b])

        def exps(self):
            for b in self.blocks:
                total = self.total[b]
                middle = 0.5 * total[BLOCK_ROWS - 1:BLOCK_ROWS]
                e_buf[block_of(b), :] = jnp.exp(total - middle)
                down = (self.weight[b] * jnp.exp(middle - total)).astype(BF16)
                u_buf[block_of(b), :] = down
                half = jnp.exp(middle)
                half_buf[b] = jnp.broadcast_to(half, (8, chans))
                self.down[b], self.half[b] = down, half

        def states(self):
            for b in self.blocks:
                for h in range(heads):
                    lanes = head_of(h)
                    hh = self.half[b][:, lanes]
                    term = dot(v_buf[block_of(b), lanes], self.down[b][:, lanes], TN) * hh
                    t_buf[b, :, lanes] = term
                    state[:, lanes] = hh * hh * state[:, lanes] + term

    whole, upper, under = slice(0, rows_x), slice(0, rows_x // 2), slice(rows_x // 2, rows_x)

    def put_pool(c, part=whole):
        at = BLOCK_ROWS + c * rows_x
        p_buf[at + part.start:at + part.stop, :] = proj(2, c, part).astype(BF16)

    def own_half(i, some_chunks):
        for c in some_chunks:
            r_buf[rows_of(c), i * chans:(i + 1) * chans] = dot(x_buf[OWN, rows_of(c), :], w_buf[i, OWN])

    with jax.named_scope("own0"):
        own_half(0, range(chunks))
    with jax.named_scope("w1"):
        w_wait(w_buf.at[1, OWN], 1)
    for side in (OWN, PEER):
        w_in(2, side).start()
    with jax.named_scope("own1"):
        own_half(1, range(chunks))

    def rest(i, c):
        return (r_buf[rows_of(c), i * chans:(i + 1) * chans] + dot(x_buf[PEER, rows_of(c), :], w_buf[i, PEER])).astype(BF16)

    with jax.named_scope("x_recv0"):
        x_out(0).wait_recv()
        w_wait(w_buf.at[0:2, PEER], 2)
        for copy in smalls:
            copy.wait()
    for i in (3, 4):
        for side in (OWN, PEER):
            w_in(i, side).start()
    posts = [Post(c) for c in range(chunks)]

    def forget(c):
        f_buf[rows_of(c), :] = rest(0, c)

    def value(c):
        v_buf[rows_of(c), :] = rest(1, c)

    with jax.named_scope("first"):
        forget(0)
        posts[0].logs()
        forget(1)
        posts[0].sums()
        value(0)
        posts[0].exps()
    with jax.named_scope("x_recv1"):
        x_out(1).wait_recv()
        w_wait(w_buf.at[2], 3)
    for i in range(2):
        wo_in(i).start()
        wo_out(i).start()

    @pl.when(leads)
    def _():
        with jax.named_scope("lead"):
            pl.semaphore_wait(ready, later)
        greet(sp - 1)

    with jax.named_scope("first2"):
        posts[1].logs()
        forget(2)
        posts[0].states()
        posts[1].sums()
        value(1)
        posts[1].exps()
        posts[2].logs()
        forget(3)
        posts[1].states()
        posts[2].sums()
        value(2)
        posts[2].exps()
        posts[3].logs()
        posts[2].states()
        posts[3].sums()
        value(3)
        posts[3].exps()
        put_pool(3, under)
        posts[3].states()
        log_half = half_buf[0, 0:1]
        for b in range(1, blocks):
            log_half = log_half * half_buf[b, 0:1]
        keep_all = jnp.broadcast_to(log_half * log_half, (HALO, chans)).astype(BF16)
        for h in range(heads):
            mine_out[h, 0:DK, :] = state[:, head_of(h)].astype(BF16)
            mine_out[h, DK:DK + HALO, :] = keep_all[:, head_of(h)]

    @pl.when(jnp.logical_not(leads) & (sp + 1 < n_sp))
    def _():
        with jax.named_scope("later"):
            pl.semaphore_wait(ready, later)

    for k in range(row_n):
        @pl.when(x_at != k)
        def _():
            mine_to(k, x_at).start()
    row_in[x_at] = mine_out[x_at]

    @pl.when(sp + 1 < n_sp)
    def _():
        h_out(sp + 1).start()

    with jax.named_scope("w34"):
        w_wait(w_buf.at[3:5], 4)
    with jax.named_scope("second"):
        put_pool(3, upper)
        for c in reversed(range(chunks - 1)):
            put_pool(c)

    def part_of(ref, at):
        return ref[at, 0:DK, :].astype(F32), ref[at, DK:DK + HALO, :].astype(F32)[0:1]

    def fold_row():
        with jax.named_scope("row_recv"):
            some(row_in, row_n - 1, m_send, m_recv).wait_recv()
        total, kept = part_of(row_in, 0)
        for k in range(1, row_n):
            term, keep = part_of(row_in, k)
            total = keep * total + term
            kept = kept * keep
        total_out[0:DK, :] = total.astype(BF16)
        total_out[DK:DK + HALO, :] = jnp.broadcast_to(kept, (HALO, DK)).astype(BF16)
        each(z_at + 1, col_n, lambda k: total_to(k, z_at).start())

    def fold_column():
        state[:, 0:DK] = jnp.zeros((DK, DK), F32)
        with jax.named_scope("col_recv"):
            when_equal(z_at, range(1, col_n), lambda n: some(total_in, n, r_send, r_recv).wait_recv())

        def take(k):
            term, keep = part_of(total_in, k)
            state[:, 0:DK] = keep * state[:, 0:DK] + term

        each(0, z_at, take)
        total = state[:, 0:DK]
        for k in range(row_n):
            start_out[k] = total.astype(BF16)
            if k + 1 < row_n:
                term, keep = part_of(row_in, k)
                total = keep * total + term
        for k in range(row_n):
            @pl.when((x_at != k) & (row0 + k > 0))
            def _():
                start_to(k, x_at).start()

        start_in[x_at] = start_out[x_at]

    count = lax.broadcasted_iota(jnp.int32, (BLOCK_ROWS, LANES), 0) + (sp * length + 1)

    gains = jnp.concatenate([gain[...]] * heads, axis=1)

    class Third:
        def __init__(self, c):
            self.c, self.rows = c, rows_of(c)
            self.blocks = [c * per + k for k in range(per)]

        def query(self):
            q_in = proj(3, self.c).astype(BF16).astype(F32)
            q_buf[self.rows, :] = (q_in * half_sigmoid(q_in) * e_buf[self.rows, :]).astype(BF16)

        def band(self):
            for b in self.blocks:
                near = p_buf[b * BLOCK_ROWS:(b + 2) * BLOCK_ROWS, :]
                for j in range(groups):
                    lanes = slice(j * GROUP_CH, (j + 1) * GROUP_CH)
                    if b:
                        a_buf[OWN, block_of(b), lanes] = dot(bands[j], near[:, lanes]).astype(BF16)
                        continue
                    window = jnp.left_shift(jnp.int32(2), tp * groups + j)
                    inside = jnp.where((back >= 0) & (back < window), 1.0, 0.0).astype(BF16)
                    share = 1.0 / jnp.minimum(count, window).astype(F32)
                    share = jnp.concatenate([share] * (GROUP_CH // LANES), axis=1)
                    sums = dot(inside, near[:, lanes])
                    a_buf[OWN, block_of(b), lanes] = (sums * share - near[BLOCK_ROWS:, lanes].astype(F32)).astype(BF16)

        def gates(self, part):
            rows = slice(self.rows.start + part.start, self.rows.start + part.stop)
            gate = proj(4, self.c, part).astype(BF16).astype(F32)
            g_buf[rows, :] = gate * half_sigmoid(gate) * gains

        def mixed(self):
            for j in range(groups):
                lanes = slice(j * GROUP_CH, (j + 1) * GROUP_CH)
                a_buf[OWN, self.rows, lanes] = (dot(a_buf[OWN, self.rows, lanes], mix[j]) * scale[:, lanes]).astype(BF16)

        def score(self):
            for b in self.blocks:
                for h in range(heads):
                    up, down = q_buf[block_of(b), head_of(h)], u_buf[block_of(b), head_of(h)]
                    f_buf[block_of(b), head_of(h)] = jnp.where(lower, dot(up, down, NT), 0.0).astype(BF16)

        def inner(self):
            for b in self.blocks:
                for h in range(heads):
                    at = block_of(b), head_of(h)
                    e_buf[at] = dot(f_buf[at], v_buf[at])

    parts = [Third(c) for c in range(chunks)]
    early = x_at >= row_n // 2

    def fold_at(stage, who):
        @pl.when(who)
        def _():
            stage()

    for c in reversed(range(chunks)):
        if c == 2:
            fold_at(fold_row, early)
        if c == 1:
            pool_out(0).start()
            fold_at(fold_row, jnp.logical_not(early))
            fold_at(fold_column, x_at == row_n // 2)
        if c == 0:
            pool_out(1).start()
            fold_at(fold_column, (x_at > 0) & (x_at != row_n // 2))

            @pl.when(sp > 0)
            def _():
                with jax.named_scope("halo_recv"):
                    h_out(sp).wait_recv()
                p_buf[BLOCK_ROWS - HALO:BLOCK_ROWS, :] = halo_in[...]

        with jax.named_scope("third"):
            parts[c].query()
            if c + 1 < chunks:
                parts[c + 1].inner()
            parts[c].band()
            parts[c].gates(whole)
            parts[c].mixed()
            parts[c].score()
    pool_out(2).start()
    fold_at(fold_column, x_at == 0)

    with jax.named_scope("wo"):
        pltpu.make_async_copy(wo_buf.at[OWN], wo_buf.at[OWN], wo_loc).wait()
        to_peer(wo_buf.at[OWN], wo_buf.at[PEER], wo_send, wo_recv).wait_recv()
        pool_out(0).wait_recv()

    pool_at, rec_at = slice(0, pool_w), slice(pool_w, pool_w + chans)

    def pool_part(c):
        rows = rows_of(c)
        r_buf[rows, :] = (
            dot(a_buf[OWN, rows, pool_at], wo_buf[OWN, pool_at]) + dot(a_buf[PEER, rows, pool_at], wo_buf[PEER, pool_at])
            + ALPHA * x_buf[OWN, rows, :].astype(F32))

    with jax.named_scope("pool"):
        pool_part(chunks - 1)
        parts[0].inner()
        pool_part(chunks - 2)
    with jax.named_scope("pool_recv"):
        pool_out(1).wait_recv()
        pool_out(2).wait_recv()
    with jax.named_scope("pool"):
        pool_part(1)
        pool_part(0)

    @pl.when(sp > 0)
    def _():
        with jax.named_scope("start_recv"):
            some(start_in, row_n - 1, b_send, b_recv).wait_recv()

    @pl.when(sp > 0)
    def _():
        for h in range(heads):
            state[:, head_of(h)] = start_in[h].astype(F32)

    @pl.when(sp == 0)
    def _():
        state[...] = jnp.zeros_like(state)

    def fourth(c):
        for k in range(per):
            b = c * per + k
            half = half_buf[b, 0:1]
            before = state[...] * half
            carried = before.astype(BF16)
            state[...] = before * half + t_buf[b]
            for h in range(heads):
                lanes = head_of(h)
                raw = e_buf[block_of(b), lanes] + dot(q_buf[block_of(b), lanes], carried[:, lanes], NT)
                power = jnp.mean(raw * raw, axis=-1, keepdims=True)
                rec = raw * lax.rsqrt(power + EPS_RMS) * g_buf[block_of(b), lanes]
                a_buf[OWN, block_of(b), pool_w + h * DK:pool_w + (h + 1) * DK] = rec.astype(BF16)

    def rec_part(side, c):
        r_buf[rows_of(c), :] += dot(a_buf[side, rows_of(c), rec_at], wo_buf[side, rec_at])

    with jax.named_scope("fourth"):
        fourth(0)
        fourth(1)
        rec_out(0).start()
        rec_out(1).start()
    with jax.named_scope("fourth2"):
        fourth(2)
        rec_part(OWN, 0)
        rec_out(2).start()
        fourth(3)
        rec_part(OWN, 1)
        rec_out(3).start()

    def fold(x):
        acc = x[:, :LANES]
        for k in range(1, feats // LANES):
            acc = acc + x[:, k * LANES:(k + 1) * LANES]
        return acc

    first_half = lax.broadcasted_iota(jnp.int32, (rows_x, LANES), 1) < LANES // 2

    def fifth(c):
        rows = rows_of(c)
        resid = r_buf[rows, :] + dot(a_buf[PEER, rows, rec_at], wo_buf[PEER, rec_at])
        r_buf[rows, :] = resid
        sums, squares = fold(resid), fold(resid * resid)
        sums = sums + pltpu.roll(sums, LANES // 2, 1)
        squares = squares + pltpu.roll(squares, LANES // 2, 1)
        stat_own[rows, :] = jnp.where(first_half, sums, squares)

    with jax.named_scope("fifth"):
        rec_part(OWN, 2)
        rec_part(OWN, 3)
        for c in range(3):
            with jax.named_scope("rec_recv"):
                rec_out(c).wait_recv()
        for c in range(3):
            fifth(c)
        s_out(0).start()
    with jax.named_scope("fifth3"):
        with jax.named_scope("rec_recv"):
            rec_out(3).wait_recv()
        fifth(3)
        s_out(1).start()

    with jax.named_scope("sent"):
        to_peer(x_buf.at[OWN], x_buf.at[PEER], x_send, x_recv.at[0]).wait_send()
        to_peer(a_buf.at[OWN], a_buf.at[PEER], a_send, a_recv.at[0]).wait_send()
        to_peer(wo_buf.at[OWN], wo_buf.at[PEER], wo_send, wo_recv).wait_send()
        some(mine_out, row_n - 1, m_send, m_recv).wait_send()
        when_equal(col_n - 1 - z_at, range(1, col_n), lambda n: some(total_in, n, r_send, r_recv).wait_send())
        starts = jnp.where((z_at > 0) | (x_at == 0), row_n - 1, row_n - 2)
        when_equal(starts, (row_n - 2, row_n - 1), lambda n: some(start_out, n, b_send, b_recv).wait_send())

        @pl.when(sp + 1 < n_sp)
        def _():
            h_out(sp + 1).wait_send()

    with jax.named_scope("tail"):
        for i, (start, n) in enumerate(stat_pieces):
            s_out(i).wait_recv()
            stats[start:start + n, :] = stat_own[start:start + n, :] + stat_peer[start:start + n, :]
        to_peer(stat_own, stat_peer, s_send, s_recv.at[0]).wait_send()


def finish(width, rows, resid, stats, gain, bias, out, o_buf, o_sem):
    pieces = resid.shape[0] // rows

    def leave(c):
        part = pl.ds(c * rows, rows)
        return pltpu.make_async_copy(o_buf.at[part], out.at[0, part], o_sem.at[c])

    half = rows // 2
    first_half = lax.broadcasted_iota(jnp.int32, (half, LANES), 1) < LANES // 2
    for c in range(pieces):
        for k in range(2):
            part = slice(c * rows + k * half, c * rows + (k + 1) * half)
            both = stats[part, :]
            mean = jnp.sum(jnp.where(first_half, both, 0.0), axis=1, keepdims=True) * (1.0 / width)
            square = jnp.sum(jnp.where(first_half, 0.0, both), axis=1, keepdims=True) * (1.0 / width)
            inv = lax.rsqrt(square - mean * mean + EPS_NORM)
            shift = -mean * inv
            o_buf[part, :] = ((resid[part, :] * inv + shift) * gain[...] + bias[...]).astype(BF16)
        leave(c).start()
    for c in range(pieces):
        leave(c).wait()


def solution(mesh):
    n_sp, n_tp = mesh.shape["sp"], mesh.shape["tp"]

    def local(stream, w_pool, w_query, w_forget, w_value, w_gate, mix, scale, bound, extra,
              gain, wo_pool, wo_rec, norm_gain, norm_bias):
        length, feats = stream.shape[1], stream.shape[2]
        chans, pool_w = bound.shape[0], scale.shape[0]
        heads = chans // DK
        blocks = length // BLOCK_ROWS
        rows_x = 256
        chunks = length // rows_x
        hbm = pl.BlockSpec(memory_space=pl.ANY)
        vmem = pl.BlockSpec(memory_space=pltpu.VMEM)
        dma = pltpu.SemaphoreType.DMA
        scratch = [
            pltpu.VMEM((n_tp, length, feats), BF16),
            pltpu.VMEM((5, n_tp, feats, chans), BF16),
            pltpu.VMEM((n_tp, pool_w + chans, feats), BF16),
            pltpu.VMEM((n_tp, length, pool_w + chans), BF16),
            pltpu.VMEM((length, chans), BF16),
            pltpu.VMEM((length, chans), BF16),
            pltpu.VMEM((length, chans), F32),
            pltpu.VMEM((blocks, DK, chans), F32),
            pltpu.VMEM((BLOCK_ROWS + length, pool_w), BF16),
            pltpu.VMEM((length, chans), BF16),
            pltpu.VMEM((length, chans), F32),
            pltpu.VMEM((length, chans), BF16),
            pltpu.VMEM((blocks, 8, chans), F32),
            pltpu.VMEM((DK, chans), F32),
            pltpu.VMEM((heads, DK + HALO, DK), BF16),
            pltpu.VMEM((heads, DK + HALO, DK), BF16),
            pltpu.VMEM((DK + HALO, DK), BF16),
            pltpu.VMEM((n_sp // heads, DK + HALO, DK), BF16),
            pltpu.VMEM((heads, DK, DK), BF16),
            pltpu.VMEM((heads, DK, DK), BF16),
            pltpu.VMEM((HALO, pool_w), BF16),
            pltpu.VMEM((length, LANES), F32),
            pltpu.VMEM((length, LANES), F32),
            pltpu.VMEM((mix.shape[0], BLOCK_ROWS, 2 * BLOCK_ROWS), BF16),
            pltpu.VMEM(mix.shape, BF16),
            pltpu.VMEM((1, pool_w), F32),
            pltpu.VMEM((1, chans), F32),
            pltpu.VMEM((heads, length), F32),
            pltpu.VMEM((1, DK), F32),
            dma((2,)), dma, dma((2,)), dma((5,)), dma, dma, dma, dma, dma((7,)),
            dma, dma, dma, dma, dma, dma, dma, dma, dma, dma((2,)), dma((5,)), pltpu.SemaphoreType.REGULAR,
        ]
        row = lambda x: x.reshape(1, -1)
        resid, stats = pl.pallas_call(
            functools.partial(mixer, n_sp, n_tp, rows_x),
            out_shape=(pltpu.VMEM((length, feats), F32), pltpu.VMEM((length, LANES), F32)),
            in_specs=[hbm] * 13,
            out_specs=(vmem, vmem),
            scratch_shapes=scratch,
            compiler_params=pltpu.CompilerParams(
                collective_id=0, has_side_effects=True, vmem_limit_bytes=LIMIT),
            name="mixer",
        )(stream, w_pool, w_query, w_forget, w_value, w_gate, mix, row(scale), row(bound), extra.T,
          row(gain), wo_pool, wo_rec)
        piece = 128
        pieces = length // piece
        return pl.pallas_call(
            functools.partial(finish, n_tp * feats, piece),
            out_shape=jax.ShapeDtypeStruct(stream.shape, BF16),
            in_specs=[vmem] * 4,
            out_specs=hbm,
            scratch_shapes=[pltpu.VMEM((length, feats), BF16), dma((pieces,))],
            compiler_params=pltpu.CompilerParams(vmem_limit_bytes=16 * 1024 * 1024),
            name="finish",
        )(resid, stats, row(norm_gain), row(norm_bias))

    placed = (
        P("fs", "sp", "tp"), P(None, "tp"), P(None, "tp"), P(None, "tp"), P(None, "tp"),
        P(None, "tp"), P("tp", None, None), P("tp"), P("tp"), P("sp", "tp"), P(),
        P("tp", None), P("tp", None), P("tp"), P("tp"),
    )
    return jax.shard_map(
        local, mesh=mesh, in_specs=placed, out_specs=P("fs", "sp", "tp"), check_vma=False
    )
```
